256 devices in a mesh: ep: 64 (over z, y, core), tp: 4 (over x).
Axes of the slice: x: 4, y: 4, z: 8, core: 2. Of those that a mesh axis runs over, the one named last changes fastest.
Arguments:
- query: bfloat16 [8192, 1536], P('ep', 'tp'), may hold values from -136 to 136
- latent: bfloat16 [8192, 512], P(('ep', 'tp')), may hold values from -6 to 6
- rope_key: bfloat16 [8192, 32], P(('ep', 'tp')), may hold values from -6 to 6
- latent_gain: float32 [512], replicated, may hold values from 0.1 to 1.9
- key_up: bfloat16 [512, 1024], P(None, 'tp'), may hold values from -0.25 to 0.25
- value_up: bfloat16 [512, 1024], P(None, 'tp'), may hold values from -2 to 2
- out_proj: bfloat16 [1024, 2048], replicated, may hold values from -0.1875 to 0.1875
- tokens: bfloat16 [16384, 2048], P(('ep', 'tp')), may hold values from -6 to 6
- moe_gain: float32 [2048], replicated, may hold values from 0.1 to 1.9
- routes: int32 [16384, 2], P(('ep', 'tp')), may hold values from 0 to 63, all different within a row; in each aligned block of 64 rows (0 to 63, 64 to 127, ...) at most 4 rows name the same one
- group_prob: float32 [16384], P(('ep', 'tp')), may hold values from 0.25 to 1
- expert_prob: float32 [16384, 2], P(('ep', 'tp')), may hold values from 0.02 to 1
- w_gate: bfloat16 [64, 2048, 1024], P('ep', None, 'tp'), may hold values from -0.125 to 0.125
- w_up: bfloat16 [64, 2048, 1024], P('ep', None, 'tp'), may hold values from -0.125 to 0.125
- w_down: bfloat16 [64, 1024, 2048], P('ep', 'tp'), may hold values from -0.1875 to 0.1875
Outputs:
- mixed: bfloat16 [8192, 2048], P(('ep', 'tp'))
- moe_out: bfloat16 [16384, 2048], P(('ep', 'tp'))
The draws below stay inside these ranges and needn't reach their ends.
Inputs may be any that keep to these rules, and one draw needn't show every extreme that they name: `routes`: each row names 2 different experts; within the rows of one device no expert is named more than 4 times.
All inputs are finite; a program needn't handle non-finite values.
Results may differ from the reference program's by a relative error of at most 0.025.
Values may be sent and summed in bfloat16 or wider, within the bound.
No kernel may reach another device: no remote copies, remote signals or barrier semaphores. Data moves between devices by JAX's collectives and lax.ppermute only.
A program may use at most 128 MiB of HBM per device.

```python
import functools
import math
import jax
import jax.numpy as jnp
import numpy as np
from jax import lax

D = 2048
HEADS = 16
NOPE = 64
ROPE_DIM = 32
V_DIM = 64
LATENT = 512
EXPERT_WIDTH = 1024
TOP = 2
M_ROWS = 64
SEQ = 8192
MOE_TOKENS = 16384
EXPERTS = 64
CAP = 4
N_TP = 4


def draw_query(key, part):
    first_key = jax.random.fold_in(jax.random.fold_in(key, 11), 0)
    full_shape = (SEQ, HEADS * (NOPE + ROPE_DIM))
    values = jnp.clip(2.0 * jax.random.normal(first_key, full_shape, jnp.float32), -8.0, 8.0)
    return values.astype(jnp.bfloat16)


def block_scale(own_key, dims, cuts, smallest, top_value):
    def one(position, blocks):
        draws = jax.random.uniform(jax.random.fold_in(jax.random.fold_in(own_key, 6), position), (blocks,), jnp.float32, smallest / len(cuts), top_value / len(cuts))
        return jnp.repeat(jnp.exp(draws), dims[position] // blocks).reshape((-1,) + (1,) * (len(dims) - position - 1))

    factor_of = one(*cuts[0])
    for cut in cuts[1:]:
        factor_of = factor_of * one(*cut)
    return factor_of


def assign_block(stream_key, own, number, rows, count, top, most, slope):
    order = jax.random.permutation(stream_key, count)
    crowded, usual = portions_of(count, rows * top, most, slope, True), portions_of(count, rows * top, most, slope, False)
    places = jnp.arange(count)

    def named(lengths, turn):
        used = int((lengths > 0).sum())
        fixed = max(1, used // 4)
        shifted = fixed + (places - fixed + turn * (used - fixed)) % max(1, count - fixed)
        return jnp.zeros((count,), jnp.int32).at[order[jnp.where(places < fixed, places, shifted)]].set(jnp.asarray(lengths, jnp.int32))

    lengths = jnp.where(number % 4 == 0, named(crowded, number // 4), named(usual, number - number // 4 - 1))
    mixed = jax.random.permutation(jax.random.fold_in(own, 3), count)
    source_of, taker = mixed[0:count // 2 * 2:2], mixed[1:count // 2 * 2:2]
    room = jnp.minimum(lengths[source_of] - 1, most - lengths[taker]) // 2
    room = jnp.where((source_of == order[0]) | (taker == order[0]) | (lengths[taker] == 0), 0, jnp.maximum(room, 0))
    shifted = jax.random.randint(jax.random.fold_in(own, 4), (count // 2,), 0, 1 << 20) % (room + 1)
    lengths = lengths.at[source_of].add(-shifted).at[taker].add(shifted)
    items = jnp.searchsorted(jnp.cumsum(lengths), jnp.arange(rows * top), side="right").astype(jnp.int32)
    grid = items.reshape(top, rows).T
    grid = grid[jax.random.permutation(jax.random.fold_in(own, 1), rows)]
    turn = jax.random.randint(jax.random.fold_in(own, 2), (rows, 1), 0, top)
    return jnp.take_along_axis(grid, (jnp.arange(top)[None, :] + turn) % top, axis=1)


def portions_of(number_of, total, reach, slope, full):
    portions = [(1 << 20) // math.isqrt(standing ** slope) + 1 for standing in range(1, number_of + 1)]
    largest = reach if full else min(reach, max(-(-total // number_of), total * portions[0] // sum(portions)))
    least = 1 if total - largest >= number_of - 1 else 0
    given, rest = [largest] + [least] * (number_of - 1), total - largest - least * (number_of - 1)
    while rest > 0:
        movable = [i for i in range(1, number_of) if given[i] < largest] or [i for i in range(1, number_of) if given[i] < reach]
        pool, budget = sum([portions[i] for i in movable]), rest
        for i in movable:
            more = min(reach - given[i], max(1, budget * portions[i] // pool), rest)
            given[i] = given[i] + more
            rest = rest - more
    return np.array(given)


def centred(key, shape, spread, bound, cuts=(), kind=jnp.bfloat16):
    array = jax.random.normal(key, shape, jnp.float32) * spread
    if len(cuts) > 0:
        array = block_scale(key, shape, cuts, -0.22, 0.18) * array
    return jnp.clip(array, min=-bound, max=bound).astype(kind)


def setup_inputs(seed: int = 0) -> dict:
    key_list = jax.random.split(jax.random.key(seed), 16)
    query = draw_query(jax.random.fold_in(key_list[15], 71), 0)
    latent = centred(key_list[1], (SEQ, LATENT), 1.0, 6.0, ((0, 256),))
    rope_key = centred(key_list[2], (SEQ, ROPE_DIM), 1.0, 6.0, ((0, 256),))
    latent_gain = jnp.clip(1.0 + 0.18 * jax.random.normal(key_list[3], (LATENT,), jnp.float32), 0.1, 1.9)
    key_up = centred(key_list[4], (LATENT, HEADS * NOPE), LATENT ** -0.5, 0.25, ((1, 4),))
    value_up = centred(key_list[5], (LATENT, HEADS * V_DIM), (LATENT // 64) ** -0.5, 2.0, ((1, 4),))
    out_proj = centred(key_list[6], (HEADS * V_DIM, D), (HEADS * V_DIM) ** -0.5, 0.1875)
    tokens = centred(key_list[7], (MOE_TOKENS, D), 1.0, 6.0, ((0, 256),))
    moe_gain = jnp.clip(1.0 + 0.18 * jax.random.normal(key_list[8], (D,), jnp.float32), 0.1, 1.9)
    routes_keys = jax.random.split(jax.random.fold_in(key_list[9], 1), MOE_TOKENS // M_ROWS)
    routes_turns = jax.random.permutation(jax.random.fold_in(key_list[9], 3), MOE_TOKENS // M_ROWS)
    routes = jax.vmap(lambda own, number: assign_block(jax.random.fold_in(key_list[9], 2), own, number, M_ROWS, EXPERTS, TOP, CAP, 2))(routes_keys, routes_turns).reshape((MOE_TOKENS, TOP))
    group_prob = jnp.clip(jnp.exp(math.log(1.0) - 1.3862944 * jax.random.uniform(key_list[10], (MOE_TOKENS,), jnp.float32) ** block_scale(key_list[10], (MOE_TOKENS,), ((0, 256),), -0.2, 0.2)), 0.25, 1.0)
    expert_prob = jnp.clip(jnp.exp(math.log(1.0) - 3.912023 * jax.random.uniform(key_list[11], (MOE_TOKENS, TOP), jnp.float32) ** block_scale(key_list[11], (MOE_TOKENS, TOP), ((0, 256),), -0.2, 0.2)), 0.02, 1.0)
    w_gate = centred(key_list[12], (EXPERTS, D, EXPERT_WIDTH), D ** -0.5, 0.125, ((0, 64), (2, 4)))
    w_up = centred(key_list[13], (EXPERTS, D, EXPERT_WIDTH), D ** -0.5, 0.125, ((0, 64), (2, 4)))
    w_down = centred(key_list[14], (EXPERTS, EXPERT_WIDTH, D), EXPERT_WIDTH ** -0.5, 0.1875, ((0, 64), (1, 4)))
    return {"query": query, "latent": latent, "rope_key": rope_key, "latent_gain": latent_gain, "key_up": key_up, "value_up": value_up, "out_proj": out_proj, "tokens": tokens, "moe_gain": moe_gain, "routes": routes, "group_prob": group_prob, "expert_prob": expert_prob, "w_gate": w_gate, "w_up": w_up, "w_down": w_down}


epsilon = 1e-06
rope_base = 10000.0
masked_value = -1e+30

def rms_scale(values, gain):
    widened = values.astype(jnp.float32)
    return widened * lax.rsqrt(lax.optimization_barrier(jnp.mean(widened * widened, axis=-1, keepdims=True)) + epsilon) * gain.astype(jnp.float32)

def tables(positions, rope_width):
    half_width = rope_width // 2
    inverse = rope_base ** (-2.0 * jnp.arange(half_width, dtype=jnp.float32) / rope_width)
    angles = positions.astype(jnp.float32)[:, None] * inverse[None, :]
    return (jnp.cos(angles), jnp.sin(angles))

def rotate(values, cosine, sine):
    half_width = values.shape[-1] // 2
    lower = values[..., :half_width]
    upper = values[..., half_width:]
    return jnp.concatenate([lower * cosine - upper * sine, lower * sine + upper * cosine], axis=-1)

def head_attention(rope_prefix, query_pos, parts):
    query_head, key_head, value_head = parts
    full_keys = jnp.concatenate([key_head, rope_prefix], axis=-1)
    scores = jnp.dot(query_head, full_keys.T, preferred_element_type=jnp.float32) * (NOPE + ROPE_DIM) ** (-0.5)
    key_pos = jnp.arange(full_keys.shape[0], dtype=jnp.int32)
    allowed = key_pos[None, :] <= query_pos[:, None]
    scores = jnp.where(allowed, scores, masked_value)
    row_peak = lax.optimization_barrier(jnp.max(scores, axis=-1, keepdims=True))
    raised = jnp.where(allowed, jnp.exp(scores - row_peak), 0.0)
    totals = lax.optimization_barrier(jnp.sum(raised, axis=-1, keepdims=True))
    summed = jnp.dot(raised.astype(jnp.bfloat16), value_head, preferred_element_type=jnp.float32)
    return (summed / totals).astype(jnp.bfloat16)

def mixer_reference(query, latent, rope_key, latent_gain, key_up, value_up, out_proj):
    seq_len = latent.shape[0]
    positions = jnp.arange(seq_len, dtype=jnp.int32)
    cosine, sine = tables(positions, ROPE_DIM)
    normed = rms_scale(latent, latent_gain).astype(jnp.bfloat16)
    rotated_key = rotate(rope_key.astype(jnp.float32), cosine, sine).astype(jnp.bfloat16)
    query_heads = query.reshape(seq_len, HEADS, NOPE + ROPE_DIM)
    turned = rotate(query_heads[..., NOPE:].astype(jnp.float32), cosine[:, None, :], sine[:, None, :]).astype(jnp.bfloat16)
    rotated_query = jnp.concatenate([query_heads[..., :NOPE], turned], axis=-1)
    key_nope = jnp.dot(normed, key_up, preferred_element_type=jnp.float32).astype(jnp.bfloat16).reshape(seq_len, HEADS, NOPE)
    values = jnp.dot(normed, value_up, preferred_element_type=jnp.float32).astype(jnp.bfloat16).reshape(seq_len, HEADS, V_DIM)
    block_len = math.gcd(seq_len, 512)
    pieces = []
    for block_at in range(seq_len // block_len):
        upto = (block_at + 1) * block_len
        query_pos = positions[block_at * block_len:upto]
        parts = (rotated_query[block_at * block_len:upto].transpose(1, 0, 2), key_nope[:upto].transpose(1, 0, 2), values[:upto].transpose(1, 0, 2))
        result = lax.map(functools.partial(head_attention, rotated_key[:upto], query_pos), parts)
        pieces.append(result.transpose(1, 0, 2).reshape(block_len, HEADS * V_DIM))
    attention = jnp.concatenate(pieces, axis=0)
    return jnp.dot(attention, out_proj, preferred_element_type=jnp.float32).astype(jnp.bfloat16)

def expert_reference(tokens, moe_gain, routes, group_prob, expert_prob, w_gate, w_up, w_down):
    amount = tokens.shape[0]
    model_width = tokens.shape[1]
    expert_count = w_gate.shape[0]
    block_count = amount // M_ROWS
    normed = rms_scale(tokens, moe_gain).astype(jnp.bfloat16)
    flat_routes = routes.reshape(block_count, M_ROWS * TOP)
    onehot = (flat_routes[:, :, None] == jnp.arange(expert_count, dtype=jnp.int32)[None, None, :]).astype(jnp.int32)
    earlier = jnp.cumsum(onehot, axis=1) - onehot
    slot_index = lax.optimization_barrier(jnp.sum(earlier * onehot, axis=2))
    block_ids = jnp.arange(block_count, dtype=jnp.int32)[:, None]
    place = block_ids * CAP + slot_index
    source_row = block_ids * M_ROWS + jnp.arange(M_ROWS * TOP, dtype=jnp.int32)[None, :] // TOP
    shares = group_prob[:, None] * expert_prob / lax.optimization_barrier(jnp.sum(expert_prob, axis=1, keepdims=True))
    row_table = jnp.full((expert_count, block_count * CAP), amount, jnp.int32).at[flat_routes, place].set(source_row)
    share_table = jnp.zeros((expert_count, block_count * CAP), jnp.float32).at[flat_routes, place].set(shares.reshape(block_count, M_ROWS * TOP))
    padded = jnp.concatenate([normed, jnp.zeros((1, model_width), jnp.bfloat16)], axis=0)
    group_width = w_down.shape[1] // N_TP

    def per_expert(running, parts):
        row_ids, row_shares, gate_weight, up_weight, down_weight = parts
        rows_here = padded[row_ids]
        gate_values = jnp.dot(rows_here, gate_weight, preferred_element_type=jnp.float32)
        up_values = jnp.dot(rows_here, up_weight, preferred_element_type=jnp.float32)
        hidden = (jax.nn.silu(gate_values) * up_values).astype(jnp.bfloat16)
        summed = jnp.zeros((rows_here.shape[0], model_width), jnp.float32)
        for group_at in range(N_TP):
            lower_edge = group_at * group_width
            partial_low = jnp.dot(hidden[:, lower_edge:lower_edge + group_width], down_weight[lower_edge:lower_edge + group_width], preferred_element_type=jnp.float32).astype(jnp.bfloat16)
            partial_low = lax.optimization_barrier(partial_low)
            summed = summed + partial_low.astype(jnp.float32)
        expert_out = summed.astype(jnp.bfloat16)
        expert_out = lax.optimization_barrier(expert_out)
        running = running.at[row_ids].add(row_shares[:, None] * expert_out.astype(jnp.float32))
        return (running, None)
    running, _ = lax.scan(per_expert, jnp.zeros((amount + 1, model_width), jnp.float32), (row_table, share_table, w_gate, w_up, w_down))
    return running[:amount].astype(jnp.bfloat16)

def reference(query, latent, rope_key, latent_gain, key_up, value_up, out_proj, tokens, moe_gain, routes, group_prob, expert_prob, w_gate, w_up, w_down):
    mixed = mixer_reference(query, latent, rope_key, latent_gain, key_up, value_up, out_proj)
    moe_out = expert_reference(tokens, moe_gain, routes, group_prob, expert_prob, w_gate, w_up, w_down)
    return (mixed, moe_out)
```

```python
import functools

import jax
import jax.numpy as jnp
from jax import lax
from jax.experimental import pallas as pl
from jax.experimental.pallas import tpu as pltpu
from jax.sharding import Mesh, PartitionSpec as P

NOPE = 64
ROPE_DIM = 32
V_DIM = 64
QK_DIM = NOPE + ROPE_DIM
KV_ROWS = QK_DIM + V_DIM
CAP = 4
BF = jnp.bfloat16
F32 = jnp.float32

epsilon = 1e-06
rope_base = 10000.0
masked_value = -1e30
log2_e = 1.4426950408889634

SMEM_SPEC = pl.BlockSpec(memory_space=pltpu.SMEM)


def mm(a, b, dims=((1,), (0,))):
    return lax.dot_general(a, b, (dims, ((), ())), preferred_element_type=F32)


def shifted(value, axis, amount):
    n = lax.axis_size(axis)
    return lax.ppermute(value, axis, [(i, (i + amount) % n) for i in range(n)])


def trig(positions):
    half = ROPE_DIM // 2
    inverse = rope_base ** (-2.0 * jnp.arange(half, dtype=F32) / ROPE_DIM)
    angles = positions.astype(F32)[:, None] * inverse[None, :]
    return jnp.cos(angles), jnp.sin(angles)


def rms_scale(values, gain):
    widened = values.astype(F32)
    return widened * lax.rsqrt(jnp.mean(widened * widened, axis=-1, keepdims=True) + epsilon) * gain


def dispatch_kernel(tokens, gain, routes, group_prob, expert_prob, outgoing, shares_out):
    rows = tokens.shape[0]
    slots = outgoing.shape[0]
    normed = rms_scale(tokens[...], gain[...]).astype(BF)
    slot = lax.broadcasted_iota(jnp.int32, (rows, slots), 1)
    expert = slot // CAP
    first = routes[:, 0:1] == expert
    second = routes[:, 1:2] == expert
    named = (first | second).astype(BF)
    before = lax.broadcasted_iota(jnp.int32, (rows, rows), 1) < lax.broadcasted_iota(
        jnp.int32, (rows, rows), 0
    )
    prior = mm(before.astype(BF), named)
    mine = (first | second) & (prior == (slot % CAP).astype(F32))
    outgoing[...] = mm(mine.astype(BF), normed, ((0,), (0,))).astype(BF)
    probs = expert_prob[...]
    shares = group_prob[...] * probs / jnp.sum(probs, axis=1, keepdims=True)
    weights = jnp.where(first, shares[:, 0:1], shares[:, 1:2])
    weights = jnp.where(mine, weights, 0.0)
    high = weights.astype(BF)
    shares_out[0:rows, :] = high
    shares_out[rows : 2 * rows, :] = (weights - high.astype(F32)).astype(BF)


def dispatch(tokens, gain, routes, group_prob, expert_prob, slots):
    rows, width = tokens.shape
    return pl.pallas_call(
        dispatch_kernel,
        out_shape=(
            jax.ShapeDtypeStruct((slots, width), BF),
            jax.ShapeDtypeStruct((2 * rows, slots), BF),
        ),
        name="dispatch",
    )(tokens, gain[None, :], routes, group_prob[:, None], expert_prob)


def hidden_kernel(rows, w_gate, w_up, out):
    gate = mm(rows[...], w_gate[...])
    up = mm(rows[...], w_up[...])
    out[...] = (gate / (1.0 + jnp.exp(-gate)) * up).astype(BF)


def hidden_of(rows, w_gate, w_up, name):
    return pl.pallas_call(
        hidden_kernel,
        out_shape=jax.ShapeDtypeStruct((rows.shape[0], w_gate.shape[1]), BF),
        name=name,
    )(rows, w_gate, w_up)


def down_kernel(h0, h1, h2, h3, w0, w1, w2a, w2b, w3, out):
    half = w2a.shape[0]
    total = mm(h0[...], w0[...]) + mm(h1[...], w1[...]) + mm(h3[...], w3[...])
    total = total + mm(h2[:, :half], w2a[...]) + mm(h2[:, half:], w2b[...])
    out[...] = total.astype(BF)


def combine_kernel(returned, shares, out):
    rows = out.shape[0]
    both = mm(shares[...], returned[...])
    out[...] = (both[:rows] + both[rows:]).astype(BF)


def ring_gathered(value):
    half = value.shape[0] // 2
    left = shifted(value, "x", 1)
    right = shifted(value, "x", -1)
    far_a = shifted(left[:half], "x", 1)
    far_b = shifted(right[half:], "x", -1)
    return left, right, far_a, far_b


def expert_half(tokens, moe_gain, routes, group_prob, expert_prob, w_gate, w_up, w_down):
    ep_axes = ("z", "y", "c")
    experts = lax.axis_size(ep_axes)
    rows, width = tokens.shape
    slots = experts * CAP
    w_gate, w_up, w_down = w_gate[0], w_up[0], w_down[0]
    down_left, down_right, down_far_a, down_far_b = ring_gathered(w_down)
    outgoing, shares = dispatch(tokens, moe_gain, routes, group_prob, expert_prob, slots)
    arrived = lax.all_to_all(
        outgoing.reshape(experts, CAP, width), ep_axes, split_axis=0, concat_axis=0, tiled=True
    ).reshape(slots, width)
    left, right, far_a, far_b = ring_gathered(arrived)
    own_hidden = hidden_of(arrived, w_gate, w_up, "hidden_own")
    left_hidden = hidden_of(left, w_gate, w_up, "hidden_left")
    right_hidden = hidden_of(right, w_gate, w_up, "hidden_right")
    far_hidden = hidden_of(jnp.concatenate([far_a, far_b], axis=0), w_gate, w_up, "hidden_far")
    from_right = shifted(left_hidden, "x", -1)
    from_left = shifted(right_hidden, "x", 1)
    from_far = shifted(far_hidden, "x", 2)
    result = pl.pallas_call(
        down_kernel, out_shape=jax.ShapeDtypeStruct((slots, width), BF), name="down"
    )(
        own_hidden,
        from_right,
        from_far,
        from_left,
        w_down,
        down_right,
        down_far_a,
        down_far_b,
        down_left,
    )
    returned = lax.all_to_all(
        result.reshape(experts, CAP, width), ep_axes, split_axis=0, concat_axis=0, tiled=True
    ).reshape(slots, width)
    return pl.pallas_call(
        combine_kernel, out_shape=jax.ShapeDtypeStruct((rows, width), BF), name="combine"
    )(returned, shares)


def query_kernel(where, query, cosine, sine, o0, o1, o2, o3, heads):
    count = heads.shape[0]
    turned = query[...].astype(F32).T
    for h in range(count):
        at = h * QK_DIM
        half = ROPE_DIM // 2
        a = turned[at + NOPE : at + NOPE + half]
        b = turned[at + NOPE + half : at + QK_DIM]
        heads[h, :NOPE, :] = turned[at : at + NOPE].astype(BF)
        heads[h, NOPE : NOPE + half, :] = (a * cosine[...] - b * sine[...]).astype(BF)
        heads[h, NOPE + half :, :] = (a * sine[...] + b * cosine[...]).astype(BF)
    for k, out in enumerate((o0, o1, o2, o3)):
        out[...] = heads[lax.rem(where[1] + k, 4)]


def keys_kernel(where, l0, l1, l2, l3, key_up, value_up, out, keys, values):
    latent = key_up.shape[0]
    strip = l0.shape[0]
    eye = (
        lax.broadcasted_iota(jnp.int32, (ROPE_DIM, ROPE_DIM), 0)
        == lax.broadcasted_iota(jnp.int32, (ROPE_DIM, ROPE_DIM), 1)
    ).astype(BF)
    for j, block in enumerate((l0, l1, l2, l3)):
        cols = slice(j * strip, (j + 1) * strip)
        got = block[:, :latent]
        keys[:, :, cols] = (
            mm(key_up[...], got, ((0,), (1,))).astype(BF).reshape(keys.shape[0], NOPE, strip)
        )
        values[:, :, cols] = (
            mm(value_up[...], got, ((0,), (1,))).astype(BF).reshape(values.shape[0], V_DIM, strip)
        )
        out[NOPE:QK_DIM, cols] = mm(eye, block[:, latent:], ((1,), (1,))).astype(BF)
    out[:NOPE, :] = keys[where[1]]
    out[QK_DIM:, :] = values[where[1]]


def attend_kernel(where, q0, q1, q2, q3, kv, o0, o1, o2, o3, q_s, top_s, acc_s):
    step = pl.program_id(0)
    z, y, c, x = where[0], where[1], where[2], where[3]
    strip = q0.shape[1]
    span = kv.shape[2]
    factor = QK_DIM ** (-0.5) * log2_e

    @pl.when(step == 0)
    def _():
        for j, q in enumerate((q0, q1, q2, q3)):
            q_s[j] = q[...].astype(F32).T.astype(BF)
        top_s[...] = jnp.full(top_s.shape, masked_value, F32)
        acc_s[...] = jnp.zeros(acc_s.shape, F32)

    def advance(masked):
        ones = jnp.ones((V_DIM, span), BF)
        extended = [jnp.concatenate([kv[p, QK_DIM:, :], ones], axis=0) for p in range(2)]
        if masked:
            col = lax.broadcasted_iota(jnp.int32, (1, span), 1)
            col_y = (y - col // strip + 4) % 4
            col_x = (x - (col // 32) % 4 + 4) % 4
            key_at = [(col_y * 2 + p) * strip + col_x * 32 + col % 32 for p in range(2)]
            row = lax.broadcasted_iota(jnp.int32, (strip, 1), 0)
        for j in range(4):
            q = q_s[j]
            scores = [mm(q, kv[p, :QK_DIM, :]) for p in range(2)]
            if masked:
                query_at = (lax.rem(y - j + 4, 4) * 2 + c) * strip + row
                scores = [
                    jnp.where(key_at[p] <= query_at, scores[p], masked_value) for p in range(2)
                ]
            old = top_s[j]
            peak = jnp.maximum(
                jnp.max(scores[0], axis=1, keepdims=True),
                jnp.max(scores[1], axis=1, keepdims=True),
            )
            new = jnp.maximum(old, peak)
            top_s[j] = new
            base = new[:, :1]
            total = acc_s[j] * jnp.exp2((old - new) * factor)
            for p in range(2):
                raised = jnp.exp2((scores[p] - base) * factor).astype(BF)
                total = total + mm(raised, extended[p], ((1,), (1,)))
            acc_s[j] = total

    pl.when(step < z)(functools.partial(advance, False))
    pl.when(step == z)(functools.partial(advance, True))

    @pl.when(step == pl.num_programs(0) - 1)
    def _():
        for j, out in enumerate((o0, o1, o2, o3)):
            total = acc_s[j]
            out[...] = (total[:, :V_DIM] / total[:, V_DIM:]).astype(BF)


def attend(where, queries, kv):
    blocks, rows, span = kv.shape
    strip = queries[0].shape[1]
    steps = blocks // 2
    whole = pl.BlockSpec((QK_DIM, strip), lambda s, w: (0, 0))
    return pl.pallas_call(
        attend_kernel,
        grid_spec=pltpu.PrefetchScalarGridSpec(
            num_scalar_prefetch=1,
            grid=(steps,),
            in_specs=[whole] * 4
            + [pl.BlockSpec((2, rows, span), lambda s, w: (jnp.minimum(s, w[0]), 0, 0))],
            out_specs=[pl.BlockSpec((strip, V_DIM), lambda s, w: (0, 0))] * 4,
            scratch_shapes=[
                pltpu.VMEM((4, strip, QK_DIM), BF),
                pltpu.VMEM((4, strip, 128), F32),
                pltpu.VMEM((4, strip, 128), F32),
            ],
        ),
        out_shape=[jax.ShapeDtypeStruct((strip, V_DIM), BF)] * 4,
        name="attend",
    )(where, *queries, kv)


def spread_kernel(where, a0, a1, a2, a3, o0, o1, o2, o3, heads, parts):
    for j, a in enumerate((a0, a1, a2, a3)):
        heads[lax.rem(where[1] + j, 4)] = a[...]
    beside = jnp.concatenate([heads[h] for h in range(4)], axis=1)
    parts[...] = beside.reshape(parts.shape)
    for k, out in enumerate((o0, o1, o2, o3)):
        out[...] = parts[lax.rem(where[3] + k, 4)]


def project_kernel(where, a0, a1, a2, a3, out_proj, out, parts):
    width = a0.shape[1]
    for k, a in enumerate((a0, a1, a2, a3)):
        parts[lax.rem(where[3] - k + 4, 4)] = a[...]
    total = mm(parts[0], out_proj[:width, :])
    for h in range(1, 4):
        total = total + mm(parts[h], out_proj[h * width : (h + 1) * width, :])
    out[...] = total.astype(BF)


def mixer_half(where, query, latent, rope_key, latent_gain, key_up, value_up, out_proj):
    strip = query.shape[0]
    own = latent.shape[0]
    query_start = ((where[0] * 4 + where[1]) * 2 + where[2]) * strip
    vmem = pl.BlockSpec(memory_space=pltpu.VMEM)

    cosine, sine = trig(query_start + jnp.arange(strip, dtype=jnp.int32))
    shape = jax.ShapeDtypeStruct((QK_DIM, strip), BF)
    blocks = pl.pallas_call(
        query_kernel,
        in_specs=[SMEM_SPEC, vmem, vmem, vmem],
        out_shape=[shape] * 4,
        scratch_shapes=[pltpu.VMEM((4, QK_DIM, strip), BF)],
        name="queries",
    )(where, query, cosine.T, sine.T)
    queries = [blocks[0]] + [shifted(blocks[k], "y", k) for k in range(1, 4)]

    normed = rms_scale(latent, latent_gain).astype(BF)
    key_cos, key_sin = trig(query_start + where[3] * own + jnp.arange(own, dtype=jnp.int32))
    half = ROPE_DIM // 2
    a = rope_key[:, :half].astype(F32)
    b = rope_key[:, half:].astype(F32)
    both = jnp.concatenate(
        [
            normed,
            (a * key_cos - b * key_sin).astype(BF),
            (a * key_sin + b * key_cos).astype(BF),
        ],
        axis=1,
    )
    near = jnp.concatenate([both] + [shifted(both, "x", k) for k in range(1, 4)], axis=0)
    latents = [near] + [shifted(near, "y", k) for k in range(1, 4)]
    kv = pl.pallas_call(
        keys_kernel,
        in_specs=[SMEM_SPEC] + [vmem] * 6,
        out_shape=jax.ShapeDtypeStruct((KV_ROWS, 4 * strip), BF),
        scratch_shapes=[
            pltpu.VMEM((4, NOPE, 4 * strip), BF),
            pltpu.VMEM((4, V_DIM, 4 * strip), BF),
        ],
        name="keys",
    )(where, *latents, key_up, value_up)
    gathered = lax.all_gather(kv, ("z", "c"), axis=0, tiled=False)

    parts = attend(where, queries, gathered)
    parts = [parts[0]] + [shifted(parts[j], "y", -j) for j in range(1, 4)]
    shape = jax.ShapeDtypeStruct((own, 4 * V_DIM), BF)
    parts = pl.pallas_call(
        spread_kernel,
        in_specs=[SMEM_SPEC] + [vmem] * 4,
        out_shape=[shape] * 4,
        scratch_shapes=[
            pltpu.VMEM((4, strip, V_DIM), BF),
            pltpu.VMEM((4, own, 4 * V_DIM), BF),
        ],
        name="spread",
    )(where, *parts)
    parts = [parts[0]] + [shifted(parts[k], "x", k) for k in range(1, 4)]
    return pl.pallas_call(
        project_kernel,
        in_specs=[SMEM_SPEC] + [vmem] * 5,
        out_shape=jax.ShapeDtypeStruct((own, out_proj.shape[1]), BF),
        scratch_shapes=[pltpu.VMEM((4, own, 4 * V_DIM), BF)],
        name="project",
    )(where, *parts, out_proj)


def body(
    query,
    latent,
    rope_key,
    latent_gain,
    key_up,
    value_up,
    out_proj,
    tokens,
    moe_gain,
    routes,
    group_prob,
    expert_prob,
    w_gate,
    w_up,
    w_down,
):
    where = jnp.stack([lax.axis_index(n) for n in ("z", "y", "c", "x")]).astype(jnp.int32)
    mixed = mixer_half(where, query, latent, rope_key, latent_gain, key_up, value_up, out_proj)
    moe_out = expert_half(tokens, moe_gain, routes, group_prob, expert_prob, w_gate, w_up, w_down)
    return (mixed, moe_out)


def solution(mesh):
    ep = ("z", "y", "c")
    every = ("z", "y", "c", "x")
    split = Mesh(mesh.devices.reshape(8, 4, 2, 4), every)
    return jax.shard_map(
        body,
        mesh=split,
        in_specs=(
            P(ep, "x"),
            P(every, None),
            P(every, None),
            P(),
            P(None, "x"),
            P(None, "x"),
            P(),
            P(every, None),
            P(),
            P(every, None),
            P(every),
            P(every, None),
            P(ep, None, "x"),
            P(ep, None, "x"),
            P(ep, "x", None),
        ),
        out_specs=(P(every, None), P(every, None)),
        check_vma=False,
    )
```

```python
import jax
import jax.numpy as jnp
from jax import lax
from jax.experimental import pallas as pl
from jax.experimental.pallas import tpu as pltpu
from jax.sharding import Mesh, PartitionSpec as P

NOPE = 64
ROPE_DIM = 32
V_DIM = 64
QK_DIM = NOPE + ROPE_DIM
KV_ROWS = QK_DIM + V_DIM
CAP = 4
BF = jnp.bfloat16
F32 = jnp.float32

epsilon = 1e-06
rope_base = 10000.0
masked_value = -1e30
log2_e = 1.4426950408889634

AXES = ("zh", "zl", "y", "c", "x")
EP = AXES[:4]

SMEM_SPEC = pl.BlockSpec(memory_space=pltpu.SMEM)
VMEM_SPEC = pl.BlockSpec(memory_space=pltpu.VMEM)


def call(kernel, out_shape, name, arrays, where=None, scratch=(), limit=16 << 20):
    arrays = [pltpu.with_memory_space_constraint(a, pltpu.VMEM) for a in arrays]
    specs = [VMEM_SPEC] * len(arrays)
    if where is not None:
        arrays, specs = [where] + arrays, [SMEM_SPEC] + specs
    single = not isinstance(out_shape, (list, tuple))
    return pl.pallas_call(
        kernel,
        in_specs=specs,
        out_specs=VMEM_SPEC if single else [VMEM_SPEC] * len(out_shape),
        out_shape=out_shape,
        scratch_shapes=list(scratch),
        compiler_params=pltpu.CompilerParams(vmem_limit_bytes=limit),
        name=name,
    )(*arrays)


def mm(a, b, dims=((1,), (0,))):
    return lax.dot_general(a, b, (dims, ((), ())), preferred_element_type=F32)


def shifted(value, axis, amount):
    n = lax.axis_size(axis)
    return lax.ppermute(value, axis, [(i, (i + amount) % n) for i in range(n)])


def trig(positions):
    half = ROPE_DIM // 2
    inverse = rope_base ** (-2.0 * jnp.arange(half, dtype=F32) / ROPE_DIM)
    angles = positions.astype(F32)[:, None] * inverse[None, :]
    return jnp.cos(angles), jnp.sin(angles)


def rms_scale(values, gain):
    widened = values.astype(F32)
    return widened * lax.rsqrt(jnp.mean(widened * widened, axis=-1, keepdims=True) + epsilon) * gain


def dispatch_kernel(tokens, gain, routes, group_prob, expert_prob, outgoing, shares_out):
    rows = tokens.shape[0]
    experts, cap, width = outgoing.shape
    slots = experts * cap
    normed = rms_scale(tokens[...], gain[...]).astype(BF)
    slot = lax.broadcasted_iota(jnp.int32, (slots, rows), 0)
    expert = slot // cap
    first = routes[0:1, :] == expert
    second = routes[1:2, :] == expert
    named = (first | second).astype(BF)
    before = lax.broadcasted_iota(jnp.int32, (rows, rows), 0) < lax.broadcasted_iota(
        jnp.int32, (rows, rows), 1
    )
    prior = mm(named, before.astype(BF))
    mine = (first | second) & (prior == (slot % cap).astype(F32))
    outgoing[...] = mm(mine.astype(BF), normed).reshape(experts, cap, width).astype(BF)
    probs = expert_prob[...]
    shares = group_prob[...] * probs / jnp.sum(probs, axis=0, keepdims=True)
    weights = jnp.where(first, shares[0:1, :], shares[1:2, :])
    weights = jnp.where(mine, weights, 0.0)
    high = weights.astype(BF)
    shares_out[:, 0:rows] = high
    shares_out[:, rows : 2 * rows] = (weights - high.astype(F32)).astype(BF)


def dispatch(tokens, gain, routes, group_prob, expert_prob, experts):
    rows, width = tokens.shape
    return call(
        dispatch_kernel,
        (
            jax.ShapeDtypeStruct((experts, CAP, width), BF),
            jax.ShapeDtypeStruct((experts * CAP, 2 * rows), BF),
        ),
        "dispatch",
        [tokens, gain[None, :], routes.T, group_prob[None, :], expert_prob.T],
    )


def hidden_kernel(rows_a, rows_b, w_gate, w_up, out):
    half = out.shape[0] // 2
    for at, rows in ((0, rows_a), (half, rows_b)):
        got = rows[...].reshape(half, w_gate.shape[0])
        gate = mm(got, w_gate[...])
        up = mm(got, w_up[...])
        out[at : at + half, :] = (gate / (1.0 + jnp.exp(-gate)) * up).astype(BF)


def hidden_of(rows_a, rows_b, w_gate, w_up, name):
    shape = jax.ShapeDtypeStruct((2 * rows_a.shape[0] * CAP, w_gate.shape[1]), BF)
    return call(hidden_kernel, shape, name, [rows_a, rows_b, w_gate, w_up])


def down_kernel(h0, h1, h2, h3, w0, w1, w2, w3, out):
    total = mm(h0[...], w0[...]) + mm(h1[...], w1[...])
    total = total + mm(h2[...], w2[...]) + mm(h3[...], w3[...])
    out[...] = total.reshape(out.shape).astype(BF)


def combine_kernel(returned, shares, out):
    rows = out.shape[0]
    got = returned[...].reshape(shares.shape[0], out.shape[1])
    both = mm(shares[...], got, ((0,), (0,)))
    out[...] = (both[:rows] + both[rows:]).astype(BF)


def both_halves(
    where,
    query,
    latent,
    rope_key,
    latent_gain,
    key_up,
    value_up,
    out_proj,
    tokens,
    moe_gain,
    routes,
    group_prob,
    expert_prob,
    w_gate,
    w_up,
    w_down,
):
    experts = lax.axis_size(EP)
    rows, width = tokens.shape
    w_gate, w_up, w_down = w_gate[0], w_up[0], w_down[0]
    down = [shifted(w_down, "x", k) for k in (-1, 2, 1)]
    outgoing, shares = dispatch(tokens, moe_gain, routes, group_prob, expert_prob, experts)
    arrived = lax.all_to_all(outgoing, EP, split_axis=0, concat_axis=0, tiled=True)
    queries, pair = query_and_pair(where, query, latent, rope_key, latent_gain, key_up, value_up)
    arrived, pair, down = lax.optimization_barrier((arrived, pair, down))
    down = [w_down] + down
    half = experts // 2
    a, b = arrived[:half], arrived[half:]
    left_a, right_b = shifted(a, "x", 1), shifted(b, "x", -1)
    left_b, right_a = shifted(b, "x", 1), shifted(a, "x", -1)
    far_a, far_b = shifted(left_a, "x", 1), shifted(right_b, "x", -1)
    parts = attend(where, queries, pair)
    left_b, right_a, parts = lax.optimization_barrier((left_b, right_a, parts))
    hidden = [
        hidden_of(a, b, w_gate, w_up, "hidden_own"),
        shifted(hidden_of(left_a, left_b, w_gate, w_up, "hidden_left"), "x", -1),
        shifted(hidden_of(far_a, far_b, w_gate, w_up, "hidden_far"), "x", 2),
        shifted(hidden_of(right_a, right_b, w_gate, w_up, "hidden_right"), "x", 1),
    ]
    shape = jax.ShapeDtypeStruct((experts, CAP, width), BF)
    result = call(down_kernel, shape, "down", hidden + down)
    returned = lax.all_to_all(result, EP, split_axis=0, concat_axis=0, tiled=True)
    mixed = project(where, parts, out_proj, latent.shape[0])
    shape = jax.ShapeDtypeStruct((rows, width), BF)
    return mixed, call(combine_kernel, shape, "combine", [returned, shares])


def heads_kernel(
    where, l0, l1, l2, l3, key_up, value_up, query, cosine, sine, o0, o1, o2, o3, strip_s, heads
):
    latent = key_up.shape[0]
    own, strip = l0.shape[0], query.shape[0]
    count = heads.shape[0]
    half = ROPE_DIM // 2
    turned = query[...].astype(F32).T
    for h in range(count):
        at = h * QK_DIM
        a = turned[at + NOPE : at + NOPE + half]
        b = turned[at + NOPE + half : at + QK_DIM]
        heads[h, :NOPE, :] = turned[at : at + NOPE].astype(BF)
        heads[h, NOPE : NOPE + half, :] = (a * cosine[...] - b * sine[...]).astype(BF)
        heads[h, NOPE + half : QK_DIM, :] = (a * sine[...] + b * cosine[...]).astype(BF)
    for k, block in enumerate((l0, l1, l2, l3)):
        strip_s[k * own : (k + 1) * own, :] = block[...]
    got = strip_s[:, :latent]
    keys = mm(key_up[...], got, ((0,), (1,))).astype(BF)
    values = mm(value_up[...], got, ((0,), (1,))).astype(BF)
    eye = (
        lax.broadcasted_iota(jnp.int32, (ROPE_DIM, ROPE_DIM), 0)
        == lax.broadcasted_iota(jnp.int32, (ROPE_DIM, ROPE_DIM), 1)
    ).astype(BF)
    rope = mm(eye, strip_s[:, latent:], ((1,), (1,))).astype(BF)
    for h in range(count):
        heads[h, QK_DIM : QK_DIM + NOPE, :] = keys[h * NOPE : (h + 1) * NOPE]
        heads[h, QK_DIM + NOPE : 2 * QK_DIM, :] = rope
        heads[h, 2 * QK_DIM :, :] = values[h * V_DIM : (h + 1) * V_DIM]
    for k, out in enumerate((o0, o1, o2, o3)):
        out[...] = heads[lax.rem(where[0] + k, 4)]


def attend_kernel(where, q0, q1, q2, q3, *refs):
    blocks, (o0, o1, o2, o3, q_s, top_s, acc_s) = refs[:8], refs[8:]
    zh, zl, y, c, x = (where[i] for i in range(5))
    strip = q0.shape[1]
    span = blocks[0].shape[2]
    factor = QK_DIM ** (-0.5) * log2_e
    for j, q in enumerate((q0, q1, q2, q3)):
        at = pl.multiple_of(lax.rem(zh - j + 4, 4) * strip, strip)
        q_s[pl.ds(at, strip), :] = q[:QK_DIM, :].astype(F32).T.astype(BF)
    top_s[...] = jnp.full(top_s.shape, masked_value, F32)
    acc_s[...] = jnp.zeros(acc_s.shape, F32)

    col = lax.broadcasted_iota(jnp.int32, (1, span), 1)
    col_zl = jnp.bitwise_xor(zl, col // strip)
    within = col % strip
    col_x = ((x - within // 32 + 4) % 4) * 32 + within % 32
    query_at = (zl * 8 + y * 2 + c) * strip + lax.broadcasted_iota(jnp.int32, (strip, 1), 0)
    ones = jnp.ones((V_DIM, span), BF)

    def advance(rows, parts, masks):
        q = q_s[rows, :]
        old = top_s[rows, :]
        scores = [mm(q, part[:QK_DIM, :]) for part in parts]
        if masks is not None:
            scores = [jnp.where(m, s, masked_value) for m, s in zip(masks, scores)]
        peak = scores[0]
        for s in scores[1:]:
            peak = jnp.maximum(peak, s)
        new = jnp.maximum(old, jnp.max(peak, axis=1, keepdims=True))
        top_s[rows, :] = new
        base = new[:, :1]
        total = acc_s[rows, :] * jnp.exp2((old - new) * factor)
        for s, part in zip(scores, parts):
            raised = jnp.exp2((s - base) * factor).astype(BF)
            extended = jnp.concatenate([part[QK_DIM:, :], ones], axis=0)
            total = total + mm(raised, extended, ((1,), (1,)))
        acc_s[rows, :] = total

    for m in range(2):
        group = blocks[4 * m : 4 * m + 4]
        masks = []
        for k in range(4):
            key_y = lax.rem(y - k + 4, 4)
            key_at = (col_zl * 8 + key_y * 2 + jnp.bitwise_xor(c, m)) * strip + col_x
            masks.append(key_at <= query_at)
        for g in range(4):
            from_zh = lax.rem(zh - g + 4, 4)
            parts = [block[from_zh] for block in group]
            advance(slice(g * strip, (g + 1) * strip), parts, masks)
            if g < 3:
                advance(slice((g + 1) * strip, 4 * strip), parts, None)
    for j, out in enumerate((o0, o1, o2, o3)):
        at = pl.multiple_of(lax.rem(zh - j + 4, 4) * strip, strip)
        total = acc_s[pl.ds(at, strip), :]
        out[...] = (total[:, :V_DIM] / total[:, V_DIM:]).astype(BF)


def spread_kernel(where, a0, a1, a2, a3, o0, o1, o2, o3, heads, parts):
    for j, a in enumerate((a0, a1, a2, a3)):
        heads[lax.rem(where[0] + j, 4)] = a[...]
    beside = jnp.concatenate([heads[h] for h in range(4)], axis=1)
    parts[...] = beside.reshape(parts.shape)
    for k, out in enumerate((o0, o1, o2, o3)):
        out[...] = parts[lax.rem(where[4] + k, 4)]


def project_kernel(where, a0, a1, a2, a3, out_proj, out, parts):
    width = a0.shape[1]
    for k, a in enumerate((a0, a1, a2, a3)):
        parts[lax.rem(where[4] - k + 4, 4)] = a[...]
    total = mm(parts[0], out_proj[:width, :])
    for h in range(1, 4):
        total = total + mm(parts[h], out_proj[h * width : (h + 1) * width, :])
    out[...] = total.astype(BF)


def query_and_pair(where, query, latent, rope_key, latent_gain, key_up, value_up):
    strip = query.shape[0]
    own = latent.shape[0]
    query_start = (((where[0] * 2 + where[1]) * 4 + where[2]) * 2 + where[3]) * strip

    normed = rms_scale(latent, latent_gain).astype(BF)
    key_cos, key_sin = trig(query_start + where[4] * own + jnp.arange(own, dtype=jnp.int32))
    half = ROPE_DIM // 2
    a = rope_key[:, :half].astype(F32)
    b = rope_key[:, half:].astype(F32)
    both = jnp.concatenate(
        [
            normed,
            (a * key_cos - b * key_sin).astype(BF),
            (a * key_sin + b * key_cos).astype(BF),
        ],
        axis=1,
    )
    near = [both] + [shifted(both, "x", k) for k in range(1, 4)]
    cosine, sine = trig(query_start + jnp.arange(strip, dtype=jnp.int32))
    blocks = call(
        heads_kernel,
        [jax.ShapeDtypeStruct((QK_DIM + KV_ROWS, strip), BF)] * 4,
        "heads",
        near + [key_up, value_up, query, cosine.T, sine.T],
        where,
        [
            pltpu.VMEM((strip, both.shape[1]), BF),
            pltpu.VMEM((4, QK_DIM + KV_ROWS, strip), BF),
        ],
    )
    blocks = [blocks[0]] + [shifted(blocks[k], "zh", k) for k in range(1, 4)]
    mine = jnp.stack([block[QK_DIM:] for block in blocks])
    return blocks, jnp.concatenate([mine, shifted(mine, "zl", 1)], axis=2)


def attend(where, blocks, pair):
    strip = blocks[0].shape[1]
    column = [pair] + [shifted(pair, "y", k) for k in range(1, 4)]
    column = column + [shifted(part, "c", 1) for part in column]
    return call(
        attend_kernel,
        [jax.ShapeDtypeStruct((strip, V_DIM), BF)] * 4,
        "attend",
        blocks + column,
        where,
        [
            pltpu.VMEM((4 * strip, QK_DIM), BF),
            pltpu.VMEM((4 * strip, 128), F32),
            pltpu.VMEM((4 * strip, 128), F32),
        ],
    )


def project(where, parts, out_proj, own):
    strip = parts[0].shape[0]
    parts = [parts[0]] + [shifted(parts[j], "zh", -j) for j in range(1, 4)]
    parts = call(
        spread_kernel,
        [jax.ShapeDtypeStruct((own, 4 * V_DIM), BF)] * 4,
        "spread",
        parts,
        where,
        [pltpu.VMEM((4, strip, V_DIM), BF), pltpu.VMEM((4, own, 4 * V_DIM), BF)],
    )
    parts = [parts[0]] + [shifted(parts[k], "x", k) for k in range(1, 4)]
    return call(
        project_kernel,
        jax.ShapeDtypeStruct((own, out_proj.shape[1]), BF),
        "project",
        parts + [out_proj],
        where,
        [pltpu.VMEM((4, own, 4 * V_DIM), BF)],
    )


def body(
    query,
    latent,
    rope_key,
    latent_gain,
    key_up,
    value_up,
    out_proj,
    tokens,
    moe_gain,
    routes,
    group_prob,
    expert_prob,
    w_gate,
    w_up,
    w_down,
):
    where = jnp.stack([lax.axis_index(n) for n in AXES]).astype(jnp.int32)
    return both_halves(
        where,
        query,
        latent,
        rope_key,
        latent_gain,
        key_up,
        value_up,
        out_proj,
        tokens,
        moe_gain,
        routes,
        group_prob,
        expert_prob,
        w_gate,
        w_up,
        w_down,
    )


def solution(mesh):
    ep, every = EP, AXES
    split = Mesh(mesh.devices.reshape(4, 2, 4, 2, 4), AXES)
    return jax.shard_map(
        body,
        mesh=split,
        in_specs=(
            P(ep, "x"),
            P(every, None),
            P(every, None),
            P(),
            P(None, "x"),
            P(None, "x"),
            P(),
            P(every, None),
            P(),
            P(every, None),
            P(every),
            P(every, None),
            P(ep, None, "x"),
            P(ep, None, "x"),
            P(ep, "x", None),
        ),
        out_specs=(P(every, None), P(every, None)),
        check_vma=False,
    )
```

```python
import jax
import jax.numpy as jnp
from jax import lax
from jax.experimental import pallas as pl
from jax.experimental.pallas import tpu as pltpu
from jax.sharding import Mesh, PartitionSpec as P


NOPE = 64
ROPE_DIM = 32
V_DIM = 64
QK_DIM = NOPE + ROPE_DIM
KV_ROWS = QK_DIM + V_DIM
CAP = 4
BF = jnp.bfloat16
F32 = jnp.float32

epsilon = 1e-06
rope_base = 10000.0
masked_value = -1e30
log2_e = 1.4426950408889634


AXES = ("zh", "zl", "y", "c", "x")
EP = AXES[:4]

SMEM_SPEC = pl.BlockSpec(memory_space=pltpu.SMEM)
VMEM_SPEC = pl.BlockSpec(memory_space=pltpu.VMEM)


def call(kernel, out_shape, arrays, where=None, scratch=(), limit=16 << 20, unplaced=()):
    arrays = [
        a if i in unplaced else pltpu.with_memory_space_constraint(a, pltpu.VMEM)
        for i, a in enumerate(arrays)
    ]
    specs = [VMEM_SPEC] * len(arrays)
    if where is not None:
        arrays, specs = [where] + arrays, [SMEM_SPEC] + specs
    single = not isinstance(out_shape, (list, tuple))
    return pl.pallas_call(
        kernel,
        in_specs=specs,
        out_specs=VMEM_SPEC if single else [VMEM_SPEC] * len(out_shape),
        out_shape=out_shape,
        scratch_shapes=list(scratch),
        compiler_params=pltpu.CompilerParams(vmem_limit_bytes=limit),
    )(*arrays)


def mm(a, b, dims=((1,), (0,))):
    return lax.dot_general(a, b, (dims, ((), ())), preferred_element_type=F32)


def shifted(value, axis, amount):
    n = lax.axis_size(axis)
    return lax.ppermute(value, axis, [(i, (i + amount) % n) for i in range(n)])


def trig(positions):
    half = ROPE_DIM // 2
    inverse = rope_base ** (-2.0 * jnp.arange(half, dtype=F32) / ROPE_DIM)
    angles = positions.astype(F32)[:, None] * inverse[None, :]
    return jnp.cos(angles), jnp.sin(angles)


def rms_scale(values, gain):
    widened = values.astype(F32)
    return widened * lax.rsqrt(jnp.mean(widened * widened, axis=-1, keepdims=True) + epsilon) * gain


def dispatch_kernel(tokens, gain, routes, group_prob, expert_prob, outgoing, shares_out):
    rows = tokens.shape[0]
    experts, cap, width = outgoing.shape
    slots = experts * cap
    normed = rms_scale(tokens[...], gain[...]).astype(BF)
    slot = lax.broadcasted_iota(jnp.int32, (slots, rows), 0)
    expert = slot // cap
    first = routes[0:1, :] == expert
    second = routes[1:2, :] == expert
    named = (first | second).astype(BF)
    before = lax.broadcasted_iota(jnp.int32, (rows, rows), 0) < lax.broadcasted_iota(
        jnp.int32, (rows, rows), 1
    )
    prior = mm(named, before.astype(BF))
    mine = (first | second) & (prior == (slot % cap).astype(F32))
    outgoing[...] = mm(mine.astype(BF), normed).reshape(experts, cap, width).astype(BF)
    probs = expert_prob[...]
    shares = group_prob[...] * probs / jnp.sum(probs, axis=0, keepdims=True)
    weights = jnp.where(first, shares[0:1, :], shares[1:2, :])
    weights = jnp.where(mine, weights, 0.0)
    high = weights.astype(BF)
    shares_out[:, 0:rows] = high
    shares_out[:, rows : 2 * rows] = (weights - high.astype(F32)).astype(BF)


def dispatch(tokens, gain, routes, group_prob, expert_prob, experts):
    rows, width = tokens.shape
    return call(
        dispatch_kernel,
        (
            jax.ShapeDtypeStruct((experts, CAP, width), BF),
            jax.ShapeDtypeStruct((experts * CAP, 2 * rows), BF),
        ),
        [tokens, gain[None, :], routes.T, group_prob[None, :], expert_prob.T],
        unplaced=range(5),
    )


def hidden_kernel(rows_a, rows_b, w_gate, w_up, out):
    half = out.shape[0] // 2
    for at, rows in ((0, rows_a), (half, rows_b)):
        got = rows[...].reshape(half, w_gate.shape[0])
        gate = mm(got, w_gate[...])
        up = mm(got, w_up[...])
        out[at : at + half, :] = (gate / (1.0 + jnp.exp(-gate)) * up).astype(BF)


def hidden_of(rows_a, rows_b, w_gate, w_up):
    shape = jax.ShapeDtypeStruct((2 * rows_a.shape[0] * CAP, w_gate.shape[1]), BF)
    return call(hidden_kernel, shape, [rows_a, rows_b, w_gate, w_up])


def down_kernel(h0, h1, h2, h3, w0, w1, w2, w3, out):
    total = mm(h0[...], w0[...]) + mm(h1[...], w1[...])
    total = total + mm(h2[...], w2[...]) + mm(h3[...], w3[...])
    out[...] = total.reshape(out.shape).astype(BF)


def combine_kernel(returned, shares, out):
    rows = out.shape[0]
    got = returned[...].reshape(shares.shape[0], out.shape[1])
    both = mm(shares[...], got, ((0,), (0,)))
    out[...] = (both[:rows] + both[rows:]).astype(BF)


def both_halves(
    where,
    query,
    latent,
    rope_key,
    latent_gain,
    key_up,
    value_up,
    out_proj,
    tokens,
    moe_gain,
    routes,
    group_prob,
    expert_prob,
    w_gate,
    w_up,
    w_down,
):
    experts = lax.axis_size(EP)
    rows, width = tokens.shape
    w_gate, w_up, w_down = w_gate[0], w_up[0], w_down[0]
    down = [shifted(w_down, "x", k) for k in (-1, 2, 1)]
    outgoing, shares = dispatch(tokens, moe_gain, routes, group_prob, expert_prob, experts)
    arrived = lax.all_to_all(outgoing, EP, split_axis=0, concat_axis=0, tiled=True)
    queries, pair = query_and_pair(where, query, latent, rope_key, latent_gain, key_up, value_up)
    down = [w_down] + down
    half = experts // 2
    a, b = arrived[:half], arrived[half:]
    left_a, right_b = shifted(a, "x", 1), shifted(b, "x", -1)
    left_b, right_a = shifted(b, "x", 1), shifted(a, "x", -1)
    far_a, far_b = shifted(left_a, "x", 1), shifted(right_b, "x", -1)
    parts = attend(where, queries, pair)
    hidden = [
        hidden_of(a, b, w_gate, w_up),
        shifted(hidden_of(left_a, left_b, w_gate, w_up), "x", -1),
        shifted(hidden_of(far_a, far_b, w_gate, w_up), "x", 2),
        shifted(hidden_of(right_a, right_b, w_gate, w_up), "x", 1),
    ]
    shape = jax.ShapeDtypeStruct((experts, CAP, width), BF)
    result = call(down_kernel, shape, hidden + down)
    returned = lax.all_to_all(result, EP, split_axis=0, concat_axis=0, tiled=True)
    mixed = project(where, parts, out_proj, latent.shape[0])
    shape = jax.ShapeDtypeStruct((rows, width), BF)
    return mixed, call(combine_kernel, shape, [returned, shares])


def heads_kernel(
    where, l0, l1, l2, l3, key_up, value_up, query, cosine, sine, o0, o1, o2, o3, strip_s, heads
):
    latent = key_up.shape[0]
    own = l0.shape[0]
    count = heads.shape[0]
    half = ROPE_DIM // 2
    turned = query[...].astype(F32).T
    for h in range(count):
        at = h * QK_DIM
        a = turned[at + NOPE : at + NOPE + half]
        b = turned[at + NOPE + half : at + QK_DIM]
        heads[h, :NOPE, :] = turned[at : at + NOPE].astype(BF)
        heads[h, NOPE : NOPE + half, :] = (a * cosine[...] - b * sine[...]).astype(BF)
        heads[h, NOPE + half : QK_DIM, :] = (a * sine[...] + b * cosine[...]).astype(BF)
    for k, block in enumerate((l0, l1, l2, l3)):
        strip_s[k * own : (k + 1) * own, :] = block[...]
    got = strip_s[:, :latent]
    keys = mm(key_up[...], got, ((0,), (1,))).astype(BF)
    values = mm(value_up[...], got, ((0,), (1,))).astype(BF)
    eye = (
        lax.broadcasted_iota(jnp.int32, (ROPE_DIM, ROPE_DIM), 0)
        == lax.broadcasted_iota(jnp.int32, (ROPE_DIM, ROPE_DIM), 1)
    ).astype(BF)
    rope = mm(eye, strip_s[:, latent:], ((1,), (1,))).astype(BF)
    for h in range(count):
        heads[h, QK_DIM : QK_DIM + NOPE, :] = keys[h * NOPE : (h + 1) * NOPE]
        heads[h, QK_DIM + NOPE : 2 * QK_DIM, :] = rope
        heads[h, 2 * QK_DIM :, :] = values[h * V_DIM : (h + 1) * V_DIM]
    for k, out in enumerate((o0, o1, o2, o3)):
        out[...] = heads[lax.rem(where[0] + k, 4)]


def attend_kernel(where, q0, q1, q2, q3, *refs):
    blocks, (o0, o1, o2, o3, q_s, top_s, acc_s) = refs[:8], refs[8:]
    zh, zl, y, c, x = (where[i] for i in range(5))
    strip = q0.shape[1]
    span = blocks[0].shape[2]
    factor = QK_DIM ** (-0.5) * log2_e
    for j, q in enumerate((q0, q1, q2, q3)):
        at = pl.multiple_of(lax.rem(zh - j + 4, 4) * strip, strip)
        q_s[pl.ds(at, strip), :] = q[:QK_DIM, :].astype(F32).T.astype(BF)
    top_s[...] = jnp.full(top_s.shape, masked_value, F32)
    acc_s[...] = jnp.zeros(acc_s.shape, F32)

    col = lax.broadcasted_iota(jnp.int32, (1, span), 1)
    col_zl = jnp.bitwise_xor(zl, col // strip)
    within = col % strip
    col_x = ((x - within // 32 + 4) % 4) * 32 + within % 32
    query_at = (zl * 8 + y * 2 + c) * strip + lax.broadcasted_iota(jnp.int32, (strip, 1), 0)
    ones = jnp.ones((V_DIM, span), BF)

    def advance(rows, parts, masks):
        q = q_s[rows, :]
        old = top_s[rows, :]
        scores = [mm(q, part[:QK_DIM, :]) for part in parts]
        if masks is not None:
            scores = [jnp.where(m, s, masked_value) for m, s in zip(masks, scores)]
        peak = scores[0]
        for s in scores[1:]:
            peak = jnp.maximum(peak, s)
        new = jnp.maximum(old, jnp.max(peak, axis=1, keepdims=True))
        top_s[rows, :] = new
        base = new[:, :1]
        total = acc_s[rows, :] * jnp.exp2((old - new) * factor)
        for s, part in zip(scores, parts):
            raised = jnp.exp2((s - base) * factor).astype(BF)
            extended = jnp.concatenate([part[QK_DIM:, :], ones], axis=0)
            total = total + mm(raised, extended, ((1,), (1,)))
        acc_s[rows, :] = total

    for m in range(2):
        group = blocks[4 * m : 4 * m + 4]
        masks = []
        for k in range(4):
            key_y = lax.rem(y - k + 4, 4)
            key_at = (col_zl * 8 + key_y * 2 + jnp.bitwise_xor(c, m)) * strip + col_x
            masks.append(key_at <= query_at)
        for g in range(4):
            from_zh = lax.rem(zh - g + 4, 4)
            parts = [block[from_zh] for block in group]
            advance(slice(g * strip, (g + 1) * strip), parts, masks)
            if g < 3:
                advance(slice((g + 1) * strip, 4 * strip), parts, None)
    for j, out in enumerate((o0, o1, o2, o3)):
        at = pl.multiple_of(lax.rem(zh - j + 4, 4) * strip, strip)
        total = acc_s[pl.ds(at, strip), :]
        out[...] = (total[:, :V_DIM] / total[:, V_DIM:]).astype(BF)


def spread_kernel(where, a0, a1, a2, a3, o0, o1, o2, o3, heads, parts):
    for j, a in enumerate((a0, a1, a2, a3)):
        heads[lax.rem(where[0] + j, 4)] = a[...]
    beside = jnp.concatenate([heads[h] for h in range(4)], axis=1)
    parts[...] = beside.reshape(parts.shape)
    for k, out in enumerate((o0, o1, o2, o3)):
        out[...] = parts[lax.rem(where[4] + k, 4)]


def project_kernel(where, a0, a1, a2, a3, out_proj, out, parts):
    width = a0.shape[1]
    for k, a in enumerate((a0, a1, a2, a3)):
        parts[lax.rem(where[4] - k + 4, 4)] = a[...]
    total = mm(parts[0], out_proj[:width, :])
    for h in range(1, 4):
        total = total + mm(parts[h], out_proj[h * width : (h + 1) * width, :])
    out[...] = total.astype(BF)


def query_and_pair(where, query, latent, rope_key, latent_gain, key_up, value_up):
    strip = query.shape[0]
    own = latent.shape[0]
    query_start = (((where[0] * 2 + where[1]) * 4 + where[2]) * 2 + where[3]) * strip

    normed = rms_scale(latent, latent_gain).astype(BF)
    key_cos, key_sin = trig(query_start + where[4] * own + jnp.arange(own, dtype=jnp.int32))
    half = ROPE_DIM // 2
    a = rope_key[:, :half].astype(F32)
    b = rope_key[:, half:].astype(F32)
    both = jnp.concatenate(
        [
            normed,
            (a * key_cos - b * key_sin).astype(BF),
            (a * key_sin + b * key_cos).astype(BF),
        ],
        axis=1,
    )
    near = [both] + [shifted(both, "x", k) for k in range(1, 4)]
    cosine, sine = trig(query_start + jnp.arange(strip, dtype=jnp.int32))
    blocks = call(
        heads_kernel,
        [jax.ShapeDtypeStruct((QK_DIM + KV_ROWS, strip), BF)] * 4,
        near + [key_up, value_up, query, cosine.T, sine.T],
        where,
        [
            pltpu.VMEM((strip, both.shape[1]), BF),
            pltpu.VMEM((4, QK_DIM + KV_ROWS, strip), BF),
        ],
        unplaced=range(4, 9),
    )
    blocks = [blocks[0]] + [shifted(blocks[k], "zh", k) for k in range(1, 4)]
    mine = jnp.stack([block[QK_DIM:] for block in blocks])
    return blocks, jnp.concatenate([mine, shifted(mine, "zl", 1)], axis=2)


def attend(where, blocks, pair):
    strip = blocks[0].shape[1]
    column = [pair] + [shifted(pair, "y", k) for k in range(1, 4)]
    column = column + [shifted(part, "c", 1) for part in column]
    return call(
        attend_kernel,
        [jax.ShapeDtypeStruct((strip, V_DIM), BF)] * 4,
        blocks + column,
        where,
        [
            pltpu.VMEM((4 * strip, QK_DIM), BF),
            pltpu.VMEM((4 * strip, 128), F32),
            pltpu.VMEM((4 * strip, 128), F32),
        ],
    )


def project(where, parts, out_proj, own):
    strip = parts[0].shape[0]
    parts = [parts[0]] + [shifted(parts[j], "zh", -j) for j in range(1, 4)]
    parts = call(
        spread_kernel,
        [jax.ShapeDtypeStruct((own, 4 * V_DIM), BF)] * 4,
        parts,
        where,
        [pltpu.VMEM((4, strip, V_DIM), BF), pltpu.VMEM((4, own, 4 * V_DIM), BF)],
    )
    parts = [parts[0]] + [shifted(parts[k], "x", k) for k in range(1, 4)]
    return call(
        project_kernel,
        jax.ShapeDtypeStruct((own, out_proj.shape[1]), BF),
        parts + [out_proj],
        where,
        [pltpu.VMEM((4, own, 4 * V_DIM), BF)],
    )


def body(
    query,
    latent,
    rope_key,
    latent_gain,
    key_up,
    value_up,
    out_proj,
    tokens,
    moe_gain,
    routes,
    group_prob,
    expert_prob,
    w_gate,
    w_up,
    w_down,
):
    where = jnp.stack([lax.axis_index(n) for n in AXES]).astype(jnp.int32)
    return both_halves(
        where,
        query,
        latent,
        rope_key,
        latent_gain,
        key_up,
        value_up,
        out_proj,
        tokens,
        moe_gain,
        routes,
        group_prob,
        expert_prob,
        w_gate,
        w_up,
        w_down,
    )


def solution(mesh):
    ep, every = EP, AXES
    split = Mesh(mesh.devices.reshape(4, 2, 4, 2, 4), AXES)
    return jax.shard_map(
        body,
        mesh=split,
        in_specs=(
            P(ep, "x"),
            P(every, None),
            P(every, None),
            P(),
            P(None, "x"),
            P(None, "x"),
            P(),
            P(every, None),
            P(),
            P(every, None),
            P(every),
            P(every, None),
            P(ep, None, "x"),
            P(ep, None, "x"),
            P(ep, "x", None),
        ),
        out_specs=(P(every, None), P(every, None)),
        check_vma=False,
    )
```

```python
import jax
import jax.numpy as jnp
from jax import lax
from jax.experimental import pallas as pl
from jax.experimental.pallas import tpu as pltpu
from jax.sharding import Mesh, PartitionSpec as P


NOPE = 64
ROPE_DIM = 32
V_DIM = 64
QK_DIM = NOPE + ROPE_DIM
KV_ROWS = QK_DIM + V_DIM
CAP = 4
BF = jnp.bfloat16
F32 = jnp.float32

epsilon = 1e-06
rope_base = 10000.0
masked_value = -1e30
log2_e = 1.4426950408889634


AXES = ("zh", "zl", "y", "c", "x")
EP = AXES[:4]

SMEM_SPEC = pl.BlockSpec(memory_space=pltpu.SMEM)
VMEM_SPEC = pl.BlockSpec(memory_space=pltpu.VMEM)


def call(kernel, out_shape, arrays, where=None, scratch=(), limit=16 << 20, unplaced=(), place=True):
    arrays = [
        pltpu.with_memory_space_constraint(a, pltpu.HBM if i in unplaced else pltpu.VMEM)
        for i, a in enumerate(arrays)
    ]
    specs = [VMEM_SPEC] * len(arrays)
    if where is not None:
        arrays, specs = [where] + arrays, [SMEM_SPEC] + specs
    single = not isinstance(out_shape, (list, tuple))
    if place:
        if single:
            out_shape = pltpu.VMEM(out_shape.shape, out_shape.dtype)
        else:
            out_shape = [pltpu.VMEM(s.shape, s.dtype) for s in out_shape]
    return pl.pallas_call(
        kernel,
        in_specs=specs,
        out_specs=VMEM_SPEC if single else [VMEM_SPEC] * len(out_shape),
        out_shape=out_shape,
        scratch_shapes=list(scratch),
        compiler_params=pltpu.CompilerParams(vmem_limit_bytes=limit),
    )(*arrays)


def mm(a, b, dims=((1,), (0,))):
    return lax.dot_general(a, b, (dims, ((), ())), preferred_element_type=F32)


def shifted(value, axis, amount):
    n = lax.axis_size(axis)
    return lax.ppermute(value, axis, [(i, (i + amount) % n) for i in range(n)])


def trig(positions):
    half = ROPE_DIM // 2
    inverse = rope_base ** (-2.0 * jnp.arange(half, dtype=F32) / ROPE_DIM)
    angles = positions.astype(F32)[:, None] * inverse[None, :]
    return jnp.cos(angles), jnp.sin(angles)


def rms_scale(values, gain):
    widened = values.astype(F32)
    return widened * lax.rsqrt(jnp.mean(widened * widened, axis=-1, keepdims=True) + epsilon) * gain


def dispatch_kernel(tokens, gain, routes, group_prob, expert_prob, outgoing, shares_out):
    rows = tokens.shape[0]
    experts, cap, width = outgoing.shape
    slots = experts * cap
    normed = rms_scale(tokens[...], gain[...]).astype(BF)
    slot = lax.broadcasted_iota(jnp.int32, (slots, rows), 0)
    expert = slot // cap
    first = routes[0:1, :] == expert
    second = routes[1:2, :] == expert
    named = (first | second).astype(BF)
    before = lax.broadcasted_iota(jnp.int32, (rows, rows), 0) < lax.broadcasted_iota(
        jnp.int32, (rows, rows), 1
    )
    prior = mm(named, before.astype(BF))
    mine = (first | second) & (prior == (slot % cap).astype(F32))
    outgoing[...] = mm(mine.astype(BF), normed).reshape(experts, cap, width).astype(BF)
    probs = expert_prob[...]
    shares = group_prob[...] * probs / jnp.sum(probs, axis=0, keepdims=True)
    weights = jnp.where(first, shares[0:1, :], shares[1:2, :])
    weights = jnp.where(mine, weights, 0.0)
    high = weights.astype(BF)
    shares_out[:, 0:rows] = high
    shares_out[:, rows : 2 * rows] = (weights - high.astype(F32)).astype(BF)


def dispatch(tokens, gain, routes, group_prob, expert_prob, experts):
    rows, width = tokens.shape
    return call(
        dispatch_kernel,
        (
            jax.ShapeDtypeStruct((experts, CAP, width), BF),
            jax.ShapeDtypeStruct((experts * CAP, 2 * rows), BF),
        ),
        [tokens, gain[None, :], routes.T, group_prob[None, :], expert_prob.T],
        unplaced=range(5),
    )


def hidden_kernel(rows_a, rows_b, w_gate, w_up, out):
    half = out.shape[0] // 2
    for at, rows in ((0, rows_a), (half, rows_b)):
        got = rows[...].reshape(half, w_gate.shape[0])
        gate = mm(got, w_gate[...])
        up = mm(got, w_up[...])
        out[at : at + half, :] = (gate / (1.0 + jnp.exp(-gate)) * up).astype(BF)


def hidden_of(rows_a, rows_b, w_gate, w_up):
    shape = jax.ShapeDtypeStruct((2 * rows_a.shape[0] * CAP, w_gate.shape[1]), BF)
    return call(hidden_kernel, shape, [rows_a, rows_b, w_gate, w_up])


def down_kernel(h0, h1, h2, h3, w0, w1, w2a, w2b, w3, out):
    half = w2a.shape[0]
    total = mm(h0[...], w0[...]) + mm(h1[...], w1[...]) + mm(h3[...], w3[...])
    total = total + mm(h2[:, :half], w2a[...]) + mm(h2[:, half:], w2b[...])
    out[...] = total.reshape(out.shape).astype(BF)


def combine_kernel(returned, shares, out):
    rows = out.shape[0]
    got = returned[...].reshape(shares.shape[0], out.shape[1])
    both = mm(shares[...], got, ((0,), (0,)))
    out[...] = (both[:rows] + both[rows:]).astype(BF)


def both_halves(
    where,
    query,
    latent,
    rope_key,
    latent_gain,
    key_up,
    value_up,
    out_proj,
    tokens,
    moe_gain,
    routes,
    group_prob,
    expert_prob,
    w_gate,
    w_up,
    w_down,
):
    experts = lax.axis_size(EP)
    rows, width = tokens.shape
    w_gate, w_up, w_down = w_gate[0], w_up[0], w_down[0]
    down_left, down_right = shifted(w_down, "x", 1), shifted(w_down, "x", -1)
    units = w_down.shape[0] // 2
    cut_a, cut_b = down_left[:units], down_right[units:]
    down_far = [shifted(cut_a, "x", 1), shifted(cut_b, "x", -1)]
    outgoing, shares = dispatch(tokens, moe_gain, routes, group_prob, expert_prob, experts)
    arrived = lax.all_to_all(outgoing, EP, split_axis=0, concat_axis=0, tiled=True)
    queries, pair = query_and_pair(where, query, latent, rope_key, latent_gain, key_up, value_up)
    half = experts // 2
    a, b = arrived[:half], arrived[half:]
    left_a, right_b = shifted(a, "x", 1), shifted(b, "x", -1)
    left_b, right_a = shifted(b, "x", 1), shifted(a, "x", -1)
    far_a, far_b = shifted(left_a, "x", 1), shifted(right_b, "x", -1)
    parts = attend(where, queries, pair)
    hidden = [
        hidden_of(a, b, w_gate, w_up),
        shifted(hidden_of(left_a, left_b, w_gate, w_up), "x", -1),
        shifted(hidden_of(far_a, far_b, w_gate, w_up), "x", 2),
        shifted(hidden_of(right_a, right_b, w_gate, w_up), "x", 1),
    ]
    shape = jax.ShapeDtypeStruct((experts, CAP, width), BF)
    down = [w_down, down_right] + down_far + [down_left]
    result = call(down_kernel, shape, hidden + down)
    returned = lax.all_to_all(result, EP, split_axis=0, concat_axis=0, tiled=True)
    mixed = project(parts, out_proj)
    shape = jax.ShapeDtypeStruct((rows, width), BF)
    return mixed, call(combine_kernel, shape, [returned, shares], place=False)


def latent_kernel(latent, gain, rope_key, cosine, sine, out):
    width = latent.shape[1]
    half = ROPE_DIM // 2
    out[:, :width] = rms_scale(latent[...], gain[...]).astype(BF)
    rope = rope_key[...].astype(F32)
    crossed = jnp.concatenate([-rope[:, half:], rope[:, :half]], axis=1)
    out[:, width:] = (rope * cosine[...] + crossed * sine[...]).astype(BF)


def heads_kernel(
    where, l0, l1, l2, l3, key_up, value_up, query, cosine, sine, o0, o1, o2, o3, strip_s, heads
):
    latent = key_up.shape[0]
    own = l0.shape[0]
    count = heads.shape[0]
    half = ROPE_DIM // 2
    turned = query[...].astype(F32).T
    for h in range(count):
        at = h * QK_DIM
        a = turned[at + NOPE : at + NOPE + half]
        b = turned[at + NOPE + half : at + QK_DIM]
        heads[h, :NOPE, :] = turned[at : at + NOPE].astype(BF)
        heads[h, NOPE : NOPE + half, :] = (a * cosine[...] - b * sine[...]).astype(BF)
        heads[h, NOPE + half : QK_DIM, :] = (a * sine[...] + b * cosine[...]).astype(BF)
    for k, block in enumerate((l0, l1, l2, l3)):
        strip_s[k * own : (k + 1) * own, :] = block[...]
    got = strip_s[:, :latent]
    keys = mm(key_up[...], got, ((0,), (1,))).astype(BF)
    values = mm(value_up[...], got, ((0,), (1,))).astype(BF)
    eye = (
        lax.broadcasted_iota(jnp.int32, (ROPE_DIM, ROPE_DIM), 0)
        == lax.broadcasted_iota(jnp.int32, (ROPE_DIM, ROPE_DIM), 1)
    ).astype(BF)
    rope = mm(eye, strip_s[:, latent:], ((1,), (1,))).astype(BF)
    for h in range(count):
        heads[h, QK_DIM : QK_DIM + NOPE, :] = keys[h * NOPE : (h + 1) * NOPE]
        heads[h, QK_DIM + NOPE : 2 * QK_DIM, :] = rope
        heads[h, 2 * QK_DIM :, :] = values[h * V_DIM : (h + 1) * V_DIM]
    for k, out in enumerate((o0, o1, o2, o3)):
        out[...] = heads[lax.rem(where[0] + k, 4)]


def stack_kernel(b0, b1, b2, b3, out):
    for j, block in enumerate((b0, b1, b2, b3)):
        out[j] = block[QK_DIM:, :]


def attend_kernel(where, q0, q1, q2, q3, *refs):
    blocks, (out, q_s, top_s, acc_s) = refs[:8], refs[8:]
    zh, zl, y, c, x = (where[i] for i in range(5))
    strip = q0.shape[1]
    span = blocks[0].shape[2]
    factor = QK_DIM ** (-0.5) * log2_e
    for j, q in enumerate((q0, q1, q2, q3)):
        at = pl.multiple_of(lax.rem(zh - j + 4, 4) * strip, strip)
        q_s[pl.ds(at, strip), :] = q[:QK_DIM, :].astype(F32).T.astype(BF)
    top_s[...] = jnp.full(top_s.shape, masked_value, F32)
    acc_s[...] = jnp.zeros(acc_s.shape, F32)

    col = lax.broadcasted_iota(jnp.int32, (1, span), 1)
    col_zl = jnp.bitwise_xor(zl, col // strip)
    within = col % strip
    col_x = ((x - within // 32 + 4) % 4) * 32 + within % 32
    query_at = (zl * 8 + y * 2 + c) * strip + lax.broadcasted_iota(jnp.int32, (strip, 1), 0)
    ones = jnp.ones((V_DIM, span), BF)

    def advance(rows, parts, masks):
        q = q_s[rows, :]
        old = top_s[rows, :]
        scores = [mm(q, part[:QK_DIM, :]) for part in parts]
        if masks is not None:
            scores = [jnp.where(m, s, masked_value) for m, s in zip(masks, scores)]
        peak = scores[0]
        for s in scores[1:]:
            peak = jnp.maximum(peak, s)
        new = jnp.maximum(old, jnp.max(peak, axis=1, keepdims=True))
        top_s[rows, :] = new
        base = new[:, :1]
        total = acc_s[rows, :] * jnp.exp2((old - new) * factor)
        for s, part in zip(scores, parts):
            raised = jnp.exp2((s - base) * factor).astype(BF)
            extended = jnp.concatenate([part[QK_DIM:, :], ones], axis=0)
            total = total + mm(raised, extended, ((1,), (1,)))
        acc_s[rows, :] = total

    for m in range(2):
        group = blocks[4 * m : 4 * m + 4]
        masks = []
        for k in range(4):
            key_y = lax.rem(y - k + 4, 4)
            key_at = (col_zl * 8 + key_y * 2 + jnp.bitwise_xor(c, m)) * strip + col_x
            masks.append(key_at <= query_at)
        for g in range(4):
            from_zh = lax.rem(zh - g + 4, 4)
            parts = [block[from_zh] for block in group]
            advance(slice(g * strip, (g + 1) * strip), parts, masks)
            if g < 3:
                advance(slice((g + 1) * strip, 4 * strip), parts, None)
    total = acc_s[...]
    divided = total / jnp.concatenate([total[:, V_DIM:], total[:, V_DIM:]], axis=1)
    out[...] = divided.reshape(out.shape).astype(BF)


def project_kernel(parts, out_proj, out):
    order = [zh * 4 + x for x in range(4) for zh in range(4)]
    beside = jnp.concatenate([parts[i, :, :V_DIM] for i in order], axis=1)
    out[...] = mm(beside, out_proj[...]).astype(BF)


def query_and_pair(where, query, latent, rope_key, latent_gain, key_up, value_up):
    strip = query.shape[0]
    own = latent.shape[0]
    query_start = (((where[0] * 2 + where[1]) * 4 + where[2]) * 2 + where[3]) * strip

    key_cos, key_sin = trig(query_start + where[4] * own + jnp.arange(own, dtype=jnp.int32))
    both = call(
        latent_kernel,
        jax.ShapeDtypeStruct((own, latent.shape[1] + ROPE_DIM), BF),
        [
            latent,
            latent_gain[None, :],
            rope_key,
            jnp.concatenate([key_cos, key_cos], axis=1),
            jnp.concatenate([key_sin, key_sin], axis=1),
        ],
        unplaced=range(3),
    )
    near = [both] + [shifted(both, "x", k) for k in range(1, 4)]
    cosine, sine = trig(query_start + jnp.arange(strip, dtype=jnp.int32))
    blocks = call(
        heads_kernel,
        [jax.ShapeDtypeStruct((QK_DIM + KV_ROWS, strip), BF)] * 4,
        near + [key_up, value_up, query, cosine.T, sine.T],
        where,
        scratch=[
            pltpu.VMEM((strip, both.shape[1]), BF),
            pltpu.VMEM((4, QK_DIM + KV_ROWS, strip), BF),
        ],
        unplaced=range(4, 7),
    )
    blocks = [blocks[0]] + [shifted(blocks[k], "zh", k) for k in range(1, 4)]
    shape = jax.ShapeDtypeStruct((4, KV_ROWS, strip), BF)
    mine = call(stack_kernel, shape, blocks)
    return blocks, jnp.concatenate([mine, shifted(mine, "zl", 1)], axis=2)


def attend(where, blocks, pair):
    strip = blocks[0].shape[1]
    column = [pair] + [shifted(pair, "y", k) for k in range(1, 4)]
    column = column + [shifted(part, "c", 1) for part in column]
    parts = call(
        attend_kernel,
        jax.ShapeDtypeStruct((16, strip // 4, 2 * V_DIM), BF),
        blocks + column,
        where,
        [
            pltpu.VMEM((4 * strip, QK_DIM), BF),
            pltpu.VMEM((4 * strip, 128), F32),
            pltpu.VMEM((4 * strip, 128), F32),
        ],
    )
    return lax.all_to_all(parts, ("zh", "x"), split_axis=0, concat_axis=0, tiled=True)


def project(parts, out_proj):
    shape = jax.ShapeDtypeStruct((parts.shape[1], out_proj.shape[1]), BF)
    return call(project_kernel, shape, [parts, out_proj], place=False)


def body(
    query,
    latent,
    rope_key,
    latent_gain,
    key_up,
    value_up,
    out_proj,
    tokens,
    moe_gain,
    routes,
    group_prob,
    expert_prob,
    w_gate,
    w_up,
    w_down,
):
    where = jnp.stack([lax.axis_index(n) for n in AXES]).astype(jnp.int32)
    return both_halves(
        where,
        query,
        latent,
        rope_key,
        latent_gain,
        key_up,
        value_up,
        out_proj,
        tokens,
        moe_gain,
        routes,
        group_prob,
        expert_prob,
        w_gate,
        w_up,
        w_down,
    )


def solution(mesh):
    ep, every = EP, AXES
    split = Mesh(mesh.devices.reshape(4, 2, 4, 2, 4), AXES)
    return jax.shard_map(
        body,
        mesh=split,
        in_specs=(
            P(ep, "x"),
            P(every, None),
            P(every, None),
            P(),
            P(None, "x"),
            P(None, "x"),
            P(),
            P(every, None),
            P(),
            P(every, None),
            P(every),
            P(every, None),
            P(ep, None, "x"),
            P(ep, None, "x"),
            P(ep, "x", None),
        ),
        out_specs=(P(every, None), P(every, None)),
        check_vma=False,
    )
```

```python
import jax
import jax.numpy as jnp
from jax import lax
from jax.experimental import pallas as pl
from jax.experimental.pallas import tpu as pltpu
from jax.sharding import Mesh, PartitionSpec as P


NOPE = 64
ROPE_DIM = 32
V_DIM = 64
QK_DIM = NOPE + ROPE_DIM
KV_ROWS = QK_DIM + V_DIM
CAP = 4
BF = jnp.bfloat16
F32 = jnp.float32

epsilon = 1e-06
rope_base = 10000.0
masked_value = -1e30
log2_e = 1.4426950408889634


AXES = ("zh", "zl", "y", "c", "x")
EP = AXES[:4]

SMEM_SPEC = pl.BlockSpec(memory_space=pltpu.SMEM)
VMEM_SPEC = pl.BlockSpec(memory_space=pltpu.VMEM)


def call(kernel, out_shape, arrays, where=None, scratch=(), limit=16 << 20, unplaced=(), place=True):
    arrays = [
        pltpu.with_memory_space_constraint(a, pltpu.HBM if i in unplaced else pltpu.VMEM)
        for i, a in enumerate(arrays)
    ]
    specs = [VMEM_SPEC] * len(arrays)
    if where is not None:
        arrays, specs = [where] + arrays, [SMEM_SPEC] + specs
    single = not isinstance(out_shape, (list, tuple))
    if place:
        if single:
            out_shape = pltpu.VMEM(out_shape.shape, out_shape.dtype)
        else:
            out_shape = [pltpu.VMEM(s.shape, s.dtype) for s in out_shape]
    return pl.pallas_call(
        kernel,
        in_specs=specs,
        out_specs=VMEM_SPEC if single else [VMEM_SPEC] * len(out_shape),
        out_shape=out_shape,
        scratch_shapes=list(scratch),
        compiler_params=pltpu.CompilerParams(vmem_limit_bytes=limit),
    )(*arrays)


def mm(a, b, dims=((1,), (0,))):
    return lax.dot_general(a, b, (dims, ((), ())), preferred_element_type=F32)


def shifted(value, axis, amount):
    n = lax.axis_size(axis)
    return lax.ppermute(value, axis, [(i, (i + amount) % n) for i in range(n)])


def trig(positions):
    half = ROPE_DIM // 2
    inverse = rope_base ** (-2.0 * jnp.arange(half, dtype=F32) / ROPE_DIM)
    angles = positions.astype(F32)[:, None] * inverse[None, :]
    return jnp.cos(angles), jnp.sin(angles)


def rms_scale(values, gain):
    widened = values.astype(F32)
    return widened * lax.rsqrt(jnp.mean(widened * widened, axis=-1, keepdims=True) + epsilon) * gain


def dispatch_kernel(tokens, gain, routes, group_prob, expert_prob, first_out, second_out, shares_out):
    rows = tokens.shape[0]
    experts, cap, width = first_out.shape
    slots = experts * cap
    normed = rms_scale(tokens[...], gain[...]).astype(BF)
    slot = lax.broadcasted_iota(jnp.int32, (slots, rows), 0)
    expert = slot // cap
    first = routes[0:1, :] == expert
    second = routes[1:2, :] == expert
    named = (first | second).astype(BF)
    before = lax.broadcasted_iota(jnp.int32, (rows, rows), 0) < lax.broadcasted_iota(
        jnp.int32, (rows, rows), 1
    )
    prior = mm(named, before.astype(BF))
    probs = expert_prob[...]
    shares = group_prob[...] * probs / jnp.sum(probs, axis=0, keepdims=True)
    weights = jnp.where(first, shares[0:1, :], shares[1:2, :])
    for chunk, out in enumerate((first_out, second_out)):
        mine = (first | second) & (prior == (chunk * cap + slot % cap).astype(F32))
        out[...] = mm(mine.astype(BF), normed).reshape(experts, cap, width).astype(BF)
        chosen = jnp.where(mine, weights, 0.0)
        high = chosen.astype(BF)
        at = slice(chunk * slots, (chunk + 1) * slots)
        shares_out[at, 0:rows] = high
        shares_out[at, rows : 2 * rows] = (chosen - high.astype(F32)).astype(BF)


def dispatch(tokens, gain, routes, group_prob, expert_prob, experts):
    rows, width = tokens.shape
    chunk = jax.ShapeDtypeStruct((experts, CAP // 2, width), BF)
    return call(
        dispatch_kernel,
        (chunk, chunk, jax.ShapeDtypeStruct((experts * CAP, 2 * rows), BF)),
        [tokens, gain[None, :], routes.T, group_prob[None, :], expert_prob.T],
        unplaced=range(5),
    )


def silu_product(rows, w_gate, w_up):
    gate = mm(rows, w_gate[...])
    return (gate / (1.0 + jnp.exp(-gate)) * mm(rows, w_up[...])).astype(BF)


def sides_kernel(left, right, w_gate, w_up, left_out, right_out):
    shape = (left_out.shape[0], w_gate.shape[0])
    left_out[...] = silu_product(left[...].reshape(shape), w_gate, w_up)
    right_out[...] = silu_product(right[...].reshape(shape), w_gate, w_up)


def far_kernel(far_a, far_b, w_gate, w_up, far_out):
    half = far_out.shape[0] // 2
    shape = (half, w_gate.shape[0])
    far_out[:half, :] = silu_product(far_a[...].reshape(shape), w_gate, w_up)
    far_out[half:, :] = silu_product(far_b[...].reshape(shape), w_gate, w_up)


def own_kernel(own, w_gate, w_up, out):
    out[...] = silu_product(own[...].reshape(out.shape[0], w_gate.shape[0]), w_gate, w_up)


def down_kernel(h0, h1, h2, h3, w0, w1, w2a, w2b, w3, out):
    half = w2a.shape[0]
    total = mm(h0[...], w0[...]) + mm(h1[...], w1[...]) + mm(h3[...], w3[...])
    total = total + mm(h2[:, :half], w2a[...]) + mm(h2[:, half:], w2b[...])
    out[...] = total.reshape(out.shape).astype(BF)


def combine_kernel(first, second, shares, out):
    rows, width = out.shape
    half = shares.shape[0] // 2
    both = mm(shares[:half, :], first[...].reshape(half, width), ((0,), (0,)))
    both = both + mm(shares[half:, :], second[...].reshape(half, width), ((0,), (0,)))
    out[...] = (both[:rows] + both[rows:]).astype(BF)


def swapped(value):
    return lax.all_to_all(value, EP, split_axis=0, concat_axis=0, tiled=True)


def expert_chunk(arrived, w_gate, w_up, down):
    experts, cap, width = arrived.shape
    half = experts // 2
    left = shifted(arrived, "x", 1)
    right = shifted(arrived, "x", -1)
    far_a = shifted(left[:half], "x", 1)
    far_b = shifted(right[half:], "x", -1)
    shape = jax.ShapeDtypeStruct((experts * cap, w_gate.shape[1]), BF)
    weights = [w_gate, w_up]
    left, right = call(sides_kernel, [shape] * 2, [left, right] + weights)
    far = call(far_kernel, shape, [far_a, far_b] + weights)
    hidden = [
        call(own_kernel, shape, [arrived] + weights),
        shifted(left, "x", -1),
        shifted(far, "x", 2),
        shifted(right, "x", 1),
    ]
    shape = jax.ShapeDtypeStruct((experts, cap, width), BF)
    return swapped(call(down_kernel, shape, hidden + down))


def latent_kernel(latent, gain, rope_key, cosine, sine, out):
    width = latent.shape[1]
    half = ROPE_DIM // 2
    out[:, :width] = rms_scale(latent[...], gain[...]).astype(BF)
    rope = rope_key[...].astype(F32)
    crossed = jnp.concatenate([-rope[:, half:], rope[:, :half]], axis=1)
    out[:, width:] = (rope * cosine[...] + crossed * sine[...]).astype(BF)


def heads_kernel(
    where, l0, l1, l2, l3, key_up, value_up, query, cosine, sine, o0, o1, o2, o3, strip_s, heads
):
    latent = key_up.shape[0]
    own = l0.shape[0]
    count = heads.shape[0]
    half = ROPE_DIM // 2
    turned = query[...].astype(F32).T
    for h in range(count):
        at = h * QK_DIM
        a = turned[at + NOPE : at + NOPE + half]
        b = turned[at + NOPE + half : at + QK_DIM]
        heads[h, :NOPE, :] = turned[at : at + NOPE].astype(BF)
        heads[h, NOPE : NOPE + half, :] = (a * cosine[...] - b * sine[...]).astype(BF)
        heads[h, NOPE + half : QK_DIM, :] = (a * sine[...] + b * cosine[...]).astype(BF)
    for k, block in enumerate((l0, l1, l2, l3)):
        strip_s[k * own : (k + 1) * own, :] = block[...]
    got = strip_s[:, :latent]
    keys = mm(key_up[...], got, ((0,), (1,))).astype(BF)
    values = mm(value_up[...], got, ((0,), (1,))).astype(BF)
    eye = (
        lax.broadcasted_iota(jnp.int32, (ROPE_DIM, ROPE_DIM), 0)
        == lax.broadcasted_iota(jnp.int32, (ROPE_DIM, ROPE_DIM), 1)
    ).astype(BF)
    rope = mm(eye, strip_s[:, latent:], ((1,), (1,))).astype(BF)
    for h in range(count):
        heads[h, QK_DIM : QK_DIM + NOPE, :] = keys[h * NOPE : (h + 1) * NOPE]
        heads[h, QK_DIM + NOPE : 2 * QK_DIM, :] = rope
        heads[h, 2 * QK_DIM :, :] = values[h * V_DIM : (h + 1) * V_DIM]
    for k, out in enumerate((o0, o1, o2, o3)):
        out[...] = heads[lax.rem(where[0] + k, 4)]


def stack_kernel(b0, b1, b2, b3, out):
    for j, block in enumerate((b0, b1, b2, b3)):
        out[j] = block[QK_DIM:, :]


def attend_kernel(where, q0, q1, q2, q3, *refs):
    blocks, outs, (q_s, top_s, acc_s) = refs[:8], refs[8:12], refs[12:]
    zh, zl, y, c, x = (where[i] for i in range(5))
    strip = q0.shape[1]
    span = blocks[0].shape[2]
    factor = QK_DIM ** (-0.5) * log2_e
    for j, q in enumerate((q0, q1, q2, q3)):
        at = pl.multiple_of(lax.rem(zh - j + 4, 4) * strip, strip)
        q_s[pl.ds(at, strip), :] = q[:QK_DIM, :].astype(F32).T.astype(BF)
    top_s[...] = jnp.full(top_s.shape, masked_value, F32)
    acc_s[...] = jnp.zeros(acc_s.shape, F32)

    col = lax.broadcasted_iota(jnp.int32, (1, span), 1)
    col_zl = jnp.bitwise_xor(zl, col // strip)
    within = col % strip
    col_x = ((x - within // 32 + 4) % 4) * 32 + within % 32
    query_at = (zl * 8 + y * 2 + c) * strip + lax.broadcasted_iota(jnp.int32, (strip, 1), 0)
    ones = jnp.ones((V_DIM, span), BF)

    def advance(rows, parts, masks):
        q = q_s[rows, :]
        old = top_s[rows, :]
        scores = [mm(q, part[:QK_DIM, :]) for part in parts]
        if masks is not None:
            scores = [jnp.where(m, s, masked_value) for m, s in zip(masks, scores)]
        peak = scores[0]
        for s in scores[1:]:
            peak = jnp.maximum(peak, s)
        new = jnp.maximum(old, jnp.max(peak, axis=1, keepdims=True))
        top_s[rows, :] = new
        base = new[:, :1]
        total = acc_s[rows, :] * jnp.exp2((old - new) * factor)
        for s, part in zip(scores, parts):
            raised = jnp.exp2((s - base) * factor).astype(BF)
            extended = jnp.concatenate([part[QK_DIM:, :], ones], axis=0)
            total = total + mm(raised, extended, ((1,), (1,)))
        acc_s[rows, :] = total

    for m in range(2):
        group = blocks[4 * m : 4 * m + 4]
        masks = []
        for k in range(4):
            key_y = lax.rem(y - k + 4, 4)
            key_at = (col_zl * 8 + key_y * 2 + jnp.bitwise_xor(c, m)) * strip + col_x
            masks.append(key_at <= query_at)
        for g in range(4):
            from_zh = lax.rem(zh - g + 4, 4)
            parts = [block[from_zh] for block in group]
            advance(slice(g * strip, (g + 1) * strip), parts, masks)
            if g < 3:
                advance(slice((g + 1) * strip, 4 * strip), parts, None)
    total = acc_s[...]
    acc_s[:, :V_DIM] = total[:, :V_DIM] / total[:, V_DIM:]
    for j, out in enumerate(outs):
        at = pl.multiple_of(lax.rem(zh - j + 4, 4) * strip, strip)
        out[...] = acc_s[pl.ds(at, strip), :V_DIM].astype(BF)


def spread_kernel(where, a0, a1, a2, a3, o0, o1, o2, o3, heads, parts):
    for j, a in enumerate((a0, a1, a2, a3)):
        heads[lax.rem(where[0] + j, 4)] = a[...]
    beside = jnp.concatenate([heads[h] for h in range(4)], axis=1)
    parts[...] = beside.reshape(parts.shape)
    for k, out in enumerate((o0, o1, o2, o3)):
        out[...] = parts[lax.rem(where[4] + k, 4)]


def project_kernel(where, a0, a1, a2, a3, out_proj, out, parts):
    width = a0.shape[1]
    for k, a in enumerate((a0, a1, a2, a3)):
        parts[lax.rem(where[4] - k + 4, 4)] = a[...]
    total = mm(parts[0], out_proj[:width, :])
    for h in range(1, 4):
        total = total + mm(parts[h], out_proj[h * width : (h + 1) * width, :])
    out[...] = total.astype(BF)


def query_and_pair(where, query, latent, rope_key, latent_gain, key_up, value_up):
    strip = query.shape[0]
    own = latent.shape[0]
    query_start = (((where[0] * 2 + where[1]) * 4 + where[2]) * 2 + where[3]) * strip

    key_cos, key_sin = trig(query_start + where[4] * own + jnp.arange(own, dtype=jnp.int32))
    both = call(
        latent_kernel,
        jax.ShapeDtypeStruct((own, latent.shape[1] + ROPE_DIM), BF),
        [
            latent,
            latent_gain[None, :],
            rope_key,
            jnp.concatenate([key_cos, key_cos], axis=1),
            jnp.concatenate([key_sin, key_sin], axis=1),
        ],
        unplaced=range(3),
    )
    near = [both] + [shifted(both, "x", k) for k in range(1, 4)]
    cosine, sine = trig(query_start + jnp.arange(strip, dtype=jnp.int32))
    blocks = call(
        heads_kernel,
        [jax.ShapeDtypeStruct((QK_DIM + KV_ROWS, strip), BF)] * 4,
        near + [key_up, value_up, query, cosine.T, sine.T],
        where,
        scratch=[
            pltpu.VMEM((strip, both.shape[1]), BF),
            pltpu.VMEM((4, QK_DIM + KV_ROWS, strip), BF),
        ],
        unplaced=range(4, 7),
    )
    blocks = [blocks[0]] + [shifted(blocks[k], "zh", k) for k in range(1, 4)]
    shape = jax.ShapeDtypeStruct((4, KV_ROWS, strip), BF)
    mine = call(stack_kernel, shape, blocks)
    return blocks, jnp.concatenate([mine, shifted(mine, "zl", 1)], axis=2)


def attend(where, blocks, pair):
    strip = blocks[0].shape[1]
    column = [pair] + [shifted(pair, "y", k) for k in range(1, 4)]
    column = column + [shifted(part, "c", 1) for part in column]
    parts = call(
        attend_kernel,
        [jax.ShapeDtypeStruct((strip, V_DIM), BF)] * 4,
        blocks + column,
        where,
        [
            pltpu.VMEM((4 * strip, QK_DIM), BF),
            pltpu.VMEM((4 * strip, 128), F32),
            pltpu.VMEM((4 * strip, 128), F32),
        ],
    )
    return [parts[0]] + [shifted(parts[j], "zh", -j) for j in range(1, 4)]


def project(where, parts, out_proj, own):
    strip = parts[0].shape[0]
    parts = call(
        spread_kernel,
        [jax.ShapeDtypeStruct((own, 4 * V_DIM), BF)] * 4,
        parts,
        where,
        [pltpu.VMEM((4, strip, V_DIM), BF), pltpu.VMEM((4, own, 4 * V_DIM), BF)],
    )
    parts = [parts[0]] + [shifted(parts[k], "x", k) for k in range(1, 4)]
    return call(
        project_kernel,
        jax.ShapeDtypeStruct((own, out_proj.shape[1]), BF),
        parts + [out_proj],
        where,
        [pltpu.VMEM((4, own, 4 * V_DIM), BF)],
        place=False,
    )


def both_halves(
    where,
    query,
    latent,
    rope_key,
    latent_gain,
    key_up,
    value_up,
    out_proj,
    tokens,
    moe_gain,
    routes,
    group_prob,
    expert_prob,
    w_gate,
    w_up,
    w_down,
):
    experts = lax.axis_size(EP)
    w_gate, w_up, w_down = w_gate[0], w_up[0], w_down[0]
    down_left, down_right = shifted(w_down, "x", 1), shifted(w_down, "x", -1)
    units = w_down.shape[0] // 2
    cut_a, cut_b = down_left[:units], down_right[units:]
    down_far = [shifted(cut_a, "x", 1), shifted(cut_b, "x", -1)]
    down = [w_down, down_right] + down_far + [down_left]
    first, second, shares = dispatch(
        tokens, moe_gain, routes, group_prob, expert_prob, experts
    )
    first, second = swapped(first), swapped(second)
    queries, pair = query_and_pair(where, query, latent, rope_key, latent_gain, key_up, value_up)
    parts = attend(where, queries, pair)
    first = expert_chunk(first, w_gate, w_up, down)
    second = expert_chunk(second, w_gate, w_up, down)
    mixed = project(where, parts, out_proj, latent.shape[0])
    shape = jax.ShapeDtypeStruct(tokens.shape, BF)
    arrays = [first, second, shares]
    return mixed, call(combine_kernel, shape, arrays, place=False)


def body(
    query,
    latent,
    rope_key,
    latent_gain,
    key_up,
    value_up,
    out_proj,
    tokens,
    moe_gain,
    routes,
    group_prob,
    expert_prob,
    w_gate,
    w_up,
    w_down,
):
    where = jnp.stack([lax.axis_index(n) for n in AXES]).astype(jnp.int32)
    return both_halves(
        where,
        query,
        latent,
        rope_key,
        latent_gain,
        key_up,
        value_up,
        out_proj,
        tokens,
        moe_gain,
        routes,
        group_prob,
        expert_prob,
        w_gate,
        w_up,
        w_down,
    )


def solution(mesh):
    ep, every = EP, AXES
    split = Mesh(mesh.devices.reshape(4, 2, 4, 2, 4), AXES)
    return jax.shard_map(
        body,
        mesh=split,
        in_specs=(
            P(ep, "x"),
            P(every, None),
            P(every, None),
            P(),
            P(None, "x"),
            P(None, "x"),
            P(),
            P(every, None),
            P(),
            P(every, None),
            P(every),
            P(every, None),
            P(ep, None, "x"),
            P(ep, None, "x"),
            P(ep, "x", None),
        ),
        out_specs=(P(every, None), P(every, None)),
        check_vma=False,
    )
```

```python
import jax
import jax.numpy as jnp
from jax import lax
from jax.experimental import pallas as pl
from jax.experimental.pallas import tpu as pltpu
from jax.sharding import Mesh, PartitionSpec as P


NOPE = 64
ROPE_DIM = 32
V_DIM = 64
QK_DIM = NOPE + ROPE_DIM
KV_ROWS = QK_DIM + V_DIM
CAP = 4
BF = jnp.bfloat16
F32 = jnp.float32

epsilon = 1e-06
rope_base = 10000.0
masked_value = -1e30
log2_e = 1.4426950408889634


AXES = ("zh", "zl", "y", "c", "x")
EP = AXES[:4]

SMEM_SPEC = pl.BlockSpec(memory_space=pltpu.SMEM)
VMEM_SPEC = pl.BlockSpec(memory_space=pltpu.VMEM)


def call(kernel, out_shape, arrays, where=None, scratch=(), limit=16 << 20, unplaced=(), place=True):
    arrays = [
        pltpu.with_memory_space_constraint(a, pltpu.HBM if i in unplaced else pltpu.VMEM)
        for i, a in enumerate(arrays)
    ]
    specs = [VMEM_SPEC] * len(arrays)
    if where is not None:
        arrays, specs = [where] + arrays, [SMEM_SPEC] + specs
    single = not isinstance(out_shape, (list, tuple))
    if place:
        if single:
            out_shape = pltpu.VMEM(out_shape.shape, out_shape.dtype)
        else:
            out_shape = [pltpu.VMEM(s.shape, s.dtype) for s in out_shape]
    return pl.pallas_call(
        kernel,
        in_specs=specs,
        out_specs=VMEM_SPEC if single else [VMEM_SPEC] * len(out_shape),
        out_shape=out_shape,
        scratch_shapes=list(scratch),
        compiler_params=pltpu.CompilerParams(vmem_limit_bytes=limit),
    )(*arrays)


def mm(a, b, dims=((1,), (0,))):
    return lax.dot_general(a, b, (dims, ((), ())), preferred_element_type=F32)


def shifted(value, axis, amount):
    n = lax.axis_size(axis)
    return lax.ppermute(value, axis, [(i, (i + amount) % n) for i in range(n)])


def trig(positions):
    half = ROPE_DIM // 2
    inverse = rope_base ** (-2.0 * jnp.arange(half, dtype=F32) / ROPE_DIM)
    angles = positions.astype(F32)[:, None] * inverse[None, :]
    return jnp.cos(angles), jnp.sin(angles)


def rms_scale(values, gain):
    widened = values.astype(F32)
    return widened * lax.rsqrt(jnp.mean(widened * widened, axis=-1, keepdims=True) + epsilon) * gain


def dispatch_kernel(tokens, gain, routes, group_prob, expert_prob, outgoing, shares_out):
    rows = tokens.shape[0]
    experts, cap, width = outgoing.shape
    slots = experts * cap
    normed = rms_scale(tokens[...], gain[...]).astype(BF)
    slot = lax.broadcasted_iota(jnp.int32, (slots, rows), 0)
    expert = slot // cap
    first = routes[0:1, :] == expert
    second = routes[1:2, :] == expert
    named = (first | second).astype(BF)
    before = lax.broadcasted_iota(jnp.int32, (rows, rows), 0) < lax.broadcasted_iota(
        jnp.int32, (rows, rows), 1
    )
    prior = mm(named, before.astype(BF))
    mine = (first | second) & (prior == (slot % cap).astype(F32))
    outgoing[...] = mm(mine.astype(BF), normed).reshape(experts, cap, width).astype(BF)
    probs = expert_prob[...]
    shares = group_prob[...] * probs / jnp.sum(probs, axis=0, keepdims=True)
    weights = jnp.where(first, shares[0:1, :], shares[1:2, :])
    weights = jnp.where(mine, weights, 0.0)
    high = weights.astype(BF)
    shares_out[:, 0:rows] = high
    shares_out[:, rows : 2 * rows] = (weights - high.astype(F32)).astype(BF)


def dispatch(tokens, gain, routes, group_prob, expert_prob, experts):
    rows, width = tokens.shape
    return call(
        dispatch_kernel,
        (
            jax.ShapeDtypeStruct((experts, CAP, width), BF),
            jax.ShapeDtypeStruct((experts * CAP, 2 * rows), BF),
        ),
        [tokens, gain[None, :], routes.T, group_prob[None, :], expert_prob.T],
        unplaced=range(5),
    )


def hidden_kernel(rows_a, rows_b, w_gate, w_up, out):
    half = out.shape[0] // 2
    for at, rows in ((0, rows_a), (half, rows_b)):
        got = rows[...].reshape(half, w_gate.shape[0])
        gate = mm(got, w_gate[...])
        up = mm(got, w_up[...])
        out[at : at + half, :] = (gate / (1.0 + jnp.exp(-gate)) * up).astype(BF)


def hidden_of(rows_a, rows_b, w_gate, w_up):
    shape = jax.ShapeDtypeStruct((2 * rows_a.shape[0] * CAP, w_gate.shape[1]), BF)
    return call(hidden_kernel, shape, [rows_a, rows_b, w_gate, w_up])


def down_kernel(h0, h1, h2, h3, w0, w1, w2a, w2b, w3, out):
    half = w2a.shape[0]
    total = mm(h0[...], w0[...]) + mm(h1[...], w1[...]) + mm(h3[...], w3[...])
    total = total + mm(h2[:, :half], w2a[...]) + mm(h2[:, half:], w2b[...])
    out[...] = total.reshape(out.shape).astype(BF)


def combine_kernel(returned, shares, out):
    rows = out.shape[0]
    got = returned[...].reshape(shares.shape[0], out.shape[1])
    both = mm(shares[...], got, ((0,), (0,)))
    out[...] = (both[:rows] + both[rows:]).astype(BF)


def both_halves(
    where,
    query,
    latent,
    rope_key,
    latent_gain,
    key_up,
    value_up,
    out_proj,
    tokens,
    moe_gain,
    routes,
    group_prob,
    expert_prob,
    w_gate,
    w_up,
    w_down,
):
    experts = lax.axis_size(EP)
    rows, width = tokens.shape
    w_gate, w_up, w_down = w_gate[0], w_up[0], w_down[0]
    down_left, down_right = shifted(w_down, "x", 1), shifted(w_down, "x", -1)
    units = w_down.shape[0] // 2
    cut_a, cut_b = down_left[:units], down_right[units:]
    down_far = [shifted(cut_a, "x", 1), shifted(cut_b, "x", -1)]
    outgoing, shares = dispatch(tokens, moe_gain, routes, group_prob, expert_prob, experts)
    arrived = lax.all_to_all(outgoing, EP, split_axis=0, concat_axis=0, tiled=True)
    queries, pair = query_and_pair(where, query, latent, rope_key, latent_gain, key_up, value_up)
    half = experts // 2
    a, b = arrived[:half], arrived[half:]
    left_a, right_b = shifted(a, "x", 1), shifted(b, "x", -1)
    left_b, right_a = shifted(b, "x", 1), shifted(a, "x", -1)
    far_a, far_b = shifted(left_a, "x", 1), shifted(right_b, "x", -1)
    parts = attend(where, queries, pair)
    hidden = [
        hidden_of(a, b, w_gate, w_up),
        shifted(hidden_of(left_a, left_b, w_gate, w_up), "x", -1),
        shifted(hidden_of(far_a, far_b, w_gate, w_up), "x", 2),
        shifted(hidden_of(right_a, right_b, w_gate, w_up), "x", 1),
    ]
    shape = jax.ShapeDtypeStruct((experts, CAP, width), BF)
    down = [w_down, down_right] + down_far + [down_left]
    result = call(down_kernel, shape, hidden + down)
    returned = lax.all_to_all(result, EP, split_axis=0, concat_axis=0, tiled=True)
    mixed = project(where, parts, out_proj, latent.shape[0])
    shape = jax.ShapeDtypeStruct((rows, width), BF)
    return mixed, call(combine_kernel, shape, [returned, shares], place=False)


def latent_kernel(latent, gain, rope_key, cosine, sine, out):
    width = latent.shape[1]
    half = ROPE_DIM // 2
    out[:, :width] = rms_scale(latent[...], gain[...]).astype(BF)
    rope = rope_key[...].astype(F32)
    crossed = jnp.concatenate([-rope[:, half:], rope[:, :half]], axis=1)
    out[:, width:] = (rope * cosine[...] + crossed * sine[...]).astype(BF)


def heads_kernel(
    where, l0, l1, l2, l3, key_up, value_up, query, cosine, sine, o0, o1, o2, o3, strip_s, heads
):
    latent = key_up.shape[0]
    own = l0.shape[0]
    count = heads.shape[0]
    half = ROPE_DIM // 2
    turned = query[...].astype(F32).T
    for h in range(count):
        at = h * QK_DIM
        a = turned[at + NOPE : at + NOPE + half]
        b = turned[at + NOPE + half : at + QK_DIM]
        heads[h, :NOPE, :] = turned[at : at + NOPE].astype(BF)
        heads[h, NOPE : NOPE + half, :] = (a * cosine[...] - b * sine[...]).astype(BF)
        heads[h, NOPE + half : QK_DIM, :] = (a * sine[...] + b * cosine[...]).astype(BF)
    for k, block in enumerate((l0, l1, l2, l3)):
        strip_s[k * own : (k + 1) * own, :] = block[...]
    got = strip_s[:, :latent]
    keys = mm(key_up[...], got, ((0,), (1,))).astype(BF)
    values = mm(value_up[...], got, ((0,), (1,))).astype(BF)
    eye = (
        lax.broadcasted_iota(jnp.int32, (ROPE_DIM, ROPE_DIM), 0)
        == lax.broadcasted_iota(jnp.int32, (ROPE_DIM, ROPE_DIM), 1)
    ).astype(BF)
    rope = mm(eye, strip_s[:, latent:], ((1,), (1,))).astype(BF)
    for h in range(count):
        heads[h, QK_DIM : QK_DIM + NOPE, :] = keys[h * NOPE : (h + 1) * NOPE]
        heads[h, QK_DIM + NOPE : 2 * QK_DIM, :] = rope
        heads[h, 2 * QK_DIM :, :] = values[h * V_DIM : (h + 1) * V_DIM]
    for k, out in enumerate((o0, o1, o2, o3)):
        out[...] = heads[lax.rem(where[0] + k, 4)]


def stack_kernel(b0, b1, b2, b3, out):
    for j, block in enumerate((b0, b1, b2, b3)):
        out[j] = block[QK_DIM:, :]


def attend_kernel(where, q0, q1, q2, q3, *refs):
    blocks, outs, (q_s, top_s, acc_s) = refs[:8], refs[8:12], refs[12:]
    zh, zl, y, c, x = (where[i] for i in range(5))
    strip = q0.shape[1]
    span = blocks[0].shape[2]
    factor = QK_DIM ** (-0.5) * log2_e
    for j, q in enumerate((q0, q1, q2, q3)):
        at = pl.multiple_of(lax.rem(zh - j + 4, 4) * strip, strip)
        q_s[pl.ds(at, strip), :] = q[:QK_DIM, :].astype(F32).T.astype(BF)
    top_s[...] = jnp.full(top_s.shape, masked_value, F32)
    acc_s[...] = jnp.zeros(acc_s.shape, F32)

    col = lax.broadcasted_iota(jnp.int32, (1, span), 1)
    col_zl = jnp.bitwise_xor(zl, col // strip)
    within = col % strip
    col_x = ((x - within // 32 + 4) % 4) * 32 + within % 32
    query_at = (zl * 8 + y * 2 + c) * strip + lax.broadcasted_iota(jnp.int32, (strip, 1), 0)
    ones = jnp.ones((V_DIM, span), BF)

    def advance(rows, parts, masks):
        q = q_s[rows, :]
        old = top_s[rows, :]
        scores = [mm(q, part[:QK_DIM, :]) for part in parts]
        if masks is not None:
            scores = [jnp.where(m, s, masked_value) for m, s in zip(masks, scores)]
        peak = scores[0]
        for s in scores[1:]:
            peak = jnp.maximum(peak, s)
        new = jnp.maximum(old, jnp.max(peak, axis=1, keepdims=True))
        top_s[rows, :] = new
        base = new[:, :1]
        total = acc_s[rows, :] * jnp.exp2((old - new) * factor)
        for s, part in zip(scores, parts):
            raised = jnp.exp2((s - base) * factor).astype(BF)
            extended = jnp.concatenate([part[QK_DIM:, :], ones], axis=0)
            total = total + mm(raised, extended, ((1,), (1,)))
        acc_s[rows, :] = total

    for m in range(2):
        group = blocks[4 * m : 4 * m + 4]
        masks = []
        for k in range(4):
            key_y = lax.rem(y - k + 4, 4)
            key_at = (col_zl * 8 + key_y * 2 + jnp.bitwise_xor(c, m)) * strip + col_x
            masks.append(key_at <= query_at)

        def one_group(g, _, group=group, masks=masks):
            from_zh = lax.rem(zh - g + 4, 4)
            parts = [block.at[from_zh] for block in group]

            def later(s, _):
                advance(pl.ds(pl.multiple_of(s * strip, strip), strip), parts, None)
                return 0

            advance(pl.ds(pl.multiple_of(g * strip, strip), strip), parts, masks)
            return lax.fori_loop(g + 1, 4, later, 0)

        lax.fori_loop(0, 4, one_group, 0)
    total = acc_s[...]
    acc_s[:, :V_DIM] = total[:, :V_DIM] / total[:, V_DIM:]
    for j, out in enumerate(outs):
        at = pl.multiple_of(lax.rem(zh - j + 4, 4) * strip, strip)
        out[...] = acc_s[pl.ds(at, strip), :V_DIM].astype(BF)


def spread_kernel(where, a0, a1, a2, a3, o0, o1, o2, o3, heads, parts):
    for j, a in enumerate((a0, a1, a2, a3)):
        heads[lax.rem(where[0] + j, 4)] = a[...]
    beside = jnp.concatenate([heads[h] for h in range(4)], axis=1)
    parts[...] = beside.reshape(parts.shape)
    for k, out in enumerate((o0, o1, o2, o3)):
        out[...] = parts[lax.rem(where[4] + k, 4)]


def project_kernel(where, a0, a1, a2, a3, out_proj, out, parts):
    width = a0.shape[1]
    for k, a in enumerate((a0, a1, a2, a3)):
        parts[lax.rem(where[4] - k + 4, 4)] = a[...]
    total = mm(parts[0], out_proj[:width, :])
    for h in range(1, 4):
        total = total + mm(parts[h], out_proj[h * width : (h + 1) * width, :])
    out[...] = total.astype(BF)


def query_and_pair(where, query, latent, rope_key, latent_gain, key_up, value_up):
    strip = query.shape[0]
    own = latent.shape[0]
    query_start = (((where[0] * 2 + where[1]) * 4 + where[2]) * 2 + where[3]) * strip

    key_cos, key_sin = trig(query_start + where[4] * own + jnp.arange(own, dtype=jnp.int32))
    both = call(
        latent_kernel,
        jax.ShapeDtypeStruct((own, latent.shape[1] + ROPE_DIM), BF),
        [
            latent,
            latent_gain[None, :],
            rope_key,
            jnp.concatenate([key_cos, key_cos], axis=1),
            jnp.concatenate([key_sin, key_sin], axis=1),
        ],
        unplaced=range(3),
    )
    near = [both] + [shifted(both, "x", k) for k in range(1, 4)]
    cosine, sine = trig(query_start + jnp.arange(strip, dtype=jnp.int32))
    blocks = call(
        heads_kernel,
        [jax.ShapeDtypeStruct((QK_DIM + KV_ROWS, strip), BF)] * 4,
        near + [key_up, value_up, query, cosine.T, sine.T],
        where,
        scratch=[
            pltpu.VMEM((strip, both.shape[1]), BF),
            pltpu.VMEM((4, QK_DIM + KV_ROWS, strip), BF),
        ],
        unplaced=range(4, 7),
    )
    blocks = [blocks[0]] + [shifted(blocks[k], "zh", k) for k in range(1, 4)]
    shape = jax.ShapeDtypeStruct((4, KV_ROWS, strip), BF)
    mine = call(stack_kernel, shape, blocks)
    return blocks, jnp.concatenate([mine, shifted(mine, "zl", 1)], axis=2)


def attend(where, blocks, pair):
    strip = blocks[0].shape[1]
    column = [pair] + [shifted(pair, "y", k) for k in range(1, 4)]
    column = column + [shifted(part, "c", 1) for part in column]
    parts = call(
        attend_kernel,
        [jax.ShapeDtypeStruct((strip, V_DIM), BF)] * 4,
        blocks + column,
        where,
        [
            pltpu.VMEM((4 * strip, QK_DIM), BF),
            pltpu.VMEM((4 * strip, 128), F32),
            pltpu.VMEM((4 * strip, 128), F32),
        ],
    )
    return [parts[0]] + [shifted(parts[j], "zh", -j) for j in range(1, 4)]


def project(where, parts, out_proj, own):
    strip = parts[0].shape[0]
    parts = call(
        spread_kernel,
        [jax.ShapeDtypeStruct((own, 4 * V_DIM), BF)] * 4,
        parts,
        where,
        [pltpu.VMEM((4, strip, V_DIM), BF), pltpu.VMEM((4, own, 4 * V_DIM), BF)],
    )
    parts = [parts[0]] + [shifted(parts[k], "x", k) for k in range(1, 4)]
    return call(
        project_kernel,
        jax.ShapeDtypeStruct((own, out_proj.shape[1]), BF),
        parts + [out_proj],
        where,
        [pltpu.VMEM((4, own, 4 * V_DIM), BF)],
        place=False,
    )


def body(
    query,
    latent,
    rope_key,
    latent_gain,
    key_up,
    value_up,
    out_proj,
    tokens,
    moe_gain,
    routes,
    group_prob,
    expert_prob,
    w_gate,
    w_up,
    w_down,
):
    where = jnp.stack([lax.axis_index(n) for n in AXES]).astype(jnp.int32)
    return both_halves(
        where,
        query,
        latent,
        rope_key,
        latent_gain,
        key_up,
        value_up,
        out_proj,
        tokens,
        moe_gain,
        routes,
        group_prob,
        expert_prob,
        w_gate,
        w_up,
        w_down,
    )


def solution(mesh):
    ep, every = EP, AXES
    split = Mesh(mesh.devices.reshape(4, 2, 4, 2, 4), AXES)
    return jax.shard_map(
        body,
        mesh=split,
        in_specs=(
            P(ep, "x"),
            P(every, None),
            P(every, None),
            P(),
            P(None, "x"),
            P(None, "x"),
            P(),
            P(every, None),
            P(),
            P(every, None),
            P(every),
            P(every, None),
            P(ep, None, "x"),
            P(ep, None, "x"),
            P(ep, "x", None),
        ),
        out_specs=(P(every, None), P(every, None)),
        check_vma=False,
    )
```

```python
import jax
import jax.numpy as jnp
from jax import lax
from jax.experimental import pallas as pl
from jax.experimental.pallas import tpu as pltpu
from jax.sharding import Mesh, PartitionSpec as P


NOPE = 64
ROPE_DIM = 32
V_DIM = 64
QK_DIM = NOPE + ROPE_DIM
KV_ROWS = QK_DIM + V_DIM
CAP = 4
BF = jnp.bfloat16
F32 = jnp.float32

epsilon = 1e-06
rope_base = 10000.0
masked_value = -1e30
log2_e = 1.4426950408889634


AXES = ("zh", "zl", "y", "c", "x")
EP = AXES[:4]

SMEM_SPEC = pl.BlockSpec(memory_space=pltpu.SMEM)
VMEM_SPEC = pl.BlockSpec(memory_space=pltpu.VMEM)


def call(kernel, out_shape, arrays, where=None, scratch=(), limit=8 << 20, unplaced=(), place=True):
    arrays = [
        pltpu.with_memory_space_constraint(a, pltpu.HBM if i in unplaced else pltpu.VMEM)
        for i, a in enumerate(arrays)
    ]
    specs = [VMEM_SPEC] * len(arrays)
    if where is not None:
        arrays, specs = [where] + arrays, [SMEM_SPEC] + specs
    single = not isinstance(out_shape, (list, tuple))
    if place:
        if single:
            out_shape = pltpu.VMEM(out_shape.shape, out_shape.dtype)
        else:
            out_shape = [pltpu.VMEM(s.shape, s.dtype) for s in out_shape]
    return pl.pallas_call(
        kernel,
        in_specs=specs,
        out_specs=VMEM_SPEC if single else [VMEM_SPEC] * len(out_shape),
        out_shape=out_shape,
        scratch_shapes=list(scratch),
        compiler_params=pltpu.CompilerParams(vmem_limit_bytes=limit),
    )(*arrays)


def mm(a, b, dims=((1,), (0,))):
    return lax.dot_general(a, b, (dims, ((), ())), preferred_element_type=F32)


def shifted(value, axis, amount):
    n = lax.axis_size(axis)
    return lax.ppermute(value, axis, [(i, (i + amount) % n) for i in range(n)])


def trig(positions):
    half = ROPE_DIM // 2
    inverse = rope_base ** (-2.0 * jnp.arange(half, dtype=F32) / ROPE_DIM)
    angles = positions.astype(F32)[:, None] * inverse[None, :]
    return jnp.cos(angles), jnp.sin(angles)


def rms_scale(values, gain):
    widened = values.astype(F32)
    return widened * lax.rsqrt(jnp.mean(widened * widened, axis=-1, keepdims=True) + epsilon) * gain


def dispatch_kernel(tokens, gain, routes, group_prob, expert_prob, outgoing, shares_out):
    rows = tokens.shape[0]
    experts, cap, width = outgoing.shape
    slots = experts * cap
    normed = rms_scale(tokens[...], gain[...]).astype(BF)
    slot = lax.broadcasted_iota(jnp.int32, (slots, rows), 0)
    expert = slot // cap
    first = routes[0:1, :] == expert
    second = routes[1:2, :] == expert
    named = (first | second).astype(BF)
    before = lax.broadcasted_iota(jnp.int32, (rows, rows), 0) < lax.broadcasted_iota(
        jnp.int32, (rows, rows), 1
    )
    prior = mm(named, before.astype(BF))
    mine = (first | second) & (prior == (slot % cap).astype(F32))
    outgoing[...] = mm(mine.astype(BF), normed).reshape(experts, cap, width).astype(BF)
    probs = expert_prob[...]
    shares = group_prob[...] * probs / jnp.sum(probs, axis=0, keepdims=True)
    weights = jnp.where(first, shares[0:1, :], shares[1:2, :])
    weights = jnp.where(mine, weights, 0.0)
    high = weights.astype(BF)
    shares_out[:, 0:rows] = high
    shares_out[:, rows : 2 * rows] = (weights - high.astype(F32)).astype(BF)


def dispatch(tokens, gain, routes, group_prob, expert_prob, experts):
    rows, width = tokens.shape
    return call(
        dispatch_kernel,
        (
            jax.ShapeDtypeStruct((experts, CAP, width), BF),
            jax.ShapeDtypeStruct((experts * CAP, 2 * rows), BF),
        ),
        [tokens, gain[None, :], routes.T, group_prob[None, :], expert_prob.T],
        unplaced=range(5),
    )


def hidden_kernel(rows_a, rows_b, w_gate, w_up, out, gate_s, up_s):
    half, span = out.shape[0] // 2, 512
    gate_s[...] = jnp.zeros(gate_s.shape, F32)
    up_s[...] = jnp.zeros(up_s.shape, F32)

    def add(step, _):
        cols = pl.ds(pl.multiple_of(step * span, span), span)
        for at, rows in ((0, rows_a), (half, rows_b)):
            got = rows[:, :, cols].reshape(half, span)
            gate_s[at : at + half, :] += mm(got, w_gate[cols, :])
            up_s[at : at + half, :] += mm(got, w_up[cols, :])
        return 0

    lax.fori_loop(0, w_gate.shape[0] // span, add, 0)
    gate = gate_s[...]
    out[...] = (gate / (1.0 + jnp.exp(-gate)) * up_s[...]).astype(BF)


def hidden_of(rows_a, rows_b, w_gate, w_up):
    shape = jax.ShapeDtypeStruct((2 * rows_a.shape[0] * CAP, w_gate.shape[1]), BF)
    scratch = [pltpu.VMEM(shape.shape, F32)] * 2
    return call(hidden_kernel, shape, [rows_a, rows_b, w_gate, w_up], scratch=scratch)


def down_kernel(h0, h1, h2, h3, w0, w1, w2a, w2b, w3, out):
    half = w2a.shape[0]
    total = mm(h0[...], w0[...]) + mm(h1[...], w1[...]) + mm(h3[...], w3[...])
    total = total + mm(h2[:, :half], w2a[...]) + mm(h2[:, half:], w2b[...])
    out[...] = total.reshape(out.shape).astype(BF)


def combine_kernel(returned, shares, out):
    rows = out.shape[0]
    got = returned[...].reshape(shares.shape[0], out.shape[1])
    both = mm(shares[...], got, ((0,), (0,)))
    out[...] = (both[:rows] + both[rows:]).astype(BF)


def both_halves(
    where,
    query,
    latent,
    rope_key,
    latent_gain,
    key_up,
    value_up,
    out_proj,
    tokens,
    moe_gain,
    routes,
    group_prob,
    expert_prob,
    w_gate,
    w_up,
    w_down,
):
    experts = lax.axis_size(EP)
    rows, width = tokens.shape
    w_gate, w_up, w_down = w_gate[0], w_up[0], w_down[0]
    down_left, down_right = shifted(w_down, "x", 1), shifted(w_down, "x", -1)
    units = w_down.shape[0] // 2
    cut_a, cut_b = down_left[:units], down_right[units:]
    down_far = [shifted(cut_a, "x", 1), shifted(cut_b, "x", -1)]
    outgoing, shares = dispatch(tokens, moe_gain, routes, group_prob, expert_prob, experts)
    arrived = lax.all_to_all(outgoing, EP, split_axis=0, concat_axis=0, tiled=True)
    queries, pair = query_and_pair(where, query, latent, rope_key, latent_gain, key_up, value_up)
    half = experts // 2
    a, b = arrived[:half], arrived[half:]
    left_a, right_b = shifted(a, "x", 1), shifted(b, "x", -1)
    left_b, right_a = shifted(b, "x", 1), shifted(a, "x", -1)
    far_a, far_b = shifted(left_a, "x", 1), shifted(right_b, "x", -1)
    parts = attend(where, queries, pair)
    hidden = [
        hidden_of(a, b, w_gate, w_up),
        shifted(hidden_of(left_a, left_b, w_gate, w_up), "x", -1),
        shifted(hidden_of(far_a, far_b, w_gate, w_up), "x", 2),
        shifted(hidden_of(right_a, right_b, w_gate, w_up), "x", 1),
    ]
    shape = jax.ShapeDtypeStruct((experts, CAP, width), BF)
    down = [w_down, down_right] + down_far + [down_left]
    result = call(down_kernel, shape, hidden + down)
    returned = lax.all_to_all(result, EP, split_axis=0, concat_axis=0, tiled=True)
    mixed = project(where, parts, out_proj, latent.shape[0])
    shape = jax.ShapeDtypeStruct((rows, width), BF)
    return mixed, call(combine_kernel, shape, [returned, shares], place=False)


def latent_kernel(latent, gain, rope_key, cosine, sine, out):
    width = latent.shape[1]
    half = ROPE_DIM // 2
    out[:, :width] = rms_scale(latent[...], gain[...]).astype(BF)
    rope = rope_key[...].astype(F32)
    crossed = jnp.concatenate([-rope[:, half:], rope[:, :half]], axis=1)
    out[:, width:] = (rope * cosine[...] + crossed * sine[...]).astype(BF)


def heads_kernel(
    where, l0, l1, l2, l3, key_up, value_up, query, cosine, sine, o0, o1, o2, o3, strip_s, heads
):
    latent = key_up.shape[0]
    own = l0.shape[0]
    count = heads.shape[0]
    half = ROPE_DIM // 2
    turned = query[...].astype(F32).T
    for h in range(count):
        at = h * QK_DIM
        a = turned[at + NOPE : at + NOPE + half]
        b = turned[at + NOPE + half : at + QK_DIM]
        heads[h, :NOPE, :] = turned[at : at + NOPE].astype(BF)
        heads[h, NOPE : NOPE + half, :] = (a * cosine[...] - b * sine[...]).astype(BF)
        heads[h, NOPE + half : QK_DIM, :] = (a * sine[...] + b * cosine[...]).astype(BF)
    for k, block in enumerate((l0, l1, l2, l3)):
        strip_s[k * own : (k + 1) * own, :] = block[...]
    got = strip_s[:, :latent]
    keys = mm(key_up[...], got, ((0,), (1,))).astype(BF)
    values = mm(value_up[...], got, ((0,), (1,))).astype(BF)
    eye = (
        lax.broadcasted_iota(jnp.int32, (ROPE_DIM, ROPE_DIM), 0)
        == lax.broadcasted_iota(jnp.int32, (ROPE_DIM, ROPE_DIM), 1)
    ).astype(BF)
    rope = mm(eye, strip_s[:, latent:], ((1,), (1,))).astype(BF)
    for h in range(count):
        heads[h, QK_DIM : QK_DIM + NOPE, :] = keys[h * NOPE : (h + 1) * NOPE]
        heads[h, QK_DIM + NOPE : 2 * QK_DIM, :] = rope
        heads[h, 2 * QK_DIM :, :] = values[h * V_DIM : (h + 1) * V_DIM]
    for k, out in enumerate((o0, o1, o2, o3)):
        out[...] = heads[lax.rem(where[0] + k, 4)]


def stack_kernel(b0, b1, b2, b3, out):
    for j, block in enumerate((b0, b1, b2, b3)):
        out[j] = block[QK_DIM:, :]


def attend_kernel(where, q0, q1, q2, q3, *refs):
    blocks, outs, (q_s, top_s, acc_s) = refs[:8], refs[8:12], refs[12:]
    zh, zl, y, c, x = (where[i] for i in range(5))
    strip = q0.shape[1]
    span = blocks[0].shape[2]
    factor = QK_DIM ** (-0.5) * log2_e
    for j, q in enumerate((q0, q1, q2, q3)):
        at = pl.multiple_of(lax.rem(zh - j + 4, 4) * strip, strip)
        q_s[pl.ds(at, strip), :] = q[:QK_DIM, :].astype(F32).T.astype(BF)
    top_s[...] = jnp.full(top_s.shape, masked_value, F32)
    acc_s[...] = jnp.zeros(acc_s.shape, F32)

    col = lax.broadcasted_iota(jnp.int32, (1, span), 1)
    col_zl = jnp.bitwise_xor(zl, col // strip)
    within = col % strip
    col_x = ((x - within // 32 + 4) % 4) * 32 + within % 32
    query_at = (zl * 8 + y * 2 + c) * strip + lax.broadcasted_iota(jnp.int32, (strip, 1), 0)
    ones = jnp.ones((V_DIM, span), BF)

    def advance(rows, parts, masks):
        q = q_s[rows, :]
        old = top_s[rows, :]
        scores = [mm(q, part[:QK_DIM, :]) for part in parts]
        if masks is not None:
            scores = [jnp.where(m, s, masked_value) for m, s in zip(masks, scores)]
        peak = scores[0]
        for s in scores[1:]:
            peak = jnp.maximum(peak, s)
        new = jnp.maximum(old, jnp.max(peak, axis=1, keepdims=True))
        top_s[rows, :] = new
        base = new[:, :1]
        total = acc_s[rows, :] * jnp.exp2((old - new) * factor)
        for s, part in zip(scores, parts):
            raised = jnp.exp2((s - base) * factor).astype(BF)
            extended = jnp.concatenate([part[QK_DIM:, :], ones], axis=0)
            total = total + mm(raised, extended, ((1,), (1,)))
        acc_s[rows, :] = total

    for m in range(2):
        group = blocks[4 * m : 4 * m + 4]
        masks = []
        for k in range(4):
            key_y = lax.rem(y - k + 4, 4)
            key_at = (col_zl * 8 + key_y * 2 + jnp.bitwise_xor(c, m)) * strip + col_x
            masks.append(key_at <= query_at)

        for g in range(4):
            from_zh = lax.rem(zh - g + 4, 4)
            parts = [block[from_zh] for block in group]
            advance(slice(g * strip, (g + 1) * strip), parts, masks)
            if g < 3:
                advance(slice((g + 1) * strip, 4 * strip), parts, None)
    total = acc_s[...]
    acc_s[:, :V_DIM] = total[:, :V_DIM] / total[:, V_DIM:]
    for j, out in enumerate(outs):
        at = pl.multiple_of(lax.rem(zh - j + 4, 4) * strip, strip)
        out[...] = acc_s[pl.ds(at, strip), :V_DIM].astype(BF)


def spread_kernel(where, a0, a1, a2, a3, o0, o1, o2, o3, heads, parts):
    for j, a in enumerate((a0, a1, a2, a3)):
        heads[lax.rem(where[0] + j, 4)] = a[...]
    beside = jnp.concatenate([heads[h] for h in range(4)], axis=1)
    parts[...] = beside.reshape(parts.shape)
    for k, out in enumerate((o0, o1, o2, o3)):
        out[...] = parts[lax.rem(where[4] + k, 4)]


def project_kernel(where, a0, a1, a2, a3, out_proj, out, parts):
    width = a0.shape[1]
    for k, a in enumerate((a0, a1, a2, a3)):
        parts[lax.rem(where[4] - k + 4, 4)] = a[...]
    total = mm(parts[0], out_proj[:width, :])
    for h in range(1, 4):
        total = total + mm(parts[h], out_proj[h * width : (h + 1) * width, :])
    out[...] = total.astype(BF)


def query_and_pair(where, query, latent, rope_key, latent_gain, key_up, value_up):
    strip = query.shape[0]
    own = latent.shape[0]
    query_start = (((where[0] * 2 + where[1]) * 4 + where[2]) * 2 + where[3]) * strip

    key_cos, key_sin = trig(query_start + where[4] * own + jnp.arange(own, dtype=jnp.int32))
    both = call(
        latent_kernel,
        jax.ShapeDtypeStruct((own, latent.shape[1] + ROPE_DIM), BF),
        [
            latent,
            latent_gain[None, :],
            rope_key,
            jnp.concatenate([key_cos, key_cos], axis=1),
            jnp.concatenate([key_sin, key_sin], axis=1),
        ],
        unplaced=range(3),
    )
    near = [both] + [shifted(both, "x", k) for k in range(1, 4)]
    cosine, sine = trig(query_start + jnp.arange(strip, dtype=jnp.int32))
    blocks = call(
        heads_kernel,
        [jax.ShapeDtypeStruct((QK_DIM + KV_ROWS, strip), BF)] * 4,
        near + [key_up, value_up, query, cosine.T, sine.T],
        where,
        scratch=[
            pltpu.VMEM((strip, both.shape[1]), BF),
            pltpu.VMEM((4, QK_DIM + KV_ROWS, strip), BF),
        ],
        unplaced=range(4, 7),
    )
    blocks = [blocks[0]] + [shifted(blocks[k], "zh", k) for k in range(1, 4)]
    shape = jax.ShapeDtypeStruct((4, KV_ROWS, strip), BF)
    mine = call(stack_kernel, shape, blocks)
    return blocks, jnp.concatenate([mine, shifted(mine, "zl", 1)], axis=2)


def attend(where, blocks, pair):
    strip = blocks[0].shape[1]
    column = [pair] + [shifted(pair, "y", k) for k in range(1, 4)]
    column = column + [shifted(part, "c", 1) for part in column]
    parts = call(
        attend_kernel,
        [jax.ShapeDtypeStruct((strip, V_DIM), BF)] * 4,
        blocks + column,
        where,
        [
            pltpu.VMEM((4 * strip, QK_DIM), BF),
            pltpu.VMEM((4 * strip, 128), F32),
            pltpu.VMEM((4 * strip, 128), F32),
        ],
    )
    return [parts[0]] + [shifted(parts[j], "zh", -j) for j in range(1, 4)]


def project(where, parts, out_proj, own):
    strip = parts[0].shape[0]
    parts = call(
        spread_kernel,
        [jax.ShapeDtypeStruct((own, 4 * V_DIM), BF)] * 4,
        parts,
        where,
        [pltpu.VMEM((4, strip, V_DIM), BF), pltpu.VMEM((4, own, 4 * V_DIM), BF)],
    )
    parts = [parts[0]] + [shifted(parts[k], "x", k) for k in range(1, 4)]
    return call(
        project_kernel,
        jax.ShapeDtypeStruct((own, out_proj.shape[1]), BF),
        parts + [out_proj],
        where,
        [pltpu.VMEM((4, own, 4 * V_DIM), BF)],
        place=False,
    )


def body(
    query,
    latent,
    rope_key,
    latent_gain,
    key_up,
    value_up,
    out_proj,
    tokens,
    moe_gain,
    routes,
    group_prob,
    expert_prob,
    w_gate,
    w_up,
    w_down,
):
    where = jnp.stack([lax.axis_index(n) for n in AXES]).astype(jnp.int32)
    return both_halves(
        where,
        query,
        latent,
        rope_key,
        latent_gain,
        key_up,
        value_up,
        out_proj,
        tokens,
        moe_gain,
        routes,
        group_prob,
        expert_prob,
        w_gate,
        w_up,
        w_down,
    )


def solution(mesh):
    ep, every = EP, AXES
    split = Mesh(mesh.devices.reshape(4, 2, 4, 2, 4), AXES)
    return jax.shard_map(
        body,
        mesh=split,
        in_specs=(
            P(ep, "x"),
            P(every, None),
            P(every, None),
            P(),
            P(None, "x"),
            P(None, "x"),
            P(),
            P(every, None),
            P(),
            P(every, None),
            P(every),
            P(every, None),
            P(ep, None, "x"),
            P(ep, None, "x"),
            P(ep, "x", None),
        ),
        out_specs=(P(every, None), P(every, None)),
        check_vma=False,
    )
```

```python
import jax
import jax.numpy as jnp
from jax import lax
from jax.experimental import pallas as pl
from jax.experimental.pallas import tpu as pltpu
from jax.sharding import Mesh, PartitionSpec as P


NOPE = 64
ROPE_DIM = 32
V_DIM = 64
QK_DIM = NOPE + ROPE_DIM
KV_ROWS = QK_DIM + V_DIM
CAP = 4
BF = jnp.bfloat16
F32 = jnp.float32

epsilon = 1e-06
rope_base = 10000.0
masked_value = -1e30
log2_e = 1.4426950408889634


AXES = ("zh", "zl", "y", "c", "x")
EP = AXES[:4]

SMEM_SPEC = pl.BlockSpec(memory_space=pltpu.SMEM)
VMEM_SPEC = pl.BlockSpec(memory_space=pltpu.VMEM)


def call(kernel, out_shape, arrays, where=None, scratch=(), limit=8 << 20, unplaced=(), place=True, free=False, **more):
    arrays = arrays if free else [
        pltpu.with_memory_space_constraint(a, pltpu.HBM if i in unplaced else pltpu.VMEM)
        for i, a in enumerate(arrays)
    ]
    specs = [VMEM_SPEC] * len(arrays)
    if where is not None:
        arrays, specs = [where] + arrays, [SMEM_SPEC] + specs
    single = not isinstance(out_shape, (list, tuple))
    if place:
        if single:
            out_shape = pltpu.VMEM(out_shape.shape, out_shape.dtype)
        else:
            out_shape = [pltpu.VMEM(s.shape, s.dtype) for s in out_shape]
    outs = VMEM_SPEC if single else [VMEM_SPEC] * len(out_shape)
    return pl.pallas_call(
        kernel,
        in_specs=specs,
        out_specs=more.pop("out_specs", outs),
        out_shape=out_shape,
        scratch_shapes=list(scratch),
        compiler_params=pltpu.CompilerParams(vmem_limit_bytes=limit),
        **more,
    )(*arrays)


def mm(a, b, dims=((1,), (0,))):
    return lax.dot_general(a, b, (dims, ((), ())), preferred_element_type=F32)


def shifted(value, axis, amount):
    n = lax.axis_size(axis)
    return lax.ppermute(value, axis, [(i, (i + amount) % n) for i in range(n)])


def trig(positions):
    half = ROPE_DIM // 2
    inverse = rope_base ** (-2.0 * jnp.arange(half, dtype=F32) / ROPE_DIM)
    angles = positions.astype(F32)[:, None] * inverse[None, :]
    return jnp.cos(angles), jnp.sin(angles)


def rms_scale(values, gain):
    widened = values.astype(F32)
    return widened * lax.rsqrt(jnp.mean(widened * widened, axis=-1, keepdims=True) + epsilon) * gain


def dispatch_kernel(
    tokens, gain, routes, group_prob, expert_prob, outgoing, shares_out, normed_s, mine_s
):
    step = pl.program_id(0)
    rows = tokens.shape[0]
    experts, cap, width = outgoing.shape
    slots = shares_out.shape[0]

    @pl.when(step == 0)
    def _():
        normed_s[...] = rms_scale(tokens[...], gain[...]).astype(BF)
        slot = lax.broadcasted_iota(jnp.int32, (slots, rows), 0)
        expert = slot // cap
        first = routes[0:1, :] == expert
        second = routes[1:2, :] == expert
        named = (first | second).astype(BF)
        before = lax.broadcasted_iota(jnp.int32, (rows, rows), 0) < lax.broadcasted_iota(
            jnp.int32, (rows, rows), 1
        )
        prior = mm(named, before.astype(BF))
        mine = (first | second) & (prior == (slot % cap).astype(F32))
        mine_s[...] = mine.astype(BF)
        probs = expert_prob[...]
        shares = group_prob[...] * probs / jnp.sum(probs, axis=0, keepdims=True)
        weights = jnp.where(first, shares[0:1, :], shares[1:2, :])
        weights = jnp.where(mine, weights, 0.0)
        high = weights.astype(BF)
        shares_out[:, 0:rows] = high
        shares_out[:, rows : 2 * rows] = (weights - high.astype(F32)).astype(BF)

    at = pl.multiple_of(step * experts * cap, experts * cap)
    chosen = mine_s[pl.ds(at, experts * cap), :]
    outgoing[...] = mm(chosen, normed_s[...]).reshape(experts, cap, width).astype(BF)


def dispatch(tokens, gain, routes, group_prob, expert_prob, experts):
    rows, width = tokens.shape
    block = pl.BlockSpec((experts // 4, CAP, width), lambda i: (i, 0, 0))
    return call(
        dispatch_kernel,
        (
            jax.ShapeDtypeStruct((experts, CAP, width), BF),
            jax.ShapeDtypeStruct((experts * CAP, 2 * rows), BF),
        ),
        [tokens, gain[None, :], routes.T, group_prob[None, :], expert_prob.T],
        unplaced=range(5),
        place=False,
        scratch=[pltpu.VMEM((rows, width), BF), pltpu.VMEM((experts * CAP, rows), BF)],
        grid=(4,),
        out_specs=[block, VMEM_SPEC],
    )


def hidden_kernel(rows_a, rows_b, w_gate, w_up, out, gate_s, up_s):
    half, span = out.shape[0] // 2, 512
    gate_s[...] = jnp.zeros(gate_s.shape, F32)
    up_s[...] = jnp.zeros(up_s.shape, F32)

    def add(step, _):
        cols = pl.ds(pl.multiple_of(step * span, span), span)
        for at, rows in ((0, rows_a), (half, rows_b)):
            got = rows[:, :, cols].reshape(half, span)
            gate_s[at : at + half, :] += mm(got, w_gate[cols, :])
            up_s[at : at + half, :] += mm(got, w_up[cols, :])
        return 0

    lax.fori_loop(0, w_gate.shape[0] // span, add, 0)
    gate = gate_s[...]
    out[...] = (gate / (1.0 + jnp.exp(-gate)) * up_s[...]).astype(BF)


def hidden_of(rows_a, rows_b, w_gate, w_up):
    shape = jax.ShapeDtypeStruct((2 * rows_a.shape[0] * CAP, w_gate.shape[1]), BF)
    scratch = [pltpu.VMEM(shape.shape, F32)] * 2
    return call(hidden_kernel, shape, [rows_a, rows_b, w_gate, w_up], scratch=scratch)


def stage_kernel(w0, w1, w2a, w2b, w3, out):
    at = 0
    for piece in (w0, w1, w2a, w2b, w3):
        out[at : at + piece.shape[0], :] = piece[...]
        at += piece.shape[0]


def down_kernel(h0, h1, h2, h3, weights, out):
    experts, cap, _ = out.shape
    rows = pl.ds(pl.multiple_of(pl.program_id(0) * experts * cap, experts * cap), experts * cap)
    hidden = jnp.concatenate([h[rows, :] for h in (h0, h1, h2, h3)], axis=1)
    out[...] = mm(hidden, weights[...]).reshape(out.shape).astype(BF)


def combine_kernel(returned, shares, out):
    rows = out.shape[0]
    got = returned[...].reshape(shares.shape[0], out.shape[1])
    both = mm(shares[...], got, ((0,), (0,)))
    out[...] = (both[:rows] + both[rows:]).astype(BF)


def both_halves(
    where,
    query,
    latent,
    rope_key,
    latent_gain,
    key_up,
    value_up,
    out_proj,
    tokens,
    moe_gain,
    routes,
    group_prob,
    expert_prob,
    w_gate,
    w_up,
    w_down,
):
    experts = lax.axis_size(EP)
    rows, width = tokens.shape
    w_gate, w_up, w_down = w_gate[0], w_up[0], w_down[0]
    down_left, down_right = shifted(w_down, "x", 1), shifted(w_down, "x", -1)
    units = w_down.shape[0] // 2
    cut_a, cut_b = down_left[:units], down_right[units:]
    down = [w_down, down_right]
    down += [shifted(cut_a, "x", 1), shifted(cut_b, "x", -1)]
    down = call(
        stage_kernel,
        jax.ShapeDtypeStruct((4 * w_down.shape[0], width), BF),
        down + [down_left],
        free=True,
    )
    outgoing, shares = dispatch(tokens, moe_gain, routes, group_prob, expert_prob, experts)
    arrived = lax.all_to_all(outgoing, EP, split_axis=0, concat_axis=0, tiled=True)
    queries, pair = query_and_pair(where, query, latent, rope_key, latent_gain, key_up, value_up)
    half = experts // 2
    a, b = arrived[:half], arrived[half:]
    left_a, right_b = shifted(a, "x", 1), shifted(b, "x", -1)
    left_b, right_a = shifted(b, "x", 1), shifted(a, "x", -1)
    far_a, far_b = shifted(left_a, "x", 1), shifted(right_b, "x", -1)
    parts = attend(where, queries, pair)
    hidden = [
        hidden_of(a, b, w_gate, w_up),
        shifted(hidden_of(left_a, left_b, w_gate, w_up), "x", -1),
        shifted(hidden_of(far_a, far_b, w_gate, w_up), "x", 2),
        shifted(hidden_of(right_a, right_b, w_gate, w_up), "x", 1),
    ]
    shape = jax.ShapeDtypeStruct((experts, CAP, width), BF)
    block = pl.BlockSpec((experts // 4, CAP, width), lambda i: (i, 0, 0))
    result = call(down_kernel, shape, hidden + [down], place=False, grid=(4,), out_specs=block)
    returned = lax.all_to_all(result, EP, split_axis=0, concat_axis=0, tiled=True)
    mixed = project(where, parts, out_proj, latent.shape[0])
    shape = jax.ShapeDtypeStruct((rows, width), BF)
    return mixed, call(combine_kernel, shape, [returned, shares], place=False)


def latent_kernel(latent, gain, rope_key, cosine, sine, out):
    width = latent.shape[1]
    half = ROPE_DIM // 2
    out[:, :width] = rms_scale(latent[...], gain[...]).astype(BF)
    rope = rope_key[...].astype(F32)
    crossed = jnp.concatenate([-rope[:, half:], rope[:, :half]], axis=1)
    out[:, width:] = (rope * cosine[...] + crossed * sine[...]).astype(BF)


def heads_kernel(
    where, l0, l1, l2, l3, key_up, value_up, query, cosine, sine, o0, o1, o2, o3, strip_s, heads
):
    latent = key_up.shape[0]
    own = l0.shape[0]
    count = heads.shape[0]
    half = ROPE_DIM // 2
    turned = query[...].astype(F32).T
    for h in range(count):
        at = h * QK_DIM
        a = turned[at + NOPE : at + NOPE + half]
        b = turned[at + NOPE + half : at + QK_DIM]
        heads[h, :NOPE, :] = turned[at : at + NOPE].astype(BF)
        heads[h, NOPE : NOPE + half, :] = (a * cosine[...] - b * sine[...]).astype(BF)
        heads[h, NOPE + half : QK_DIM, :] = (a * sine[...] + b * cosine[...]).astype(BF)
    for k, block in enumerate((l0, l1, l2, l3)):
        strip_s[k * own : (k + 1) * own, :] = block[...]
    got = strip_s[:, :latent]
    keys = mm(key_up[...], got, ((0,), (1,))).astype(BF)
    values = mm(value_up[...], got, ((0,), (1,))).astype(BF)
    eye = (
        lax.broadcasted_iota(jnp.int32, (ROPE_DIM, ROPE_DIM), 0)
        == lax.broadcasted_iota(jnp.int32, (ROPE_DIM, ROPE_DIM), 1)
    ).astype(BF)
    rope = mm(eye, strip_s[:, latent:], ((1,), (1,))).astype(BF)
    for h in range(count):
        heads[h, QK_DIM : QK_DIM + NOPE, :] = keys[h * NOPE : (h + 1) * NOPE]
        heads[h, QK_DIM + NOPE : 2 * QK_DIM, :] = rope
        heads[h, 2 * QK_DIM :, :] = values[h * V_DIM : (h + 1) * V_DIM]
    for k, out in enumerate((o0, o1, o2, o3)):
        out[...] = heads[lax.rem(where[0] + k, 4)]


def stack_kernel(b0, b1, b2, b3, out):
    for j, block in enumerate((b0, b1, b2, b3)):
        out[j] = block[QK_DIM:, :]


def attend_kernel(where, q0, q1, q2, q3, *refs):
    blocks, outs, (q_s, top_s, acc_s) = refs[:8], refs[8:12], refs[12:]
    zh, zl, y, c, x = (where[i] for i in range(5))
    strip = q0.shape[1]
    span = blocks[0].shape[2]
    factor = QK_DIM ** (-0.5) * log2_e
    for j, q in enumerate((q0, q1, q2, q3)):
        at = pl.multiple_of(lax.rem(zh - j + 4, 4) * strip, strip)
        q_s[pl.ds(at, strip), :] = q[:QK_DIM, :].astype(F32).T.astype(BF)
    top_s[...] = jnp.full(top_s.shape, masked_value, F32)
    acc_s[...] = jnp.zeros(acc_s.shape, F32)

    col = lax.broadcasted_iota(jnp.int32, (1, span), 1)
    col_zl = jnp.bitwise_xor(zl, col // strip)
    within = col % strip
    col_x = ((x - within // 32 + 4) % 4) * 32 + within % 32
    query_at = (zl * 8 + y * 2 + c) * strip + lax.broadcasted_iota(jnp.int32, (strip, 1), 0)
    ones = jnp.ones((V_DIM, span), BF)

    def advance(rows, parts, masks):
        q = q_s[rows, :]
        old = top_s[rows, :]
        scores = [mm(q, part[:QK_DIM, :]) for part in parts]
        if masks is not None:
            scores = [jnp.where(m, s, masked_value) for m, s in zip(masks, scores)]
        peak = scores[0]
        for s in scores[1:]:
            peak = jnp.maximum(peak, s)
        new = jnp.maximum(old, jnp.max(peak, axis=1, keepdims=True))
        top_s[rows, :] = new
        base = new[:, :1]
        total = acc_s[rows, :] * jnp.exp2((old - new) * factor)
        for s, part in zip(scores, parts):
            raised = jnp.exp2((s - base) * factor).astype(BF)
            extended = jnp.concatenate([part[QK_DIM:, :], ones], axis=0)
            total = total + mm(raised, extended, ((1,), (1,)))
        acc_s[rows, :] = total

    for m in range(2):
        group = blocks[4 * m : 4 * m + 4]
        masks = []
        for k in range(4):
            key_y = lax.rem(y - k + 4, 4)
            key_at = (col_zl * 8 + key_y * 2 + jnp.bitwise_xor(c, m)) * strip + col_x
            masks.append(key_at <= query_at)

        for g in range(4):
            from_zh = lax.rem(zh - g + 4, 4)
            parts = [block[from_zh] for block in group]
            advance(slice(g * strip, (g + 1) * strip), parts, masks)
            if g < 3:
                advance(slice((g + 1) * strip, 4 * strip), parts, None)
    total = acc_s[...]
    acc_s[:, :V_DIM] = total[:, :V_DIM] / total[:, V_DIM:]
    for j, out in enumerate(outs):
        at = pl.multiple_of(lax.rem(zh - j + 4, 4) * strip, strip)
        out[...] = acc_s[pl.ds(at, strip), :V_DIM].astype(BF)


def spread_kernel(where, a0, a1, a2, a3, o0, o1, o2, o3, heads, parts):
    for j, a in enumerate((a0, a1, a2, a3)):
        heads[lax.rem(where[0] + j, 4)] = a[...]
    beside = jnp.concatenate([heads[h] for h in range(4)], axis=1)
    parts[...] = beside.reshape(parts.shape)
    for k, out in enumerate((o0, o1, o2, o3)):
        out[...] = parts[lax.rem(where[4] + k, 4)]


def project_kernel(where, a0, a1, a2, a3, out_proj, out, parts):
    width = a0.shape[1]
    for k, a in enumerate((a0, a1, a2, a3)):
        parts[lax.rem(where[4] - k + 4, 4)] = a[...]
    total = mm(parts[0], out_proj[:width, :])
    for h in range(1, 4):
        total = total + mm(parts[h], out_proj[h * width : (h + 1) * width, :])
    out[...] = total.astype(BF)


def query_and_pair(where, query, latent, rope_key, latent_gain, key_up, value_up):
    strip = query.shape[0]
    own = latent.shape[0]
    query_start = (((where[0] * 2 + where[1]) * 4 + where[2]) * 2 + where[3]) * strip

    key_cos, key_sin = trig(query_start + where[4] * own + jnp.arange(own, dtype=jnp.int32))
    both = call(
        latent_kernel,
        jax.ShapeDtypeStruct((own, latent.shape[1] + ROPE_DIM), BF),
        [
            latent,
            latent_gain[None, :],
            rope_key,
            jnp.concatenate([key_cos, key_cos], axis=1),
            jnp.concatenate([key_sin, key_sin], axis=1),
        ],
        unplaced=range(3),
    )
    near = [both] + [shifted(both, "x", k) for k in range(1, 4)]
    cosine, sine = trig(query_start + jnp.arange(strip, dtype=jnp.int32))
    blocks = call(
        heads_kernel,
        [jax.ShapeDtypeStruct((QK_DIM + KV_ROWS, strip), BF)] * 4,
        near + [key_up, value_up, query, cosine.T, sine.T],
        where,
        scratch=[
            pltpu.VMEM((strip, both.shape[1]), BF),
            pltpu.VMEM((4, QK_DIM + KV_ROWS, strip), BF),
        ],
        unplaced=range(4, 7),
    )
    blocks = [blocks[0]] + [shifted(blocks[k], "zh", k) for k in range(1, 4)]
    shape = jax.ShapeDtypeStruct((4, KV_ROWS, strip), BF)
    mine = call(stack_kernel, shape, blocks)
    return blocks, jnp.concatenate([mine, shifted(mine, "zl", 1)], axis=2)


def attend(where, blocks, pair):
    strip = blocks[0].shape[1]
    column = [pair] + [shifted(pair, "y", k) for k in range(1, 4)]
    column = column + [shifted(part, "c", 1) for part in column]
    parts = call(
        attend_kernel,
        [jax.ShapeDtypeStruct((strip, V_DIM), BF)] * 4,
        blocks + column,
        where,
        [
            pltpu.VMEM((4 * strip, QK_DIM), BF),
            pltpu.VMEM((4 * strip, 128), F32),
            pltpu.VMEM((4 * strip, 128), F32),
        ],
    )
    return [parts[0]] + [shifted(parts[j], "zh", -j) for j in range(1, 4)]


def project(where, parts, out_proj, own):
    strip = parts[0].shape[0]
    parts = call(
        spread_kernel,
        [jax.ShapeDtypeStruct((own, 4 * V_DIM), BF)] * 4,
        parts,
        where,
        [pltpu.VMEM((4, strip, V_DIM), BF), pltpu.VMEM((4, own, 4 * V_DIM), BF)],
    )
    parts = [parts[0]] + [shifted(parts[k], "x", k) for k in range(1, 4)]
    return call(
        project_kernel,
        jax.ShapeDtypeStruct((own, out_proj.shape[1]), BF),
        parts + [out_proj],
        where,
        [pltpu.VMEM((4, own, 4 * V_DIM), BF)],
        place=False,
    )


def body(
    query,
    latent,
    rope_key,
    latent_gain,
    key_up,
    value_up,
    out_proj,
    tokens,
    moe_gain,
    routes,
    group_prob,
    expert_prob,
    w_gate,
    w_up,
    w_down,
):
    where = jnp.stack([lax.axis_index(n) for n in AXES]).astype(jnp.int32)
    return both_halves(
        where,
        query,
        latent,
        rope_key,
        latent_gain,
        key_up,
        value_up,
        out_proj,
        tokens,
        moe_gain,
        routes,
        group_prob,
        expert_prob,
        w_gate,
        w_up,
        w_down,
    )


def solution(mesh):
    ep, every = EP, AXES
    split = Mesh(mesh.devices.reshape(4, 2, 4, 2, 4), AXES)
    return jax.shard_map(
        body,
        mesh=split,
        in_specs=(
            P(ep, "x"),
            P(every, None),
            P(every, None),
            P(),
            P(None, "x"),
            P(None, "x"),
            P(),
            P(every, None),
            P(),
            P(every, None),
            P(every),
            P(every, None),
            P(ep, None, "x"),
            P(ep, None, "x"),
            P(ep, "x", None),
        ),
        out_specs=(P(every, None), P(every, None)),
        check_vma=False,
    )
```

```python
import functools

import jax
import jax.numpy as jnp
from jax import lax
from jax.experimental import pallas as pl
from jax.experimental.pallas import tpu as pltpu
from jax.sharding import Mesh, PartitionSpec as P


NOPE = 64
ROPE_DIM = 32
V_DIM = 64
QK_DIM = NOPE + ROPE_DIM
KV_ROWS = QK_DIM + V_DIM
CAP = 4
BF = jnp.bfloat16
F32 = jnp.float32

epsilon = 1e-06
rope_base = 10000.0
masked_value = -1e30
log2_e = 1.4426950408889634


AXES = ("zh", "zl", "y", "c", "x")
EP = AXES[:4]

SMEM_SPEC = pl.BlockSpec(memory_space=pltpu.SMEM)
VMEM_SPEC = pl.BlockSpec(memory_space=pltpu.VMEM)


def call(kernel, out_shape, arrays, where=None, scratch=(), limit=8 << 20, unplaced=(), place=True):
    arrays = [
        pltpu.with_memory_space_constraint(a, pltpu.HBM if i in unplaced else pltpu.VMEM)
        for i, a in enumerate(arrays)
    ]
    specs = [VMEM_SPEC] * len(arrays)
    if where is not None:
        arrays, specs = [where] + arrays, [SMEM_SPEC] + specs
    single = not isinstance(out_shape, (list, tuple))
    if place:
        if single:
            out_shape = pltpu.VMEM(out_shape.shape, out_shape.dtype)
        else:
            out_shape = [pltpu.VMEM(s.shape, s.dtype) for s in out_shape]
    return pl.pallas_call(
        kernel,
        in_specs=specs,
        out_specs=VMEM_SPEC if single else [VMEM_SPEC] * len(out_shape),
        out_shape=out_shape,
        scratch_shapes=list(scratch),
        compiler_params=pltpu.CompilerParams(vmem_limit_bytes=limit),
    )(*arrays)


def mm(a, b, dims=((1,), (0,))):
    return lax.dot_general(a, b, (dims, ((), ())), preferred_element_type=F32)


def shifted(value, axis, amount):
    n = lax.axis_size(axis)
    return lax.ppermute(value, axis, [(i, (i + amount) % n) for i in range(n)])


def trig(positions):
    half = ROPE_DIM // 2
    inverse = rope_base ** (-2.0 * jnp.arange(half, dtype=F32) / ROPE_DIM)
    angles = positions.astype(F32)[:, None] * inverse[None, :]
    return jnp.cos(angles), jnp.sin(angles)


def rms_scale(values, gain):
    widened = values.astype(F32)
    return widened * lax.rsqrt(jnp.mean(widened * widened, axis=-1, keepdims=True) + epsilon) * gain


def over_columns(width, span, work):
    def step(i, _):
        work(pl.ds(pl.multiple_of(i * span, span), span))
        return 0

    lax.fori_loop(0, width // span, step, 0)


def dispatch_kernel(
    tokens, gain, routes, group_prob, expert_prob, outgoing, shares_out, normed_s
):
    rows = tokens.shape[0]
    experts, cap, width = outgoing.shape
    slots = experts * cap
    normed_s[...] = rms_scale(tokens[...], gain[...]).astype(BF)
    slot = lax.broadcasted_iota(jnp.int32, (slots, rows), 0)
    expert = slot // cap
    first = routes[0:1, :] == expert
    second = routes[1:2, :] == expert
    named = (first | second).astype(BF)
    before = lax.broadcasted_iota(jnp.int32, (rows, rows), 0) < lax.broadcasted_iota(
        jnp.int32, (rows, rows), 1
    )
    prior = mm(named, before.astype(BF))
    mine = (first | second) & (prior == (slot % cap).astype(F32))
    chosen = mine.astype(BF)

    def send(cols):
        part = mm(chosen, normed_s[:, cols]).astype(BF)
        outgoing[:, :, cols] = part.reshape(experts, cap, part.shape[1])

    over_columns(width, 512, send)
    probs = expert_prob[...]
    shares = group_prob[...] * probs / jnp.sum(probs, axis=0, keepdims=True)
    weights = jnp.where(first, shares[0:1, :], shares[1:2, :])
    weights = jnp.where(mine, weights, 0.0)
    high = weights.astype(BF)
    shares_out[:, 0:rows] = high
    shares_out[:, rows : 2 * rows] = (weights - high.astype(F32)).astype(BF)


def dispatch(tokens, gain, routes, group_prob, expert_prob, experts):
    rows, width = tokens.shape
    return call(
        dispatch_kernel,
        (
            jax.ShapeDtypeStruct((experts, CAP, width), BF),
            jax.ShapeDtypeStruct((experts * CAP, 2 * rows), BF),
        ),
        [tokens, gain[None, :], routes.T, group_prob[None, :], expert_prob.T],
        unplaced=range(5),
        place=False,
        scratch=[pltpu.VMEM((rows, width), BF)],
    )


def hidden_kernel(rows_a, rows_b, w_gate, w_up, out, gate_s, up_s):
    half, span = out.shape[0] // 2, 512
    gate_s[...] = jnp.zeros(gate_s.shape, F32)
    up_s[...] = jnp.zeros(up_s.shape, F32)

    def add(step, _):
        cols = pl.ds(pl.multiple_of(step * span, span), span)
        for at, rows in ((0, rows_a), (half, rows_b)):
            got = rows[:, :, cols].reshape(half, span)
            gate_s[at : at + half, :] += mm(got, w_gate[cols, :])
            up_s[at : at + half, :] += mm(got, w_up[cols, :])
        return 0

    lax.fori_loop(0, w_gate.shape[0] // span, add, 0)
    gate = gate_s[...]
    out[...] = (gate / (1.0 + jnp.exp(-gate)) * up_s[...]).astype(BF)


def hidden_of(rows_a, rows_b, w_gate, w_up):
    shape = jax.ShapeDtypeStruct((2 * rows_a.shape[0] * CAP, w_gate.shape[1]), BF)
    scratch = [pltpu.VMEM(shape.shape, F32)] * 2
    return call(hidden_kernel, shape, [rows_a, rows_b, w_gate, w_up], scratch=scratch)


def down_kernel(h0, h1, h2, h3, w0, w1, w2a, w2b, w3, out):
    half = w2a.shape[0]
    experts, cap, width = out.shape
    own, right, far, left = h0[...], h1[...], h2[...], h3[...]

    def lower(cols):
        total = mm(own, w0[:, cols]) + mm(right, w1[:, cols]) + mm(left, w3[:, cols])
        total = total + mm(far[:, :half], w2a[:, cols]) + mm(far[:, half:], w2b[:, cols])
        out[:, :, cols] = total.astype(BF).reshape(experts, cap, total.shape[1])

    over_columns(width, 512, lower)


def combine_kernel(returned, shares, out):
    rows = out.shape[0]
    got = returned[...].reshape(shares.shape[0], out.shape[1])
    both = mm(shares[...], got, ((0,), (0,)))
    out[...] = (both[:rows] + both[rows:]).astype(BF)


def both_halves(
    where,
    query,
    latent,
    rope_key,
    latent_gain,
    key_up,
    value_up,
    out_proj,
    tokens,
    moe_gain,
    routes,
    group_prob,
    expert_prob,
    w_gate,
    w_up,
    w_down,
):
    experts = lax.axis_size(EP)
    rows, width = tokens.shape
    w_gate, w_up, w_down = w_gate[0], w_up[0], w_down[0]
    down_left, down_right = shifted(w_down, "x", 1), shifted(w_down, "x", -1)
    units = w_down.shape[0] // 2
    cut_a, cut_b = down_left[:units], down_right[units:]
    down_far = [shifted(cut_a, "x", 1), shifted(cut_b, "x", -1)]
    outgoing, shares = dispatch(tokens, moe_gain, routes, group_prob, expert_prob, experts)
    arrived = lax.all_to_all(outgoing, EP, split_axis=0, concat_axis=0, tiled=True)
    queries, pair = query_and_pair(where, query, latent, rope_key, latent_gain, key_up, value_up)
    half = experts // 2
    a, b = arrived[:half], arrived[half:]
    left_a, right_b = shifted(a, "x", 1), shifted(b, "x", -1)
    left_b, right_a = shifted(b, "x", 1), shifted(a, "x", -1)
    far_a, far_b = shifted(left_a, "x", 1), shifted(right_b, "x", -1)
    parts = attend(where, queries, pair)
    hidden = [
        hidden_of(a, b, w_gate, w_up),
        shifted(hidden_of(left_a, left_b, w_gate, w_up), "x", -1),
        shifted(hidden_of(far_a, far_b, w_gate, w_up), "x", 2),
        shifted(hidden_of(right_a, right_b, w_gate, w_up), "x", 1),
    ]
    shape = jax.ShapeDtypeStruct((experts, CAP, width), BF)
    down = [w_down, down_right] + down_far + [down_left]
    result = call(down_kernel, shape, hidden + down, place=False)
    returned = lax.all_to_all(result, EP, split_axis=0, concat_axis=0, tiled=True)
    mixed = project(where, parts, out_proj, latent.shape[0])
    shape = jax.ShapeDtypeStruct((rows, width), BF)
    return mixed, call(combine_kernel, shape, [returned, shares], place=False)


def latent_kernel(latent, gain, rope_key, cosine, sine, out):
    width = latent.shape[1]
    half = ROPE_DIM // 2
    out[:, :width] = rms_scale(latent[...], gain[...]).astype(BF)
    rope = rope_key[...].astype(F32)
    crossed = jnp.concatenate([-rope[:, half:], rope[:, :half]], axis=1)
    out[:, width:] = (rope * cosine[...] + crossed * sine[...]).astype(BF)


def heads_kernel(
    where, l0, l1, l2, l3, key_up, value_up, query, cosine, sine, o0, o1, o2, o3, strip_s, heads
):
    latent = key_up.shape[0]
    own = l0.shape[0]
    count = heads.shape[0]
    half = ROPE_DIM // 2
    turned = query[...].astype(F32).T
    for h in range(count):
        at = h * QK_DIM
        a = turned[at + NOPE : at + NOPE + half]
        b = turned[at + NOPE + half : at + QK_DIM]
        heads[h, :NOPE, :] = turned[at : at + NOPE].astype(BF)
        heads[h, NOPE : NOPE + half, :] = (a * cosine[...] - b * sine[...]).astype(BF)
        heads[h, NOPE + half : QK_DIM, :] = (a * sine[...] + b * cosine[...]).astype(BF)
    for k, block in enumerate((l0, l1, l2, l3)):
        strip_s[k * own : (k + 1) * own, :] = block[...]
    got = strip_s[:, :latent]
    keys = mm(key_up[...], got, ((0,), (1,))).astype(BF)
    values = mm(value_up[...], got, ((0,), (1,))).astype(BF)
    eye = (
        lax.broadcasted_iota(jnp.int32, (ROPE_DIM, ROPE_DIM), 0)
        == lax.broadcasted_iota(jnp.int32, (ROPE_DIM, ROPE_DIM), 1)
    ).astype(BF)
    rope = mm(eye, strip_s[:, latent:], ((1,), (1,))).astype(BF)
    for h in range(count):
        heads[h, QK_DIM : QK_DIM + NOPE, :] = keys[h * NOPE : (h + 1) * NOPE]
        heads[h, QK_DIM + NOPE : 2 * QK_DIM, :] = rope
        heads[h, 2 * QK_DIM :, :] = values[h * V_DIM : (h + 1) * V_DIM]
    for k, out in enumerate((o0, o1, o2, o3)):
        out[...] = heads[lax.rem(where[0] + k, 4)]


def stack_kernel(b0, b1, b2, b3, out):
    for j, block in enumerate((b0, b1, b2, b3)):
        out[j] = block[QK_DIM:, :]


def attend_kernel(where, *refs, columns, first):
    zh, zl, y, c, x = (where[i] for i in range(5))
    count = 2 * len(columns)
    if first:
        queries, blocks, (q_s, top_s, acc_s) = refs[:4], refs[4 : 4 + count], refs[4 + count :]
        strip = queries[0].shape[1]
        for j, q in enumerate(queries):
            at = pl.multiple_of(lax.rem(zh - j + 4, 4) * strip, strip)
            q_s[pl.ds(at, strip), :] = q[:QK_DIM, :].astype(F32).T.astype(BF)
        top_s[...] = jnp.full(top_s.shape, masked_value, F32)
        acc_s[...] = jnp.zeros(acc_s.shape, F32)
    else:
        q_s, top_in, acc_in = refs[:3]
        blocks, outs, (top_s, acc_s) = refs[3 : 3 + count], refs[3 + count : -2], refs[-2:]
        strip = outs[0].shape[0]
        top_s[...] = top_in[...]
        acc_s[...] = acc_in[...]
    span = blocks[0].shape[2]
    factor = QK_DIM ** (-0.5) * log2_e

    col = lax.broadcasted_iota(jnp.int32, (1, span), 1)
    col_zl = jnp.bitwise_xor(zl, col // strip)
    within = col % strip
    col_x = ((x - within // 32 + 4) % 4) * 32 + within % 32
    query_at = (zl * 8 + y * 2 + c) * strip + lax.broadcasted_iota(jnp.int32, (strip, 1), 0)
    ones = jnp.ones((V_DIM, span), BF)

    def advance(rows, parts, masks):
        q = q_s[rows, :]
        old = top_s[rows, :]
        scores = [mm(q, part[:QK_DIM, :]) for part in parts]
        if masks is not None:
            scores = [jnp.where(m, s, masked_value) for m, s in zip(masks, scores)]
        peak = scores[0]
        for s in scores[1:]:
            peak = jnp.maximum(peak, s)
        new = jnp.maximum(old, jnp.max(peak, axis=1, keepdims=True))
        top_s[rows, :] = new
        base = new[:, :1]
        total = acc_s[rows, :] * jnp.exp2((old - new) * factor)
        for s, part in zip(scores, parts):
            raised = jnp.exp2((s - base) * factor).astype(BF)
            extended = jnp.concatenate([part[QK_DIM:, :], ones], axis=0)
            total = total + mm(raised, extended, ((1,), (1,)))
        acc_s[rows, :] = total

    for m in range(2):
        group = blocks[m * len(columns) : (m + 1) * len(columns)]
        masks = []
        for k in columns:
            key_y = lax.rem(y - k + 4, 4)
            key_at = (col_zl * 8 + key_y * 2 + jnp.bitwise_xor(c, m)) * strip + col_x
            masks.append(key_at <= query_at)

        for g in range(4):
            from_zh = lax.rem(zh - g + 4, 4)
            parts = [block[from_zh] for block in group]
            advance(slice(g * strip, (g + 1) * strip), parts, masks)
            if g < 3:
                advance(slice((g + 1) * strip, 4 * strip), parts, None)
    if first:
        return
    total = acc_s[...]
    acc_s[:, :V_DIM] = total[:, :V_DIM] / total[:, V_DIM:]
    for j, out in enumerate(outs):
        at = pl.multiple_of(lax.rem(zh - j + 4, 4) * strip, strip)
        out[...] = acc_s[pl.ds(at, strip), :V_DIM].astype(BF)


def spread_kernel(where, a0, a1, a2, a3, o0, o1, o2, o3, heads, parts):
    for j, a in enumerate((a0, a1, a2, a3)):
        heads[lax.rem(where[0] + j, 4)] = a[...]
    beside = jnp.concatenate([heads[h] for h in range(4)], axis=1)
    parts[...] = beside.reshape(parts.shape)
    for k, out in enumerate((o0, o1, o2, o3)):
        out[...] = parts[lax.rem(where[4] + k, 4)]


def project_kernel(where, a0, a1, a2, a3, out_proj, out, parts):
    width = a0.shape[1]
    for k, a in enumerate((a0, a1, a2, a3)):
        parts[lax.rem(where[4] - k + 4, 4)] = a[...]
    total = mm(parts[0], out_proj[:width, :])
    for h in range(1, 4):
        total = total + mm(parts[h], out_proj[h * width : (h + 1) * width, :])
    out[...] = total.astype(BF)


def query_and_pair(where, query, latent, rope_key, latent_gain, key_up, value_up):
    strip = query.shape[0]
    own = latent.shape[0]
    query_start = (((where[0] * 2 + where[1]) * 4 + where[2]) * 2 + where[3]) * strip

    key_cos, key_sin = trig(query_start + where[4] * own + jnp.arange(own, dtype=jnp.int32))
    both = call(
        latent_kernel,
        jax.ShapeDtypeStruct((own, latent.shape[1] + ROPE_DIM), BF),
        [
            latent,
            latent_gain[None, :],
            rope_key,
            jnp.concatenate([key_cos, key_cos], axis=1),
            jnp.concatenate([key_sin, key_sin], axis=1),
        ],
        unplaced=range(3),
    )
    near = [both] + [shifted(both, "x", k) for k in range(1, 4)]
    cosine, sine = trig(query_start + jnp.arange(strip, dtype=jnp.int32))
    blocks = call(
        heads_kernel,
        [jax.ShapeDtypeStruct((QK_DIM + KV_ROWS, strip), BF)] * 4,
        near + [key_up, value_up, query, cosine.T, sine.T],
        where,
        scratch=[
            pltpu.VMEM((strip, both.shape[1]), BF),
            pltpu.VMEM((4, QK_DIM + KV_ROWS, strip), BF),
        ],
        unplaced=range(4, 7),
    )
    blocks = [blocks[0]] + [shifted(blocks[k], "zh", k) for k in range(1, 4)]
    shape = jax.ShapeDtypeStruct((4, KV_ROWS, strip), BF)
    mine = call(stack_kernel, shape, blocks)
    return blocks, jnp.concatenate([mine, shifted(mine, "zl", 1)], axis=2)


def attend(where, blocks, pair):
    strip = blocks[0].shape[1]
    column = [pair] + [shifted(pair, "y", k) for k in range(1, 4)]
    other = [shifted(part, "c", 1) for part in column]
    early, late = (0, 1, 3), (2,)
    state = call(
        functools.partial(attend_kernel, columns=early, first=True),
        [
            jax.ShapeDtypeStruct((4 * strip, QK_DIM), BF),
            jax.ShapeDtypeStruct((4 * strip, 128), F32),
            jax.ShapeDtypeStruct((4 * strip, 128), F32),
        ],
        blocks + [column[k] for k in early] + [other[k] for k in early],
        where,
    )
    parts = call(
        functools.partial(attend_kernel, columns=late, first=False),
        [jax.ShapeDtypeStruct((strip, V_DIM), BF)] * 4,
        list(state) + [column[k] for k in late] + [other[k] for k in late],
        where,
        [pltpu.VMEM((4 * strip, 128), F32), pltpu.VMEM((4 * strip, 128), F32)],
    )
    return [parts[0]] + [shifted(parts[j], "zh", -j) for j in range(1, 4)]


def project(where, parts, out_proj, own):
    strip = parts[0].shape[0]
    parts = call(
        spread_kernel,
        [jax.ShapeDtypeStruct((own, 4 * V_DIM), BF)] * 4,
        parts,
        where,
        [pltpu.VMEM((4, strip, V_DIM), BF), pltpu.VMEM((4, own, 4 * V_DIM), BF)],
    )
    parts = [parts[0]] + [shifted(parts[k], "x", k) for k in range(1, 4)]
    return call(
        project_kernel,
        jax.ShapeDtypeStruct((own, out_proj.shape[1]), BF),
        parts + [out_proj],
        where,
        [pltpu.VMEM((4, own, 4 * V_DIM), BF)],
        place=False,
    )


def body(
    query,
    latent,
    rope_key,
    latent_gain,
    key_up,
    value_up,
    out_proj,
    tokens,
    moe_gain,
    routes,
    group_prob,
    expert_prob,
    w_gate,
    w_up,
    w_down,
):
    where = jnp.stack([lax.axis_index(n) for n in AXES]).astype(jnp.int32)
    return both_halves(
        where,
        query,
        latent,
        rope_key,
        latent_gain,
        key_up,
        value_up,
        out_proj,
        tokens,
        moe_gain,
        routes,
        group_prob,
        expert_prob,
        w_gate,
        w_up,
        w_down,
    )


def solution(mesh):
    ep, every = EP, AXES
    split = Mesh(mesh.devices.reshape(4, 2, 4, 2, 4), AXES)
    return jax.shard_map(
        body,
        mesh=split,
        in_specs=(
            P(ep, "x"),
            P(every, None),
            P(every, None),
            P(),
            P(None, "x"),
            P(None, "x"),
            P(),
            P(every, None),
            P(),
            P(every, None),
            P(every),
            P(every, None),
            P(ep, None, "x"),
            P(ep, None, "x"),
            P(ep, "x", None),
        ),
        out_specs=(P(every, None), P(every, None)),
        check_vma=False,
    )
```

```python
import jax
import jax.numpy as jnp
from jax import lax
from jax.experimental import pallas as pl
from jax.experimental.pallas import tpu as pltpu
from jax.sharding import Mesh, PartitionSpec as P


NOPE = 64
ROPE_DIM = 32
V_DIM = 64
QK_DIM = NOPE + ROPE_DIM
KV_ROWS = QK_DIM + V_DIM
CAP = 4
BF = jnp.bfloat16
F32 = jnp.float32

epsilon = 1e-06
rope_base = 10000.0
masked_value = -1e30
log2_e = 1.4426950408889634


AXES = ("zh", "zl", "y", "c", "x")
EP = AXES[:4]

SMEM_SPEC = pl.BlockSpec(memory_space=pltpu.SMEM)
VMEM_SPEC = pl.BlockSpec(memory_space=pltpu.VMEM)


def call(kernel, out_shape, arrays, where=None, scratch=(), limit=8 << 20, unplaced=(), place=True):
    arrays = [
        pltpu.with_memory_space_constraint(a, pltpu.HBM if i in unplaced else pltpu.VMEM)
        for i, a in enumerate(arrays)
    ]
    specs = [VMEM_SPEC] * len(arrays)
    if where is not None:
        arrays, specs = [where] + arrays, [SMEM_SPEC] + specs
    single = not isinstance(out_shape, (list, tuple))
    if place:
        if single:
            out_shape = pltpu.VMEM(out_shape.shape, out_shape.dtype)
        else:
            out_shape = [pltpu.VMEM(s.shape, s.dtype) for s in out_shape]
    return pl.pallas_call(
        kernel,
        in_specs=specs,
        out_specs=VMEM_SPEC if single else [VMEM_SPEC] * len(out_shape),
        out_shape=out_shape,
        scratch_shapes=list(scratch),
        compiler_params=pltpu.CompilerParams(vmem_limit_bytes=limit),
    )(*arrays)


def mm(a, b, dims=((1,), (0,))):
    return lax.dot_general(a, b, (dims, ((), ())), preferred_element_type=F32)


def shifted(value, axis, amount):
    n = lax.axis_size(axis)
    return lax.ppermute(value, axis, [(i, (i + amount) % n) for i in range(n)])


def trig(positions):
    half = ROPE_DIM // 2
    inverse = rope_base ** (-2.0 * jnp.arange(half, dtype=F32) / ROPE_DIM)
    angles = positions.astype(F32)[:, None] * inverse[None, :]
    return jnp.cos(angles), jnp.sin(angles)


def rms_scale(values, gain):
    widened = values.astype(F32)
    return widened * lax.rsqrt(jnp.mean(widened * widened, axis=-1, keepdims=True) + epsilon) * gain


def dispatch_kernel(tokens, gain, routes, group_prob, expert_prob, outgoing, shares_out):
    rows = tokens.shape[0]
    experts, cap, width = outgoing.shape
    slots = experts * cap
    normed = rms_scale(tokens[...], gain[...]).astype(BF)
    slot = lax.broadcasted_iota(jnp.int32, (slots, rows), 0)
    expert = slot // cap
    first = routes[0:1, :] == expert
    second = routes[1:2, :] == expert
    named = (first | second).astype(BF)
    before = lax.broadcasted_iota(jnp.int32, (rows, rows), 0) < lax.broadcasted_iota(
        jnp.int32, (rows, rows), 1
    )
    prior = mm(named, before.astype(BF))
    mine = (first | second) & (prior == (slot % cap).astype(F32))
    outgoing[...] = mm(mine.astype(BF), normed).reshape(experts, cap, width).astype(BF)
    probs = expert_prob[...]
    shares = group_prob[...] * probs / jnp.sum(probs, axis=0, keepdims=True)
    weights = jnp.where(first, shares[0:1, :], shares[1:2, :])
    weights = jnp.where(mine, weights, 0.0)
    high = weights.astype(BF)
    shares_out[:, 0:rows] = high
    shares_out[:, rows : 2 * rows] = (weights - high.astype(F32)).astype(BF)


def dispatch(tokens, gain, routes, group_prob, expert_prob, experts):
    rows, width = tokens.shape
    return call(
        dispatch_kernel,
        (
            jax.ShapeDtypeStruct((experts, CAP, width), BF),
            jax.ShapeDtypeStruct((experts * CAP, 2 * rows), BF),
        ),
        [tokens, gain[None, :], routes.T, group_prob[None, :], expert_prob.T],
        unplaced=range(5),
    )


def hidden_kernel(rows_a, rows_b, w_gate, w_up, out, gate_s, up_s):
    half, span = out.shape[0] // 2, 512
    gate_s[...] = jnp.zeros(gate_s.shape, F32)
    up_s[...] = jnp.zeros(up_s.shape, F32)

    def add(step, _):
        cols = pl.ds(pl.multiple_of(step * span, span), span)
        for at, rows in ((0, rows_a), (half, rows_b)):
            got = rows[:, :, cols].reshape(half, span)
            gate_s[at : at + half, :] += mm(got, w_gate[cols, :])
            up_s[at : at + half, :] += mm(got, w_up[cols, :])
        return 0

    lax.fori_loop(0, w_gate.shape[0] // span, add, 0)
    gate = gate_s[...]
    out[...] = (gate / (1.0 + jnp.exp(-gate)) * up_s[...]).astype(BF)


def hidden_of(rows_a, rows_b, w_gate, w_up):
    shape = jax.ShapeDtypeStruct((2 * rows_a.shape[0] * CAP, w_gate.shape[1]), BF)
    scratch = [pltpu.VMEM(shape.shape, F32)] * 2
    return call(hidden_kernel, shape, [rows_a, rows_b, w_gate, w_up], scratch=scratch)


def down_kernel(h0, h1, h2, h3, w0, w1, w2a, w2b, w3, out):
    half = w2a.shape[0]
    total = mm(h0[...], w0[...]) + mm(h1[...], w1[...]) + mm(h3[...], w3[...])
    total = total + mm(h2[:, :half], w2a[...]) + mm(h2[:, half:], w2b[...])
    out[...] = total.reshape(out.shape).astype(BF)


def combine_kernel(returned, shares, out):
    rows = out.shape[0]
    got = returned[...].reshape(shares.shape[0], out.shape[1])
    both = mm(shares[...], got, ((0,), (0,)))
    out[...] = (both[:rows] + both[rows:]).astype(BF)


def both_halves(
    where,
    query,
    latent,
    rope_key,
    latent_gain,
    key_up,
    value_up,
    out_proj,
    tokens,
    moe_gain,
    routes,
    group_prob,
    expert_prob,
    w_gate,
    w_up,
    w_down,
):
    experts = lax.axis_size(EP)
    rows, width = tokens.shape
    w_gate, w_up, w_down = w_gate[0], w_up[0], w_down[0]
    down_left, down_right = shifted(w_down, "x", 1), shifted(w_down, "x", -1)
    units = w_down.shape[0] // 2
    cut_a, cut_b = down_left[:units], down_right[units:]
    down_far = [shifted(cut_a, "x", 1), shifted(cut_b, "x", -1)]
    outgoing, shares = dispatch(tokens, moe_gain, routes, group_prob, expert_prob, experts)
    arrived = lax.all_to_all(outgoing, EP, split_axis=0, concat_axis=0, tiled=True)
    queries, pair = query_and_pair(where, query, latent, rope_key, latent_gain, key_up, value_up)
    half = experts // 2
    a, b = arrived[:half], arrived[half:]
    left_a, right_b = shifted(a, "x", 1), shifted(b, "x", -1)
    left_b, right_a = shifted(b, "x", 1), shifted(a, "x", -1)
    far_a, far_b = shifted(left_a, "x", 1), shifted(right_b, "x", -1)
    parts = attend(where, queries, pair)
    hidden = [
        hidden_of(a, b, w_gate, w_up),
        shifted(hidden_of(left_a, left_b, w_gate, w_up), "x", -1),
        shifted(hidden_of(far_a, far_b, w_gate, w_up), "x", 2),
        shifted(hidden_of(right_a, right_b, w_gate, w_up), "x", 1),
    ]
    shape = jax.ShapeDtypeStruct((experts, CAP, width), BF)
    down = [w_down, down_right] + down_far + [down_left]
    result = call(down_kernel, shape, hidden + down)
    returned = lax.all_to_all(result, EP, split_axis=0, concat_axis=0, tiled=True)
    mixed = project(where, parts, out_proj, latent.shape[0])
    shape = jax.ShapeDtypeStruct((rows, width), BF)
    return mixed, call(combine_kernel, shape, [returned, shares], place=False)


def latent_kernel(latent, gain, rope_key, cosine, sine, out):
    width = latent.shape[1]
    half = ROPE_DIM // 2
    out[:, :width] = rms_scale(latent[...], gain[...]).astype(BF)
    rope = rope_key[...].astype(F32)
    crossed = jnp.concatenate([-rope[:, half:], rope[:, :half]], axis=1)
    out[:, width:] = (rope * cosine[...] + crossed * sine[...]).astype(BF)


def heads_kernel(
    where, l0, l1, l2, l3, key_up, value_up, query, cosine, sine, o0, o1, o2, o3, strip_s, heads
):
    latent = key_up.shape[0]
    own = l0.shape[0]
    count = heads.shape[0]
    half = ROPE_DIM // 2
    turned = query[...].astype(F32).T
    for h in range(count):
        at = h * QK_DIM
        a = turned[at + NOPE : at + NOPE + half]
        b = turned[at + NOPE + half : at + QK_DIM]
        heads[h, :NOPE, :] = turned[at : at + NOPE].astype(BF)
        heads[h, NOPE : NOPE + half, :] = (a * cosine[...] - b * sine[...]).astype(BF)
        heads[h, NOPE + half : QK_DIM, :] = (a * sine[...] + b * cosine[...]).astype(BF)
    for k, block in enumerate((l0, l1, l2, l3)):
        strip_s[k * own : (k + 1) * own, :] = block[...]
    got = strip_s[:, :latent]
    keys = mm(key_up[...], got, ((0,), (1,))).astype(BF)
    values = mm(value_up[...], got, ((0,), (1,))).astype(BF)
    eye = (
        lax.broadcasted_iota(jnp.int32, (ROPE_DIM, ROPE_DIM), 0)
        == lax.broadcasted_iota(jnp.int32, (ROPE_DIM, ROPE_DIM), 1)
    ).astype(BF)
    rope = mm(eye, strip_s[:, latent:], ((1,), (1,))).astype(BF)
    for h in range(count):
        heads[h, QK_DIM : QK_DIM + NOPE, :] = keys[h * NOPE : (h + 1) * NOPE]
        heads[h, QK_DIM + NOPE : 2 * QK_DIM, :] = rope
        heads[h, 2 * QK_DIM :, :] = values[h * V_DIM : (h + 1) * V_DIM]
    for k, out in enumerate((o0, o1, o2, o3)):
        out[...] = heads[lax.rem(where[0] + k, 4)]


def stack_kernel(b0, b1, b2, b3, out):
    for j, block in enumerate((b0, b1, b2, b3)):
        out[j] = block[QK_DIM:, :]


def attend_kernel(where, q0, q1, q2, q3, *refs):
    blocks, outs, (q_s, top_s, acc_s) = refs[:8], refs[8:12], refs[12:]
    zh, zl, y, c, x = (where[i] for i in range(5))
    strip = q0.shape[1]
    span = blocks[0].shape[2]
    factor = QK_DIM ** (-0.5) * log2_e
    for j, q in enumerate((q0, q1, q2, q3)):
        at = pl.multiple_of(lax.rem(zh - j + 4, 4) * strip, strip)
        q_s[pl.ds(at, strip), :] = q[:QK_DIM, :].astype(F32).T.astype(BF)
    top_s[...] = jnp.full(top_s.shape, masked_value, F32)
    acc_s[...] = jnp.zeros(acc_s.shape, F32)

    col = lax.broadcasted_iota(jnp.int32, (1, span), 1)
    col_zl = jnp.bitwise_xor(zl, col // strip)
    within = col % strip
    col_x = ((x - within // 32 + 4) % 4) * 32 + within % 32
    query_at = (zl * 8 + y * 2 + c) * strip + lax.broadcasted_iota(jnp.int32, (strip, 1), 0)
    ones = jnp.ones((V_DIM, span), BF)

    def advance(rows, parts, masks):
        q = q_s[rows, :]
        old = top_s[rows, :]
        scores = [mm(q, part[:QK_DIM, :]) for part in parts]
        if masks is not None:
            scores = [jnp.where(m, s, masked_value) for m, s in zip(masks, scores)]
        peak = scores[0]
        for s in scores[1:]:
            peak = jnp.maximum(peak, s)
        new = jnp.maximum(old, jnp.max(peak, axis=1, keepdims=True))
        top_s[rows, :] = new
        base = new[:, :1]
        total = acc_s[rows, :] * jnp.exp2((old - new) * factor)
        for s, part in zip(scores, parts):
            raised = jnp.exp2((s - base) * factor).astype(BF)
            extended = jnp.concatenate([part[QK_DIM:, :], ones], axis=0)
            total = total + mm(raised, extended, ((1,), (1,)))
        acc_s[rows, :] = total

    for m in range(2):
        group = blocks[4 * m : 4 * m + 4]
        masks = []
        for k in range(4):
            key_y = lax.rem(y - k + 4, 4)
            key_at = (col_zl * 8 + key_y * 2 + jnp.bitwise_xor(c, m)) * strip + col_x
            masks.append(key_at <= query_at)

        for g in range(4):
            from_zh = lax.rem(zh - g + 4, 4)
            parts = [block[from_zh] for block in group]
            advance(slice(g * strip, (g + 1) * strip), parts, masks)
            if g < 3:
                advance(slice((g + 1) * strip, 4 * strip), parts, None)
    total = acc_s[...]
    acc_s[:, :V_DIM] = total[:, :V_DIM] / total[:, V_DIM:]
    own = strip // 4
    for k, out in enumerate(outs):
        for g in range(4):
            at = pl.multiple_of(g * strip + lax.rem(x + k, 4) * own, own)
            out[g * own : (g + 1) * own, :] = acc_s[pl.ds(at, own), :V_DIM].astype(BF)


def spread_kernel(where, a0, a1, a2, a3, o0, o1, o2, o3, heads, parts):
    for k, a in enumerate((a0, a1, a2, a3)):
        heads[lax.rem(where[4] - k + 4, 4)] = a[...]
    beside = jnp.concatenate([heads[h] for h in range(4)], axis=1)
    parts[...] = beside.reshape(parts.shape)
    for j, out in enumerate((o0, o1, o2, o3)):
        out[...] = parts[lax.rem(where[0] + j, 4)]


def project_kernel(where, a0, a1, a2, a3, out_proj, out, parts):
    for j, a in enumerate((a0, a1, a2, a3)):
        parts[lax.rem(where[0] - j + 4, 4)] = a[...]
    pieces = [parts[h % 4, :, h // 4 * V_DIM : (h // 4 + 1) * V_DIM] for h in range(16)]
    out[...] = mm(jnp.concatenate(pieces, axis=1), out_proj[...]).astype(BF)


def query_and_pair(where, query, latent, rope_key, latent_gain, key_up, value_up):
    strip = query.shape[0]
    own = latent.shape[0]
    query_start = (((where[0] * 2 + where[1]) * 4 + where[2]) * 2 + where[3]) * strip

    key_cos, key_sin = trig(query_start + where[4] * own + jnp.arange(own, dtype=jnp.int32))
    both = call(
        latent_kernel,
        jax.ShapeDtypeStruct((own, latent.shape[1] + ROPE_DIM), BF),
        [
            latent,
            latent_gain[None, :],
            rope_key,
            jnp.concatenate([key_cos, key_cos], axis=1),
            jnp.concatenate([key_sin, key_sin], axis=1),
        ],
        unplaced=range(3),
    )
    near = [both] + [shifted(both, "x", k) for k in range(1, 4)]
    cosine, sine = trig(query_start + jnp.arange(strip, dtype=jnp.int32))
    blocks = call(
        heads_kernel,
        [jax.ShapeDtypeStruct((QK_DIM + KV_ROWS, strip), BF)] * 4,
        near + [key_up, value_up, query, cosine.T, sine.T],
        where,
        scratch=[
            pltpu.VMEM((strip, both.shape[1]), BF),
            pltpu.VMEM((4, QK_DIM + KV_ROWS, strip), BF),
        ],
        unplaced=range(4, 7),
    )
    blocks = [blocks[0]] + [shifted(blocks[k], "zh", k) for k in range(1, 4)]
    shape = jax.ShapeDtypeStruct((4, KV_ROWS, strip), BF)
    mine = call(stack_kernel, shape, blocks)
    return blocks, jnp.concatenate([mine, shifted(mine, "zl", 1)], axis=2)


def attend(where, blocks, pair):
    strip = blocks[0].shape[1]
    column = [pair] + [shifted(pair, "y", k) for k in range(1, 4)]
    column = column + [shifted(part, "c", 1) for part in column]
    parts = call(
        attend_kernel,
        [jax.ShapeDtypeStruct((strip, V_DIM), BF)] * 4,
        blocks + column,
        where,
        [
            pltpu.VMEM((4 * strip, QK_DIM), BF),
            pltpu.VMEM((4 * strip, 128), F32),
            pltpu.VMEM((4 * strip, 128), F32),
        ],
    )
    return [parts[0]] + [shifted(parts[k], "x", k) for k in range(1, 4)]


def project(where, parts, out_proj, own):
    strip = parts[0].shape[0]
    parts = call(
        spread_kernel,
        [jax.ShapeDtypeStruct((own, 4 * V_DIM), BF)] * 4,
        parts,
        where,
        [pltpu.VMEM((4, strip, V_DIM), BF), pltpu.VMEM((4, own, 4 * V_DIM), BF)],
    )
    parts = [parts[0]] + [shifted(parts[j], "zh", j) for j in range(1, 4)]
    return call(
        project_kernel,
        jax.ShapeDtypeStruct((own, out_proj.shape[1]), BF),
        parts + [out_proj],
        where,
        [pltpu.VMEM((4, own, 4 * V_DIM), BF)],
        place=False,
    )


def body(
    query,
    latent,
    rope_key,
    latent_gain,
    key_up,
    value_up,
    out_proj,
    tokens,
    moe_gain,
    routes,
    group_prob,
    expert_prob,
    w_gate,
    w_up,
    w_down,
):
    where = jnp.stack([lax.axis_index(n) for n in AXES]).astype(jnp.int32)
    return both_halves(
        where,
        query,
        latent,
        rope_key,
        latent_gain,
        key_up,
        value_up,
        out_proj,
        tokens,
        moe_gain,
        routes,
        group_prob,
        expert_prob,
        w_gate,
        w_up,
        w_down,
    )


def solution(mesh):
    ep, every = EP, AXES
    split = Mesh(mesh.devices.reshape(4, 2, 4, 2, 4), AXES)
    return jax.shard_map(
        body,
        mesh=split,
        in_specs=(
            P(ep, "x"),
            P(every, None),
            P(every, None),
            P(),
            P(None, "x"),
            P(None, "x"),
            P(),
            P(every, None),
            P(),
            P(every, None),
            P(every),
            P(every, None),
            P(ep, None, "x"),
            P(ep, None, "x"),
            P(ep, "x", None),
        ),
        out_specs=(P(every, None), P(every, None)),
        check_vma=False,
    )
```

```python
import jax
import jax.numpy as jnp
from jax import lax
from jax.experimental import pallas as pl
from jax.experimental.pallas import tpu as pltpu
from jax.sharding import Mesh, PartitionSpec as P


NOPE = 64
ROPE_DIM = 32
V_DIM = 64
QK_DIM = NOPE + ROPE_DIM
KV_ROWS = QK_DIM + V_DIM
CAP = 4
BF = jnp.bfloat16
F32 = jnp.float32

epsilon = 1e-06
rope_base = 10000.0
masked_value = -1e30
log2_e = 1.4426950408889634


AXES = ("zh", "zl", "y", "c", "x")
EP = AXES[:4]

SMEM_SPEC = pl.BlockSpec(memory_space=pltpu.SMEM)
VMEM_SPEC = pl.BlockSpec(memory_space=pltpu.VMEM)


def call(kernel, out_shape, arrays, where=None, scratch=(), limit=8 << 20, unplaced=(), place=pltpu.VMEM):
    arrays = [
        pltpu.with_memory_space_constraint(a, pltpu.HBM if i in unplaced else pltpu.VMEM)
        for i, a in enumerate(arrays)
    ]
    specs = [VMEM_SPEC] * len(arrays)
    if where is not None:
        arrays, specs = [where] + arrays, [SMEM_SPEC] + specs
    single = not isinstance(out_shape, (list, tuple))
    if place is not None:
        if single:
            out_shape = place(out_shape.shape, out_shape.dtype)
        else:
            out_shape = [place(s.shape, s.dtype) for s in out_shape]
    return pl.pallas_call(
        kernel,
        in_specs=specs,
        out_specs=VMEM_SPEC if single else [VMEM_SPEC] * len(out_shape),
        out_shape=out_shape,
        scratch_shapes=list(scratch),
        compiler_params=pltpu.CompilerParams(vmem_limit_bytes=limit),
    )(*arrays)


def mm(a, b, dims=((1,), (0,))):
    return lax.dot_general(a, b, (dims, ((), ())), preferred_element_type=F32)


def shifted(value, axis, amount):
    n = lax.axis_size(axis)
    return lax.ppermute(value, axis, [(i, (i + amount) % n) for i in range(n)])


def paired(value, mate):
    n = lax.axis_size("x")
    return lax.ppermute(value, "x", [(i, mate(i)) for i in range(n)])


def weight_mate(i):
    return i ^ 1


def row_mate(i):
    return 3 - i


def trig(positions):
    half = ROPE_DIM // 2
    inverse = rope_base ** (-2.0 * jnp.arange(half, dtype=F32) / ROPE_DIM)
    angles = positions.astype(F32)[:, None] * inverse[None, :]
    return jnp.cos(angles), jnp.sin(angles)


def rms_scale(values, gain):
    widened = values.astype(F32)
    return widened * lax.rsqrt(jnp.mean(widened * widened, axis=-1, keepdims=True) + epsilon) * gain


def dispatch_kernel(tokens, gain, routes, group_prob, expert_prob, outgoing, shares_out):
    rows = tokens.shape[0]
    experts, cap, width = outgoing.shape
    slots = experts * cap
    normed = rms_scale(tokens[...], gain[...]).astype(BF)
    slot = lax.broadcasted_iota(jnp.int32, (slots, rows), 0)
    expert = slot // cap
    first = routes[0:1, :] == expert
    second = routes[1:2, :] == expert
    named = (first | second).astype(BF)
    before = lax.broadcasted_iota(jnp.int32, (rows, rows), 0) < lax.broadcasted_iota(
        jnp.int32, (rows, rows), 1
    )
    prior = mm(named, before.astype(BF))
    mine = (first | second) & (prior == (slot % cap).astype(F32))
    outgoing[...] = mm(mine.astype(BF), normed).reshape(experts, cap, width).astype(BF)
    probs = expert_prob[...]
    shares = group_prob[...] * probs / jnp.sum(probs, axis=0, keepdims=True)
    weights = jnp.where(first, shares[0:1, :], shares[1:2, :])
    weights = jnp.where(mine, weights, 0.0)
    high = weights.astype(BF)
    shares_out[:, 0:rows] = high
    shares_out[:, rows : 2 * rows] = (weights - high.astype(F32)).astype(BF)


def dispatch(tokens, gain, routes, group_prob, expert_prob, experts):
    rows, width = tokens.shape
    return call(
        dispatch_kernel,
        (
            jax.ShapeDtypeStruct((experts, CAP, width), BF),
            jax.ShapeDtypeStruct((experts * CAP, 2 * rows), BF),
        ),
        [tokens, gain[None, :], routes.T, group_prob[None, :], expert_prob.T],
        unplaced=range(5),
        place=pltpu.HBM,
    )


def hidden_kernel(rows, gate_a, up_a, gate_b, up_b, out, gate_s, up_s):
    count, span, units = out.shape[0], 1024, gate_a.shape[1]
    gate_s[...] = jnp.zeros(gate_s.shape, F32)
    up_s[...] = jnp.zeros(up_s.shape, F32)

    def add(step, _):
        cols = pl.ds(pl.multiple_of(step * span, span), span)
        got = rows[:, :, cols].reshape(count, span)
        for at, gate, up in ((0, gate_a, up_a), (units, gate_b, up_b)):
            gate_s[:, at : at + units] += mm(got, gate[cols, :])
            up_s[:, at : at + units] += mm(got, up[cols, :])
        return 0

    lax.fori_loop(0, gate_a.shape[0] // span, add, 0)
    gate = gate_s[...]
    out[...] = (gate / (1.0 + jnp.exp(-gate)) * up_s[...]).astype(BF)


def hidden_of(rows, weights):
    shape = jax.ShapeDtypeStruct((rows.shape[0] * CAP, 2 * weights[0].shape[1]), BF)
    scratch = [pltpu.VMEM(shape.shape, F32)] * 2
    return call(hidden_kernel, shape, [rows] + weights, scratch=scratch)


def down_kernel(own, mate, w0, w1, w2, w3, out):
    units = w0.shape[0]
    total = mm(own[:, :units], w0[...]) + mm(own[:, units:], w1[...])
    total = total + mm(mate[:, :units], w2[...]) + mm(mate[:, units:], w3[...])
    out[...] = total.astype(BF).reshape(out.shape)


def combine_kernel(returned, shares, out):
    rows = out.shape[0]
    got = returned[...].reshape(shares.shape[0], out.shape[1])
    both = mm(shares[...], got, ((0,), (0,)))
    out[...] = (both[:rows] + both[rows:]).astype(BF)


def both_halves(
    where,
    query,
    latent,
    rope_key,
    latent_gain,
    key_up,
    value_up,
    out_proj,
    tokens,
    moe_gain,
    routes,
    group_prob,
    expert_prob,
    w_gate,
    w_up,
    w_down,
):
    experts = lax.axis_size(EP)
    rows, width = tokens.shape
    w_gate, w_up, w_down = w_gate[0], w_up[0], w_down[0]
    down_w, down_r = paired(w_down, weight_mate), paired(w_down, row_mate)
    down_rw = paired(down_w, row_mate)
    gate_w, up_w = paired(w_gate, weight_mate), paired(w_up, weight_mate)
    weights = [w_gate, w_up, gate_w, up_w]
    outgoing, shares = dispatch(tokens, moe_gain, routes, group_prob, expert_prob, experts)
    arrived = lax.all_to_all(outgoing, EP, split_axis=0, concat_axis=0, tiled=True)
    queries, pair = query_and_pair(where, query, latent, rope_key, latent_gain, key_up, value_up)
    mate_rows = paired(arrived, row_mate)
    parts = attend(where, queries, pair)
    mate_hidden = paired(hidden_of(mate_rows, weights), row_mate)
    own_hidden = hidden_of(arrived, weights)
    shape = jax.ShapeDtypeStruct((experts, CAP, width), BF)
    arrays = [own_hidden, mate_hidden, w_down, down_w, down_r, down_rw]
    result = call(down_kernel, shape, arrays, place=pltpu.HBM)
    returned = lax.all_to_all(result, EP, split_axis=0, concat_axis=0, tiled=True)
    mixed = project(where, parts, out_proj, latent.shape[0])
    shape = jax.ShapeDtypeStruct((rows, width), BF)
    return mixed, call(combine_kernel, shape, [returned, shares], place=None)


def latent_kernel(latent, gain, rope_key, cosine, sine, out):
    width = latent.shape[1]
    half = ROPE_DIM // 2
    out[:, :width] = rms_scale(latent[...], gain[...]).astype(BF)
    rope = rope_key[...].astype(F32)
    crossed = jnp.concatenate([-rope[:, half:], rope[:, :half]], axis=1)
    out[:, width:] = (rope * cosine[...] + crossed * sine[...]).astype(BF)


def heads_kernel(
    where, l0, l1, l2, l3, key_up, value_up, query, cosine, sine, o0, o1, o2, o3, strip_s, heads
):
    latent = key_up.shape[0]
    own = l0.shape[0]
    count = heads.shape[0]
    half = ROPE_DIM // 2
    turned = query[...].astype(F32).T
    for h in range(count):
        at = h * QK_DIM
        a = turned[at + NOPE : at + NOPE + half]
        b = turned[at + NOPE + half : at + QK_DIM]
        heads[h, :NOPE, :] = turned[at : at + NOPE].astype(BF)
        heads[h, NOPE : NOPE + half, :] = (a * cosine[...] - b * sine[...]).astype(BF)
        heads[h, NOPE + half : QK_DIM, :] = (a * sine[...] + b * cosine[...]).astype(BF)
    for k, block in enumerate((l0, l1, l2, l3)):
        strip_s[k * own : (k + 1) * own, :] = block[...]
    got = strip_s[:, :latent]
    keys = mm(key_up[...], got, ((0,), (1,))).astype(BF)
    values = mm(value_up[...], got, ((0,), (1,))).astype(BF)
    eye = (
        lax.broadcasted_iota(jnp.int32, (ROPE_DIM, ROPE_DIM), 0)
        == lax.broadcasted_iota(jnp.int32, (ROPE_DIM, ROPE_DIM), 1)
    ).astype(BF)
    rope = mm(eye, strip_s[:, latent:], ((1,), (1,))).astype(BF)
    for h in range(count):
        heads[h, QK_DIM : QK_DIM + NOPE, :] = keys[h * NOPE : (h + 1) * NOPE]
        heads[h, QK_DIM + NOPE : 2 * QK_DIM, :] = rope
        heads[h, 2 * QK_DIM :, :] = values[h * V_DIM : (h + 1) * V_DIM]
    for k, out in enumerate((o0, o1, o2, o3)):
        out[...] = heads[lax.rem(where[0] + k, 4)]


def stack_kernel(b0, b1, b2, b3, out):
    for j, block in enumerate((b0, b1, b2, b3)):
        out[j] = block[QK_DIM:, :]


def attend_kernel(where, q0, q1, q2, q3, *refs):
    blocks, outs, (q_s, top_s, acc_s) = refs[:8], refs[8:12], refs[12:]
    zh, zl, y, c, x = (where[i] for i in range(5))
    strip = q0.shape[1]
    span = blocks[0].shape[2]
    factor = QK_DIM ** (-0.5) * log2_e
    for j, q in enumerate((q0, q1, q2, q3)):
        at = pl.multiple_of(lax.rem(zh - j + 4, 4) * strip, strip)
        q_s[pl.ds(at, strip), :] = q[:QK_DIM, :].astype(F32).T.astype(BF)
    top_s[...] = jnp.full(top_s.shape, masked_value, F32)
    acc_s[...] = jnp.zeros(acc_s.shape, F32)

    col = lax.broadcasted_iota(jnp.int32, (1, span), 1)
    col_zl = jnp.bitwise_xor(zl, col // strip)
    within = col % strip
    col_x = ((x - within // 32 + 4) % 4) * 32 + within % 32
    query_at = (zl * 8 + y * 2 + c) * strip + lax.broadcasted_iota(jnp.int32, (strip, 1), 0)
    ones = jnp.ones((V_DIM, span), BF)

    def advance(rows, parts, masks):
        q = q_s[rows, :]
        old = top_s[rows, :]
        scores = [mm(q, part[:QK_DIM, :]) for part in parts]
        if masks is not None:
            scores = [jnp.where(m, s, masked_value) for m, s in zip(masks, scores)]
        peak = scores[0]
        for s in scores[1:]:
            peak = jnp.maximum(peak, s)
        new = jnp.maximum(old, jnp.max(peak, axis=1, keepdims=True))
        top_s[rows, :] = new
        base = new[:, :1]
        total = acc_s[rows, :] * jnp.exp2((old - new) * factor)
        for s, part in zip(scores, parts):
            raised = jnp.exp2((s - base) * factor).astype(BF)
            extended = jnp.concatenate([part[QK_DIM:, :], ones], axis=0)
            total = total + mm(raised, extended, ((1,), (1,)))
        acc_s[rows, :] = total

    for m in range(2):
        group = blocks[4 * m : 4 * m + 4]
        masks = []
        for k in range(4):
            key_y = lax.rem(y - k + 4, 4)
            key_at = (col_zl * 8 + key_y * 2 + jnp.bitwise_xor(c, m)) * strip + col_x
            masks.append(key_at <= query_at)

        for g in range(4):
            from_zh = lax.rem(zh - g + 4, 4)
            parts = [block[from_zh] for block in group]
            advance(slice(g * strip, (g + 1) * strip), parts, masks)
            if g < 3:
                advance(slice((g + 1) * strip, 4 * strip), parts, None)
    total = acc_s[...]
    acc_s[:, :V_DIM] = total[:, :V_DIM] / total[:, V_DIM:]
    own = strip // 4
    for k, out in enumerate(outs):
        for g in range(4):
            at = pl.multiple_of(g * strip + lax.rem(x + k, 4) * own, own)
            out[g * own : (g + 1) * own, :] = acc_s[pl.ds(at, own), :V_DIM].astype(BF)


def spread_kernel(where, a0, a1, a2, a3, o0, o1, o2, o3, heads, parts):
    for k, a in enumerate((a0, a1, a2, a3)):
        heads[lax.rem(where[4] - k + 4, 4)] = a[...]
    beside = jnp.concatenate([heads[h] for h in range(4)], axis=1)
    parts[...] = beside.reshape(parts.shape)
    for j, out in enumerate((o0, o1, o2, o3)):
        out[...] = parts[lax.rem(where[0] + j, 4)]


def project_kernel(where, a0, a1, a2, a3, out_proj, out, parts, rows):
    @pl.when(pl.program_id(0) == 0)
    def _():
        for j, a in enumerate((a0, a1, a2, a3)):
            parts[lax.rem(where[0] - j + 4, 4)] = a[...]
        pieces = [parts[h % 4, :, h // 4 * V_DIM : (h // 4 + 1) * V_DIM] for h in range(16)]
        rows[...] = jnp.concatenate(pieces, axis=1)

    out[...] = mm(rows[...], out_proj[...]).astype(BF)


def query_and_pair(where, query, latent, rope_key, latent_gain, key_up, value_up):
    strip = query.shape[0]
    own = latent.shape[0]
    query_start = (((where[0] * 2 + where[1]) * 4 + where[2]) * 2 + where[3]) * strip

    key_cos, key_sin = trig(query_start + where[4] * own + jnp.arange(own, dtype=jnp.int32))
    both = call(
        latent_kernel,
        jax.ShapeDtypeStruct((own, latent.shape[1] + ROPE_DIM), BF),
        [
            latent,
            latent_gain[None, :],
            rope_key,
            jnp.concatenate([key_cos, key_cos], axis=1),
            jnp.concatenate([key_sin, key_sin], axis=1),
        ],
        unplaced=range(3),
    )
    near = [both] + [shifted(both, "x", k) for k in range(1, 4)]
    cosine, sine = trig(query_start + jnp.arange(strip, dtype=jnp.int32))
    blocks = call(
        heads_kernel,
        [jax.ShapeDtypeStruct((QK_DIM + KV_ROWS, strip), BF)] * 4,
        near + [key_up, value_up, query, cosine.T, sine.T],
        where,
        scratch=[
            pltpu.VMEM((strip, both.shape[1]), BF),
            pltpu.VMEM((4, QK_DIM + KV_ROWS, strip), BF),
        ],
        unplaced=range(4, 7),
    )
    blocks = [blocks[0]] + [shifted(blocks[k], "zh", k) for k in range(1, 4)]
    shape = jax.ShapeDtypeStruct((4, KV_ROWS, strip), BF)
    mine = call(stack_kernel, shape, blocks)
    return blocks, jnp.concatenate([mine, shifted(mine, "zl", 1)], axis=2)


def attend(where, blocks, pair):
    strip = blocks[0].shape[1]
    column = [pair] + [shifted(pair, "y", k) for k in range(1, 4)]
    column = column + [shifted(part, "c", 1) for part in column]
    parts = call(
        attend_kernel,
        [jax.ShapeDtypeStruct((strip, V_DIM), BF)] * 4,
        blocks + column,
        where,
        [
            pltpu.VMEM((4 * strip, QK_DIM), BF),
            pltpu.VMEM((4 * strip, 128), F32),
            pltpu.VMEM((4 * strip, 128), F32),
        ],
    )
    return [parts[0]] + [shifted(parts[k], "x", k) for k in range(1, 4)]


def project(where, parts, out_proj, own):
    strip = parts[0].shape[0]
    parts = call(
        spread_kernel,
        [jax.ShapeDtypeStruct((own, 4 * V_DIM), BF)] * 4,
        parts,
        where,
        [pltpu.VMEM((4, strip, V_DIM), BF), pltpu.VMEM((4, own, 4 * V_DIM), BF)],
    )
    parts = [parts[0]] + [shifted(parts[j], "zh", j) for j in range(1, 4)]
    height, width = out_proj.shape
    span = width // 4
    built = pl.pallas_call(
        project_kernel,
        grid=(4,),
        in_specs=[SMEM_SPEC]
        + [VMEM_SPEC] * 4
        + [pl.BlockSpec((height, span), lambda i: (0, i))],
        out_specs=pl.BlockSpec((own, span), lambda i: (0, i)),
        out_shape=jax.ShapeDtypeStruct((own, width), BF),
        scratch_shapes=[pltpu.VMEM((4, own, 4 * V_DIM), BF), pltpu.VMEM((own, height), BF)],
        compiler_params=pltpu.CompilerParams(vmem_limit_bytes=8 << 20),
        name="project",
    )
    parts = [pltpu.with_memory_space_constraint(a, pltpu.VMEM) for a in parts]
    return built(where, *parts, pltpu.with_memory_space_constraint(out_proj, pltpu.HBM))


def body(
    query,
    latent,
    rope_key,
    latent_gain,
    key_up,
    value_up,
    out_proj,
    tokens,
    moe_gain,
    routes,
    group_prob,
    expert_prob,
    w_gate,
    w_up,
    w_down,
):
    where = jnp.stack([lax.axis_index(n) for n in AXES]).astype(jnp.int32)
    return both_halves(
        where,
        query,
        latent,
        rope_key,
        latent_gain,
        key_up,
        value_up,
        out_proj,
        tokens,
        moe_gain,
        routes,
        group_prob,
        expert_prob,
        w_gate,
        w_up,
        w_down,
    )


def solution(mesh):
    ep, every = EP, AXES
    split = Mesh(mesh.devices.reshape(4, 2, 4, 2, 4), AXES)
    return jax.shard_map(
        body,
        mesh=split,
        in_specs=(
            P(ep, "x"),
            P(every, None),
            P(every, None),
            P(),
            P(None, "x"),
            P(None, "x"),
            P(),
            P(every, None),
            P(),
            P(every, None),
            P(every),
            P(every, None),
            P(ep, None, "x"),
            P(ep, None, "x"),
            P(ep, "x", None),
        ),
        out_specs=(P(every, None), P(every, None)),
        check_vma=False,
    )
```

```python
import jax
import jax.numpy as jnp
from jax import lax
from jax.experimental import pallas as pl
from jax.experimental.pallas import tpu as pltpu
from jax.sharding import Mesh, PartitionSpec as P


NOPE = 64
ROPE_DIM = 32
V_DIM = 64
QK_DIM = NOPE + ROPE_DIM
KV_ROWS = QK_DIM + V_DIM
CAP = 4
BF = jnp.bfloat16
F32 = jnp.float32

epsilon = 1e-06
rope_base = 10000.0
masked_value = -1e30
log2_e = 1.4426950408889634


AXES = ("zh", "zl", "y", "c", "x")
EP = AXES[:4]

SMEM_SPEC = pl.BlockSpec(memory_space=pltpu.SMEM)
VMEM_SPEC = pl.BlockSpec(memory_space=pltpu.VMEM)


def call(kernel, out_shape, arrays, where=None, scratch=(), limit=8 << 20, unplaced=(), place=pltpu.VMEM):
    arrays = [
        pltpu.with_memory_space_constraint(a, pltpu.HBM if i in unplaced else pltpu.VMEM)
        for i, a in enumerate(arrays)
    ]
    specs = [VMEM_SPEC] * len(arrays)
    if where is not None:
        arrays, specs = [where] + arrays, [SMEM_SPEC] + specs
    single = not isinstance(out_shape, (list, tuple))
    if place is not None:
        if single:
            out_shape = place(out_shape.shape, out_shape.dtype)
        else:
            out_shape = [place(s.shape, s.dtype) for s in out_shape]
    return pl.pallas_call(
        kernel,
        in_specs=specs,
        out_specs=VMEM_SPEC if single else [VMEM_SPEC] * len(out_shape),
        out_shape=out_shape,
        scratch_shapes=list(scratch),
        compiler_params=pltpu.CompilerParams(vmem_limit_bytes=limit),
    )(*arrays)


def mm(a, b, dims=((1,), (0,))):
    return lax.dot_general(a, b, (dims, ((), ())), preferred_element_type=F32)


def shifted(value, axis, amount):
    n = lax.axis_size(axis)
    return lax.ppermute(value, axis, [(i, (i + amount) % n) for i in range(n)])


def paired(value, mate):
    n = lax.axis_size("x")
    return lax.ppermute(value, "x", [(i, mate(i)) for i in range(n)])


def weight_mate(i):
    return i ^ 1


def row_mate(i):
    return 3 - i


def trig(positions):
    half = ROPE_DIM // 2
    inverse = rope_base ** (-2.0 * jnp.arange(half, dtype=F32) / ROPE_DIM)
    angles = positions.astype(F32)[:, None] * inverse[None, :]
    return jnp.cos(angles), jnp.sin(angles)


def rms_scale(values, gain):
    widened = values.astype(F32)
    return widened * lax.rsqrt(jnp.mean(widened * widened, axis=-1, keepdims=True) + epsilon) * gain


def dispatch_kernel(tokens, gain, routes, group_prob, expert_prob, outgoing, shares_out):
    rows = tokens.shape[0]
    experts, cap, width = outgoing.shape
    slots = experts * cap
    normed = rms_scale(tokens[...], gain[...]).astype(BF)
    slot = lax.broadcasted_iota(jnp.int32, (slots, rows), 0)
    expert = slot // cap
    first = routes[0:1, :] == expert
    second = routes[1:2, :] == expert
    named = (first | second).astype(BF)
    before = lax.broadcasted_iota(jnp.int32, (rows, rows), 0) < lax.broadcasted_iota(
        jnp.int32, (rows, rows), 1
    )
    prior = mm(named, before.astype(BF))
    mine = (first | second) & (prior == (slot % cap).astype(F32))
    outgoing[...] = mm(mine.astype(BF), normed).reshape(experts, cap, width).astype(BF)
    probs = expert_prob[...]
    shares = group_prob[...] * probs / jnp.sum(probs, axis=0, keepdims=True)
    weights = jnp.where(first, shares[0:1, :], shares[1:2, :])
    weights = jnp.where(mine, weights, 0.0)
    high = weights.astype(BF)
    shares_out[:, 0:rows] = high
    shares_out[:, rows : 2 * rows] = (weights - high.astype(F32)).astype(BF)


def dispatch(tokens, gain, routes, group_prob, expert_prob, experts):
    rows, width = tokens.shape
    return call(
        dispatch_kernel,
        (
            jax.ShapeDtypeStruct((experts, CAP, width), BF),
            jax.ShapeDtypeStruct((experts * CAP, 2 * rows), BF),
        ),
        [tokens, gain[None, :], routes.T, group_prob[None, :], expert_prob.T],
        unplaced=range(5),
        place=pltpu.HBM,
    )


def hidden_kernel(rows, w_gate, w_up, out, gate_s, up_s):
    count, span = out.shape[0], 1024
    gate_s[...] = jnp.zeros(gate_s.shape, F32)
    up_s[...] = jnp.zeros(up_s.shape, F32)

    def add(step, _):
        cols = pl.ds(pl.multiple_of(step * span, span), span)
        got = rows[:, :, cols].reshape(count, span)
        gate_s[...] += mm(got, w_gate[cols, :])
        up_s[...] += mm(got, w_up[cols, :])
        return 0

    lax.fori_loop(0, w_gate.shape[0] // span, add, 0)
    gate = gate_s[...]
    out[...] = (gate / (1.0 + jnp.exp(-gate)) * up_s[...]).astype(BF)


def hidden_of(rows, weights):
    shape = jax.ShapeDtypeStruct((rows.shape[0] * CAP, weights[0].shape[1]), BF)
    scratch = [pltpu.VMEM(shape.shape, F32)] * 2
    return call(hidden_kernel, shape, [rows] + weights, scratch=scratch)


def stage_kernel(w0, w1, w2, w3, out):
    for k, piece in enumerate((w0, w1, w2, w3)):
        out[k] = piece[...]


def down_kernel(h0, h1, h2, h3, weights, out):
    total = mm(h0[...], weights[0]) + mm(h1[...], weights[1])
    total = total + mm(h2[...], weights[2]) + mm(h3[...], weights[3])
    out[...] = total.astype(BF).reshape(out.shape)


def combine_kernel(returned, shares, out):
    rows = out.shape[0]
    got = returned[...].reshape(shares.shape[0], out.shape[1])
    both = mm(shares[...], got, ((0,), (0,)))
    out[...] = (both[:rows] + both[rows:]).astype(BF)


def both_halves(
    where,
    query,
    latent,
    rope_key,
    latent_gain,
    key_up,
    value_up,
    out_proj,
    tokens,
    moe_gain,
    routes,
    group_prob,
    expert_prob,
    w_gate,
    w_up,
    w_down,
):
    experts = lax.axis_size(EP)
    rows, width = tokens.shape
    w_gate, w_up, w_down = w_gate[0], w_up[0], w_down[0]
    down_w, down_r = paired(w_down, weight_mate), paired(w_down, row_mate)
    down_rw = paired(down_w, row_mate)
    gate_w, up_w = paired(w_gate, weight_mate), paired(w_up, weight_mate)
    set_a, set_b = [w_gate, w_up], [gate_w, up_w]
    outgoing, shares = dispatch(tokens, moe_gain, routes, group_prob, expert_prob, experts)
    arrived = lax.all_to_all(outgoing, EP, split_axis=0, concat_axis=0, tiled=True)
    queries, pair = query_and_pair(where, query, latent, rope_key, latent_gain, key_up, value_up)
    mate_rows = paired(arrived, row_mate)
    parts = attend(where, queries, pair)
    own_a = hidden_of(arrived, set_a)
    mate_a = paired(hidden_of(mate_rows, set_a), row_mate)
    mate_b = paired(hidden_of(mate_rows, set_b), row_mate)
    own_b = hidden_of(arrived, set_b)
    shape = jax.ShapeDtypeStruct((4, *w_down.shape), BF)
    down = call(stage_kernel, shape, [w_down, down_w, down_r, down_rw], unplaced=range(4))
    shape = jax.ShapeDtypeStruct((experts, CAP, width), BF)
    arrays = [own_a, own_b, mate_a, mate_b, down]
    result = call(down_kernel, shape, arrays, place=pltpu.HBM)
    returned = lax.all_to_all(result, EP, split_axis=0, concat_axis=0, tiled=True)
    mixed = project(where, parts, out_proj, latent.shape[0])
    shape = jax.ShapeDtypeStruct((rows, width), BF)
    return mixed, call(combine_kernel, shape, [returned, shares], place=None)


def latent_kernel(latent, gain, rope_key, cosine, sine, out):
    width = latent.shape[1]
    half = ROPE_DIM // 2
    out[:, :width] = rms_scale(latent[...], gain[...]).astype(BF)
    rope = rope_key[...].astype(F32)
    crossed = jnp.concatenate([-rope[:, half:], rope[:, :half]], axis=1)
    out[:, width:] = (rope * cosine[...] + crossed * sine[...]).astype(BF)


def heads_kernel(
    where, l0, l1, l2, l3, key_up, value_up, query, cosine, sine, o0, o1, o2, o3, strip_s, heads
):
    latent = key_up.shape[0]
    own = l0.shape[0]
    count = heads.shape[0]
    half = ROPE_DIM // 2
    turned = query[...].astype(F32).T
    for h in range(count):
        at = h * QK_DIM
        a = turned[at + NOPE : at + NOPE + half]
        b = turned[at + NOPE + half : at + QK_DIM]
        heads[h, :NOPE, :] = turned[at : at + NOPE].astype(BF)
        heads[h, NOPE : NOPE + half, :] = (a * cosine[...] - b * sine[...]).astype(BF)
        heads[h, NOPE + half : QK_DIM, :] = (a * sine[...] + b * cosine[...]).astype(BF)
    for k, block in enumerate((l0, l1, l2, l3)):
        strip_s[k * own : (k + 1) * own, :] = block[...]
    got = strip_s[:, :latent]
    keys = mm(key_up[...], got, ((0,), (1,))).astype(BF)
    values = mm(value_up[...], got, ((0,), (1,))).astype(BF)
    eye = (
        lax.broadcasted_iota(jnp.int32, (ROPE_DIM, ROPE_DIM), 0)
        == lax.broadcasted_iota(jnp.int32, (ROPE_DIM, ROPE_DIM), 1)
    ).astype(BF)
    rope = mm(eye, strip_s[:, latent:], ((1,), (1,))).astype(BF)
    for h in range(count):
        heads[h, QK_DIM : QK_DIM + NOPE, :] = keys[h * NOPE : (h + 1) * NOPE]
        heads[h, QK_DIM + NOPE : 2 * QK_DIM, :] = rope
        heads[h, 2 * QK_DIM :, :] = values[h * V_DIM : (h + 1) * V_DIM]
    for k, out in enumerate((o0, o1, o2, o3)):
        out[...] = heads[lax.rem(where[0] + k, 4)]


def stack_kernel(b0, b1, b2, b3, out):
    for j, block in enumerate((b0, b1, b2, b3)):
        out[j] = block[QK_DIM:, :]


def attend_kernel(where, q0, q1, q2, q3, *refs):
    blocks, outs, (q_s, top_s, acc_s) = refs[:8], refs[8:12], refs[12:]
    zh, zl, y, c, x = (where[i] for i in range(5))
    strip = q0.shape[1]
    span = blocks[0].shape[2]
    factor = QK_DIM ** (-0.5) * log2_e
    for j, q in enumerate((q0, q1, q2, q3)):
        at = pl.multiple_of(lax.rem(zh - j + 4, 4) * strip, strip)
        q_s[pl.ds(at, strip), :] = q[:QK_DIM, :].astype(F32).T.astype(BF)
    top_s[...] = jnp.full(top_s.shape, masked_value, F32)
    acc_s[...] = jnp.zeros(acc_s.shape, F32)

    col = lax.broadcasted_iota(jnp.int32, (1, span), 1)
    col_zl = jnp.bitwise_xor(zl, col // strip)
    within = col % strip
    col_x = ((x - within // 32 + 4) % 4) * 32 + within % 32
    query_at = (zl * 8 + y * 2 + c) * strip + lax.broadcasted_iota(jnp.int32, (strip, 1), 0)
    ones = jnp.ones((V_DIM, span), BF)

    def advance(rows, parts, masks):
        q = q_s[rows, :]
        old = top_s[rows, :]
        scores = [mm(q, part[:QK_DIM, :]) for part in parts]
        if masks is not None:
            scores = [jnp.where(m, s, masked_value) for m, s in zip(masks, scores)]
        peak = scores[0]
        for s in scores[1:]:
            peak = jnp.maximum(peak, s)
        new = jnp.maximum(old, jnp.max(peak, axis=1, keepdims=True))
        top_s[rows, :] = new
        base = new[:, :1]
        total = acc_s[rows, :] * jnp.exp2((old - new) * factor)
        for s, part in zip(scores, parts):
            raised = jnp.exp2((s - base) * factor).astype(BF)
            extended = jnp.concatenate([part[QK_DIM:, :], ones], axis=0)
            total = total + mm(raised, extended, ((1,), (1,)))
        acc_s[rows, :] = total

    for m in range(2):
        group = blocks[4 * m : 4 * m + 4]
        masks = []
        for k in range(4):
            key_y = lax.rem(y - k + 4, 4)
            key_at = (col_zl * 8 + key_y * 2 + jnp.bitwise_xor(c, m)) * strip + col_x
            masks.append(key_at <= query_at)

        for g in range(4):
            from_zh = lax.rem(zh - g + 4, 4)
            parts = [block[from_zh] for block in group]
            advance(slice(g * strip, (g + 1) * strip), parts, masks)
            if g < 3:
                advance(slice((g + 1) * strip, 4 * strip), parts, None)
    total = acc_s[...]
    acc_s[:, :V_DIM] = total[:, :V_DIM] / total[:, V_DIM:]
    for j, out in enumerate(outs):
        at = pl.multiple_of(lax.rem(zh - j + 4, 4) * strip, strip)
        out[...] = acc_s[pl.ds(at, strip), :V_DIM].astype(BF)


def spread_kernel(where, a0, a1, a2, a3, o0, o1, o2, o3, heads, parts):
    for j, a in enumerate((a0, a1, a2, a3)):
        heads[lax.rem(where[0] + j, 4)] = a[...]
    beside = jnp.concatenate([heads[h] for h in range(4)], axis=1)
    parts[...] = beside.reshape(parts.shape)
    for k, out in enumerate((o0, o1, o2, o3)):
        out[...] = parts[lax.rem(where[4] + k, 4)]


def project_kernel(where, a0, a1, a2, a3, out_proj, out, parts):
    width = a0.shape[1]
    for k, a in enumerate((a0, a1, a2, a3)):
        parts[lax.rem(where[4] - k + 4, 4)] = a[...]
    total = mm(parts[0], out_proj[:width, :])
    for h in range(1, 4):
        total = total + mm(parts[h], out_proj[h * width : (h + 1) * width, :])
    out[...] = total.astype(BF)


def query_and_pair(where, query, latent, rope_key, latent_gain, key_up, value_up):
    strip = query.shape[0]
    own = latent.shape[0]
    query_start = (((where[0] * 2 + where[1]) * 4 + where[2]) * 2 + where[3]) * strip

    key_cos, key_sin = trig(query_start + where[4] * own + jnp.arange(own, dtype=jnp.int32))
    both = call(
        latent_kernel,
        jax.ShapeDtypeStruct((own, latent.shape[1] + ROPE_DIM), BF),
        [
            latent,
            latent_gain[None, :],
            rope_key,
            jnp.concatenate([key_cos, key_cos], axis=1),
            jnp.concatenate([key_sin, key_sin], axis=1),
        ],
        unplaced=range(3),
    )
    near = [both] + [shifted(both, "x", k) for k in range(1, 4)]
    cosine, sine = trig(query_start + jnp.arange(strip, dtype=jnp.int32))
    blocks = call(
        heads_kernel,
        [jax.ShapeDtypeStruct((QK_DIM + KV_ROWS, strip), BF)] * 4,
        near + [key_up, value_up, query, cosine.T, sine.T],
        where,
        scratch=[
            pltpu.VMEM((strip, both.shape[1]), BF),
            pltpu.VMEM((4, QK_DIM + KV_ROWS, strip), BF),
        ],
        unplaced=range(4, 7),
    )
    blocks = [blocks[0]] + [shifted(blocks[k], "zh", k) for k in range(1, 4)]
    shape = jax.ShapeDtypeStruct((4, KV_ROWS, strip), BF)
    mine = call(stack_kernel, shape, blocks)
    return blocks, jnp.concatenate([mine, shifted(mine, "zl", 1)], axis=2)


def attend(where, blocks, pair):
    strip = blocks[0].shape[1]
    column = [pair] + [shifted(pair, "y", k) for k in range(1, 4)]
    column = column + [shifted(part, "c", 1) for part in column]
    parts = call(
        attend_kernel,
        [jax.ShapeDtypeStruct((strip, V_DIM), BF)] * 4,
        blocks + column,
        where,
        [
            pltpu.VMEM((4 * strip, QK_DIM), BF),
            pltpu.VMEM((4 * strip, 128), F32),
            pltpu.VMEM((4 * strip, 128), F32),
        ],
    )
    return [parts[0]] + [shifted(parts[j], "zh", -j) for j in range(1, 4)]


def project(where, parts, out_proj, own):
    strip = parts[0].shape[0]
    parts = call(
        spread_kernel,
        [jax.ShapeDtypeStruct((own, 4 * V_DIM), BF)] * 4,
        parts,
        where,
        [pltpu.VMEM((4, strip, V_DIM), BF), pltpu.VMEM((4, own, 4 * V_DIM), BF)],
    )
    parts = [parts[0]] + [shifted(parts[k], "x", k) for k in range(1, 4)]
    return call(
        project_kernel,
        jax.ShapeDtypeStruct((own, out_proj.shape[1]), BF),
        parts + [out_proj],
        where,
        [pltpu.VMEM((4, own, 4 * V_DIM), BF)],
        place=None,
    )


def body(
    query,
    latent,
    rope_key,
    latent_gain,
    key_up,
    value_up,
    out_proj,
    tokens,
    moe_gain,
    routes,
    group_prob,
    expert_prob,
    w_gate,
    w_up,
    w_down,
):
    where = jnp.stack([lax.axis_index(n) for n in AXES]).astype(jnp.int32)
    return both_halves(
        where,
        query,
        latent,
        rope_key,
        latent_gain,
        key_up,
        value_up,
        out_proj,
        tokens,
        moe_gain,
        routes,
        group_prob,
        expert_prob,
        w_gate,
        w_up,
        w_down,
    )


def solution(mesh):
    ep, every = EP, AXES
    split = Mesh(mesh.devices.reshape(4, 2, 4, 2, 4), AXES)
    return jax.shard_map(
        body,
        mesh=split,
        in_specs=(
            P(ep, "x"),
            P(every, None),
            P(every, None),
            P(),
            P(None, "x"),
            P(None, "x"),
            P(),
            P(every, None),
            P(),
            P(every, None),
            P(every),
            P(every, None),
            P(ep, None, "x"),
            P(ep, None, "x"),
            P(ep, "x", None),
        ),
        out_specs=(P(every, None), P(every, None)),
        check_vma=False,
    )
```

```python
import jax
import jax.numpy as jnp
from jax import lax
from jax.experimental import pallas as pl
from jax.experimental.pallas import tpu as pltpu
from jax.sharding import Mesh, PartitionSpec as P


NOPE = 64
ROPE_DIM = 32
V_DIM = 64
QK_DIM = NOPE + ROPE_DIM
KV_ROWS = QK_DIM + V_DIM
CAP = 4
BF = jnp.bfloat16
F32 = jnp.float32

epsilon = 1e-06
rope_base = 10000.0
masked_value = -1e30
log2_e = 1.4426950408889634


AXES = ("zh", "zl", "y", "c", "x")
EP = AXES[:4]

SMEM_SPEC = pl.BlockSpec(memory_space=pltpu.SMEM)
VMEM_SPEC = pl.BlockSpec(memory_space=pltpu.VMEM)


def call(kernel, out_shape, arrays, where=None, scratch=(), limit=8 << 20, unplaced=(), place=pltpu.VMEM):
    arrays = [
        pltpu.with_memory_space_constraint(a, pltpu.HBM if i in unplaced else pltpu.VMEM)
        for i, a in enumerate(arrays)
    ]
    specs = [VMEM_SPEC] * len(arrays)
    if where is not None:
        arrays, specs = [where] + arrays, [SMEM_SPEC] + specs
    single = not isinstance(out_shape, (list, tuple))
    if place is not None:
        if single:
            out_shape = place(out_shape.shape, out_shape.dtype)
        else:
            out_shape = [place(s.shape, s.dtype) for s in out_shape]
    return pl.pallas_call(
        kernel,
        in_specs=specs,
        out_specs=VMEM_SPEC if single else [VMEM_SPEC] * len(out_shape),
        out_shape=out_shape,
        scratch_shapes=list(scratch),
        compiler_params=pltpu.CompilerParams(vmem_limit_bytes=limit),
    )(*arrays)


def mm(a, b, dims=((1,), (0,))):
    return lax.dot_general(a, b, (dims, ((), ())), preferred_element_type=F32)


def shifted(value, axis, amount):
    n = lax.axis_size(axis)
    return lax.ppermute(value, axis, [(i, (i + amount) % n) for i in range(n)])


def paired(value, mate):
    n = lax.axis_size("x")
    return lax.ppermute(value, "x", [(i, mate(i)) for i in range(n)])


def weight_mate(i):
    return i ^ 1


def row_mate(i):
    return 3 - i


def trig(positions):
    half = ROPE_DIM // 2
    inverse = rope_base ** (-2.0 * jnp.arange(half, dtype=F32) / ROPE_DIM)
    angles = positions.astype(F32)[:, None] * inverse[None, :]
    return jnp.cos(angles), jnp.sin(angles)


def rms_scale(values, gain):
    widened = values.astype(F32)
    return widened * lax.rsqrt(jnp.mean(widened * widened, axis=-1, keepdims=True) + epsilon) * gain


def dispatch_kernel(tokens, gain, routes, group_prob, expert_prob, outgoing, shares_out):
    rows = tokens.shape[0]
    experts, cap, width = outgoing.shape
    slots = experts * cap
    normed = rms_scale(tokens[...], gain[...]).astype(BF)
    slot = lax.broadcasted_iota(jnp.int32, (slots, rows), 0)
    expert = slot // cap
    first = routes[0:1, :] == expert
    second = routes[1:2, :] == expert
    named = (first | second).astype(BF)
    before = lax.broadcasted_iota(jnp.int32, (rows, rows), 0) < lax.broadcasted_iota(
        jnp.int32, (rows, rows), 1
    )
    prior = mm(named, before.astype(BF))
    mine = (first | second) & (prior == (slot % cap).astype(F32))
    outgoing[...] = mm(mine.astype(BF), normed).reshape(experts, cap, width).astype(BF)
    probs = expert_prob[...]
    shares = group_prob[...] * probs / jnp.sum(probs, axis=0, keepdims=True)
    weights = jnp.where(first, shares[0:1, :], shares[1:2, :])
    weights = jnp.where(mine, weights, 0.0)
    high = weights.astype(BF)
    shares_out[:, 0:rows] = high
    shares_out[:, rows : 2 * rows] = (weights - high.astype(F32)).astype(BF)


def dispatch(tokens, gain, routes, group_prob, expert_prob, experts):
    rows, width = tokens.shape
    return call(
        dispatch_kernel,
        (
            jax.ShapeDtypeStruct((experts, CAP, width), BF),
            jax.ShapeDtypeStruct((experts * CAP, 2 * rows), BF),
        ),
        [tokens, gain[None, :], routes.T, group_prob[None, :], expert_prob.T],
        unplaced=range(5),
        place=pltpu.HBM,
    )


def hidden_kernel(rows, w_gate, w_up, out, gate_s, up_s):
    count, span = out.shape[0], 1024
    gate_s[...] = jnp.zeros(gate_s.shape, F32)
    up_s[...] = jnp.zeros(up_s.shape, F32)

    def add(step, _):
        cols = pl.ds(pl.multiple_of(step * span, span), span)
        got = rows[:, :, cols].reshape(count, span)
        gate_s[...] += mm(got, w_gate[cols, :])
        up_s[...] += mm(got, w_up[cols, :])
        return 0

    lax.fori_loop(0, w_gate.shape[0] // span, add, 0)
    gate = gate_s[...]
    out[...] = (gate / (1.0 + jnp.exp(-gate)) * up_s[...]).astype(BF)


def hidden_of(rows, weights):
    shape = jax.ShapeDtypeStruct((rows.shape[0] * CAP, weights[0].shape[1]), BF)
    scratch = [pltpu.VMEM(shape.shape, F32)] * 2
    return call(hidden_kernel, shape, [rows] + weights, scratch=scratch)


def copy_kernel(value, out):
    out[...] = value[...]


def in_vmem(value):
    shape = jax.ShapeDtypeStruct(value.shape, value.dtype)
    return call(copy_kernel, shape, [value], unplaced=[0])


def stage_kernel(w0, w1, w2, w3, out):
    for k, piece in enumerate((w0, w1, w2, w3)):
        out[k] = piece[...]


def down_kernel(h0, h1, h2, h3, weights, out):
    total = mm(h0[...], weights[0]) + mm(h1[...], weights[1])
    total = total + mm(h2[...], weights[2]) + mm(h3[...], weights[3])
    out[...] = total.astype(BF).reshape(out.shape)


def both_halves(
    where,
    query,
    latent,
    rope_key,
    latent_gain,
    key_up,
    value_up,
    out_proj,
    tokens,
    moe_gain,
    routes,
    group_prob,
    expert_prob,
    w_gate,
    w_up,
    w_down,
):
    experts = lax.axis_size(EP)
    rows, width = tokens.shape
    w_gate, w_up, w_down = w_gate[0], w_up[0], w_down[0]
    down_w, down_r = paired(w_down, weight_mate), paired(w_down, row_mate)
    down_rw = paired(down_w, row_mate)
    gate_w, up_w = paired(w_gate, weight_mate), paired(w_up, weight_mate)
    set_a, set_b = [w_gate, w_up], [in_vmem(gate_w), up_w]
    outgoing, shares = dispatch(tokens, moe_gain, routes, group_prob, expert_prob, experts)
    arrived = lax.all_to_all(outgoing, EP, split_axis=0, concat_axis=0, tiled=True)
    queries, pair = query_and_pair(where, query, latent, rope_key, latent_gain, key_up, value_up)
    mate_rows = paired(arrived, row_mate)
    parts = attend(where, queries, pair)
    own_a = hidden_of(arrived, set_a)
    mate_a = paired(hidden_of(mate_rows, set_a), row_mate)
    mate_b = paired(hidden_of(mate_rows, set_b), row_mate)
    own_b = hidden_of(arrived, set_b)
    shape = jax.ShapeDtypeStruct((4, *w_down.shape), BF)
    down = call(stage_kernel, shape, [w_down, down_w, down_r, down_rw], unplaced=range(4))
    shape = jax.ShapeDtypeStruct((experts, CAP, width), BF)
    arrays = [own_a, own_b, mate_a, mate_b, down]
    result = call(down_kernel, shape, arrays, place=pltpu.HBM)
    returned = lax.all_to_all(result, EP, split_axis=0, concat_axis=0, tiled=True)
    parts = out_parts(where, parts, latent.shape[0])
    height, span = out_proj.shape[0], width // 4
    near = [pltpu.with_memory_space_constraint(a, pltpu.VMEM) for a in [returned, shares] + parts]
    finish = pl.pallas_call(
        finish_kernel,
        in_specs=[SMEM_SPEC] + [VMEM_SPEC] * 6 + [pl.BlockSpec(memory_space=pl.ANY)],
        out_specs=[VMEM_SPEC] * 2,
        out_shape=[
            jax.ShapeDtypeStruct((rows, width), BF),
            jax.ShapeDtypeStruct((latent.shape[0], width), BF),
        ],
        scratch_shapes=[
            pltpu.VMEM((4, latent.shape[0], 4 * V_DIM), BF),
            pltpu.VMEM((4, height, span), BF),
            pltpu.SemaphoreType.DMA((4,)),
        ],
        compiler_params=pltpu.CompilerParams(vmem_limit_bytes=8 << 20),
        name="finish",
    )
    far = pltpu.with_memory_space_constraint(out_proj, pltpu.HBM)
    moe_out, mixed = finish(where, *near, far)
    return mixed, moe_out


def latent_kernel(latent, gain, rope_key, cosine, sine, out):
    width = latent.shape[1]
    half = ROPE_DIM // 2
    out[:, :width] = rms_scale(latent[...], gain[...]).astype(BF)
    rope = rope_key[...].astype(F32)
    crossed = jnp.concatenate([-rope[:, half:], rope[:, :half]], axis=1)
    out[:, width:] = (rope * cosine[...] + crossed * sine[...]).astype(BF)


def heads_kernel(
    where, l0, l1, l2, l3, key_up, value_up, query, cosine, sine, o0, o1, o2, o3, strip_s, heads
):
    latent = key_up.shape[0]
    own = l0.shape[0]
    count = heads.shape[0]
    half = ROPE_DIM // 2
    turned = query[...].astype(F32).T
    for h in range(count):
        at = h * QK_DIM
        a = turned[at + NOPE : at + NOPE + half]
        b = turned[at + NOPE + half : at + QK_DIM]
        heads[h, :NOPE, :] = turned[at : at + NOPE].astype(BF)
        heads[h, NOPE : NOPE + half, :] = (a * cosine[...] - b * sine[...]).astype(BF)
        heads[h, NOPE + half : QK_DIM, :] = (a * sine[...] + b * cosine[...]).astype(BF)
    for k, block in enumerate((l0, l1, l2, l3)):
        strip_s[k * own : (k + 1) * own, :] = block[...]
    got = strip_s[:, :latent]
    keys = mm(key_up[...], got, ((0,), (1,))).astype(BF)
    values = mm(value_up[...], got, ((0,), (1,))).astype(BF)
    eye = (
        lax.broadcasted_iota(jnp.int32, (ROPE_DIM, ROPE_DIM), 0)
        == lax.broadcasted_iota(jnp.int32, (ROPE_DIM, ROPE_DIM), 1)
    ).astype(BF)
    rope = mm(eye, strip_s[:, latent:], ((1,), (1,))).astype(BF)
    for h in range(count):
        heads[h, QK_DIM : QK_DIM + NOPE, :] = keys[h * NOPE : (h + 1) * NOPE]
        heads[h, QK_DIM + NOPE : 2 * QK_DIM, :] = rope
        heads[h, 2 * QK_DIM :, :] = values[h * V_DIM : (h + 1) * V_DIM]
    for k, out in enumerate((o0, o1, o2, o3)):
        out[...] = heads[lax.rem(where[0] + k, 4)]


def stack_kernel(b0, b1, b2, b3, out):
    for j, block in enumerate((b0, b1, b2, b3)):
        out[j] = block[QK_DIM:, :]


def attend_kernel(where, q0, q1, q2, q3, *refs):
    blocks, outs, (q_s, top_s, acc_s) = refs[:8], refs[8:12], refs[12:]
    zh, zl, y, c, x = (where[i] for i in range(5))
    strip = q0.shape[1]
    span = blocks[0].shape[2]
    factor = QK_DIM ** (-0.5) * log2_e
    for j, q in enumerate((q0, q1, q2, q3)):
        at = pl.multiple_of(lax.rem(zh - j + 4, 4) * strip, strip)
        q_s[pl.ds(at, strip), :] = q[:QK_DIM, :].astype(F32).T.astype(BF)
    top_s[...] = jnp.full(top_s.shape, masked_value, F32)
    acc_s[...] = jnp.zeros(acc_s.shape, F32)

    col = lax.broadcasted_iota(jnp.int32, (1, span), 1)
    col_zl = jnp.bitwise_xor(zl, col // strip)
    within = col % strip
    col_x = ((x - within // 32 + 4) % 4) * 32 + within % 32
    query_at = (zl * 8 + y * 2 + c) * strip + lax.broadcasted_iota(jnp.int32, (strip, 1), 0)
    ones = jnp.ones((V_DIM, span), BF)

    def advance(rows, parts, masks):
        q = q_s[rows, :]
        old = top_s[rows, :]
        scores = [mm(q, part[:QK_DIM, :]) for part in parts]
        if masks is not None:
            scores = [jnp.where(m, s, masked_value) for m, s in zip(masks, scores)]
        peak = scores[0]
        for s in scores[1:]:
            peak = jnp.maximum(peak, s)
        new = jnp.maximum(old, jnp.max(peak, axis=1, keepdims=True))
        top_s[rows, :] = new
        base = new[:, :1]
        total = acc_s[rows, :] * jnp.exp2((old - new) * factor)
        for s, part in zip(scores, parts):
            raised = jnp.exp2((s - base) * factor).astype(BF)
            extended = jnp.concatenate([part[QK_DIM:, :], ones], axis=0)
            total = total + mm(raised, extended, ((1,), (1,)))
        acc_s[rows, :] = total

    for m in range(2):
        group = blocks[4 * m : 4 * m + 4]
        masks = []
        for k in range(4):
            key_y = lax.rem(y - k + 4, 4)
            key_at = (col_zl * 8 + key_y * 2 + jnp.bitwise_xor(c, m)) * strip + col_x
            masks.append(key_at <= query_at)

        for g in range(4):
            from_zh = lax.rem(zh - g + 4, 4)
            parts = [block[from_zh] for block in group]
            advance(slice(g * strip, (g + 1) * strip), parts, masks)
            if g < 3:
                advance(slice((g + 1) * strip, 4 * strip), parts, None)
    total = acc_s[...]
    acc_s[:, :V_DIM] = total[:, :V_DIM] / total[:, V_DIM:]
    own = strip // 4
    for k, out in enumerate(outs):
        for g in range(4):
            at = pl.multiple_of(g * strip + lax.rem(x + k, 4) * own, own)
            out[g * own : (g + 1) * own, :] = acc_s[pl.ds(at, own), :V_DIM].astype(BF)


def spread_kernel(where, a0, a1, a2, a3, o0, o1, o2, o3, heads, parts):
    for k, a in enumerate((a0, a1, a2, a3)):
        heads[lax.rem(where[4] - k + 4, 4)] = a[...]
    beside = jnp.concatenate([heads[h] for h in range(4)], axis=1)
    parts[...] = beside.reshape(parts.shape)
    for j, out in enumerate((o0, o1, o2, o3)):
        out[...] = parts[lax.rem(where[0] + j, 4)]


def finish_kernel(
    where, returned, shares, a0, a1, a2, a3, out_proj, moe_out, mixed, parts, weights, sems
):
    count, _, span = weights.shape
    copies = [
        pltpu.make_async_copy(out_proj.at[:, pl.ds(c * span, span)], weights.at[c], sems.at[c])
        for c in range(count)
    ]
    for copy in copies:
        copy.start()
    rows = moe_out.shape[0]
    got = returned[...].reshape(shares.shape[0], moe_out.shape[1])
    both = mm(shares[...], got, ((0,), (0,)))
    moe_out[...] = (both[:rows] + both[rows:]).astype(BF)
    for j, a in enumerate((a0, a1, a2, a3)):
        parts[lax.rem(where[0] - j + 4, 4)] = a[...]
    pieces = [parts[h % 4, :, h // 4 * V_DIM : (h // 4 + 1) * V_DIM] for h in range(16)]
    beside = jnp.concatenate(pieces, axis=1)
    for c, copy in enumerate(copies):
        copy.wait()
        mixed[:, c * span : (c + 1) * span] = mm(beside, weights[c]).astype(BF)


def query_and_pair(where, query, latent, rope_key, latent_gain, key_up, value_up):
    strip = query.shape[0]
    own = latent.shape[0]
    query_start = (((where[0] * 2 + where[1]) * 4 + where[2]) * 2 + where[3]) * strip

    key_cos, key_sin = trig(query_start + where[4] * own + jnp.arange(own, dtype=jnp.int32))
    both = call(
        latent_kernel,
        jax.ShapeDtypeStruct((own, latent.shape[1] + ROPE_DIM), BF),
        [
            latent,
            latent_gain[None, :],
            rope_key,
            jnp.concatenate([key_cos, key_cos], axis=1),
            jnp.concatenate([key_sin, key_sin], axis=1),
        ],
        unplaced=range(3),
    )
    near = [both] + [shifted(both, "x", k) for k in range(1, 4)]
    cosine, sine = trig(query_start + jnp.arange(strip, dtype=jnp.int32))
    blocks = call(
        heads_kernel,
        [jax.ShapeDtypeStruct((QK_DIM + KV_ROWS, strip), BF)] * 4,
        near + [key_up, value_up, query, cosine.T, sine.T],
        where,
        scratch=[
            pltpu.VMEM((strip, both.shape[1]), BF),
            pltpu.VMEM((4, QK_DIM + KV_ROWS, strip), BF),
        ],
        unplaced=range(4, 7),
    )
    blocks = [blocks[0]] + [shifted(blocks[k], "zh", k) for k in range(1, 4)]
    shape = jax.ShapeDtypeStruct((4, KV_ROWS, strip), BF)
    mine = call(stack_kernel, shape, blocks)
    return blocks, jnp.concatenate([mine, shifted(mine, "zl", 1)], axis=2)


def attend(where, blocks, pair):
    strip = blocks[0].shape[1]
    column = [pair] + [shifted(pair, "y", k) for k in range(1, 4)]
    column = column + [shifted(part, "c", 1) for part in column]
    parts = call(
        attend_kernel,
        [jax.ShapeDtypeStruct((strip, V_DIM), BF)] * 4,
        blocks + column,
        where,
        [
            pltpu.VMEM((4 * strip, QK_DIM), BF),
            pltpu.VMEM((4 * strip, 128), F32),
            pltpu.VMEM((4 * strip, 128), F32),
        ],
    )
    return [parts[0]] + [shifted(parts[k], "x", k) for k in range(1, 4)]


def out_parts(where, parts, own):
    strip = parts[0].shape[0]
    parts = call(
        spread_kernel,
        [jax.ShapeDtypeStruct((own, 4 * V_DIM), BF)] * 4,
        parts,
        where,
        [pltpu.VMEM((4, strip, V_DIM), BF), pltpu.VMEM((4, own, 4 * V_DIM), BF)],
    )
    parts = [parts[0]] + [shifted(parts[j], "zh", j) for j in range(1, 4)]
    return parts


def body(
    query,
    latent,
    rope_key,
    latent_gain,
    key_up,
    value_up,
    out_proj,
    tokens,
    moe_gain,
    routes,
    group_prob,
    expert_prob,
    w_gate,
    w_up,
    w_down,
):
    where = jnp.stack([lax.axis_index(n) for n in AXES]).astype(jnp.int32)
    return both_halves(
        where,
        query,
        latent,
        rope_key,
        latent_gain,
        key_up,
        value_up,
        out_proj,
        tokens,
        moe_gain,
        routes,
        group_prob,
        expert_prob,
        w_gate,
        w_up,
        w_down,
    )


def solution(mesh):
    ep, every = EP, AXES
    split = Mesh(mesh.devices.reshape(4, 2, 4, 2, 4), AXES)
    return jax.shard_map(
        body,
        mesh=split,
        in_specs=(
            P(ep, "x"),
            P(every, None),
            P(every, None),
            P(),
            P(None, "x"),
            P(None, "x"),
            P(),
            P(every, None),
            P(),
            P(every, None),
            P(every),
            P(every, None),
            P(ep, None, "x"),
            P(ep, None, "x"),
            P(ep, "x", None),
        ),
        out_specs=(P(every, None), P(every, None)),
        check_vma=False,
    )
```

```python
import jax
import jax.numpy as jnp
from jax import lax
from jax.experimental import pallas as pl
from jax.experimental.pallas import tpu as pltpu
from jax.sharding import Mesh, PartitionSpec as P


NOPE = 64
ROPE_DIM = 32
V_DIM = 64
QK_DIM = NOPE + ROPE_DIM
KV_ROWS = QK_DIM + V_DIM
CAP = 4
BF = jnp.bfloat16
F32 = jnp.float32

epsilon = 1e-06
rope_base = 10000.0
masked_value = -1e30
log2_e = 1.4426950408889634


AXES = ("zh", "zl", "y", "c", "x")
EP = AXES[:4]

SMEM_SPEC = pl.BlockSpec(memory_space=pltpu.SMEM)
VMEM_SPEC = pl.BlockSpec(memory_space=pltpu.VMEM)


def call(kernel, out_shape, arrays, where=None, scratch=(), limit=8 << 20, unplaced=(), place=pltpu.VMEM):
    arrays = [
        pltpu.with_memory_space_constraint(a, pltpu.HBM if i in unplaced else pltpu.VMEM)
        for i, a in enumerate(arrays)
    ]
    specs = [VMEM_SPEC] * len(arrays)
    if where is not None:
        arrays, specs = [where] + arrays, [SMEM_SPEC] + specs
    single = not isinstance(out_shape, (list, tuple))
    if place is not None:
        if single:
            out_shape = place(out_shape.shape, out_shape.dtype)
        else:
            out_shape = [place(s.shape, s.dtype) for s in out_shape]
    return pl.pallas_call(
        kernel,
        in_specs=specs,
        out_specs=VMEM_SPEC if single else [VMEM_SPEC] * len(out_shape),
        out_shape=out_shape,
        scratch_shapes=list(scratch),
        compiler_params=pltpu.CompilerParams(vmem_limit_bytes=limit),
    )(*arrays)


def mm(a, b, dims=((1,), (0,))):
    return lax.dot_general(a, b, (dims, ((), ())), preferred_element_type=F32)


def shifted(value, axis, amount):
    n = lax.axis_size(axis)
    return lax.ppermute(value, axis, [(i, (i + amount) % n) for i in range(n)])


def paired(value, mate):
    n = lax.axis_size("x")
    return lax.ppermute(value, "x", [(i, mate(i)) for i in range(n)])


def weight_mate(i):
    return i ^ 1


def row_mate(i):
    return 3 - i


def trig(positions):
    half = ROPE_DIM // 2
    inverse = rope_base ** (-2.0 * jnp.arange(half, dtype=F32) / ROPE_DIM)
    angles = positions.astype(F32)[:, None] * inverse[None, :]
    return jnp.cos(angles), jnp.sin(angles)


def rms_scale(values, gain):
    widened = values.astype(F32)
    return widened * lax.rsqrt(jnp.mean(widened * widened, axis=-1, keepdims=True) + epsilon) * gain


def dispatch_kernel(tokens, gain, routes, group_prob, expert_prob, outgoing, shares_out):
    rows = tokens.shape[0]
    experts, cap, width = outgoing.shape
    slots = experts * cap
    normed = rms_scale(tokens[...], gain[...]).astype(BF)
    slot = lax.broadcasted_iota(jnp.int32, (slots, rows), 0)
    expert = slot // cap
    first = routes[0:1, :] == expert
    second = routes[1:2, :] == expert
    named = (first | second).astype(BF)
    before = lax.broadcasted_iota(jnp.int32, (rows, rows), 0) < lax.broadcasted_iota(
        jnp.int32, (rows, rows), 1
    )
    prior = mm(named, before.astype(BF))
    mine = (first | second) & (prior == (slot % cap).astype(F32))
    outgoing[...] = mm(mine.astype(BF), normed).reshape(experts, cap, width).astype(BF)
    probs = expert_prob[...]
    shares = group_prob[...] * probs / jnp.sum(probs, axis=0, keepdims=True)
    weights = jnp.where(first, shares[0:1, :], shares[1:2, :])
    weights = jnp.where(mine, weights, 0.0)
    high = weights.astype(BF)
    shares_out[:, 0:rows] = high
    shares_out[:, rows : 2 * rows] = (weights - high.astype(F32)).astype(BF)


def dispatch(tokens, gain, routes, group_prob, expert_prob, experts):
    rows, width = tokens.shape
    return call(
        dispatch_kernel,
        (
            jax.ShapeDtypeStruct((experts, CAP, width), BF),
            jax.ShapeDtypeStruct((experts * CAP, 2 * rows), BF),
        ),
        [tokens, gain[None, :], routes.T, group_prob[None, :], expert_prob.T],
        unplaced=range(5),
        place=pltpu.HBM,
    )


def hidden_kernel(rows, w_gate, w_up, out, gate_s, up_s):
    count, span = out.shape[0], 1024
    gate_s[...] = jnp.zeros(gate_s.shape, F32)
    up_s[...] = jnp.zeros(up_s.shape, F32)

    def add(step, _):
        cols = pl.ds(pl.multiple_of(step * span, span), span)
        got = rows[:, :, cols].reshape(count, span)
        gate_s[...] += mm(got, w_gate[cols, :])
        up_s[...] += mm(got, w_up[cols, :])
        return 0

    lax.fori_loop(0, w_gate.shape[0] // span, add, 0)
    gate = gate_s[...]
    out[...] = (gate / (1.0 + jnp.exp(-gate)) * up_s[...]).astype(BF)


def hidden_of(rows, weights):
    shape = jax.ShapeDtypeStruct((rows.shape[0] * CAP, weights[0].shape[1]), BF)
    scratch = [pltpu.VMEM(shape.shape, F32)] * 2
    return call(hidden_kernel, shape, [rows] + weights, scratch=scratch)


def late_hidden_kernel(rows, w_gate, w_up, out, gate_s, up_s, up_v, sems):
    count, steps = out.shape[0], sems.shape[0]
    span = w_up.shape[0] // steps
    parts = [slice(c * span, (c + 1) * span) for c in range(steps)]
    copies = [
        pltpu.make_async_copy(w_up.at[pl.ds(c * span, span), :], up_v.at[c], sems.at[c])
        for c in range(steps)
    ]
    for copy in copies:
        copy.start()
    for c, cols in enumerate(parts):
        got = rows[:, :, cols].reshape(count, span)
        gate = mm(got, w_gate[cols, :])
        copies[c].wait()
        up = mm(got, up_v[c])
        gate_s[...] = gate if c == 0 else gate_s[...] + gate
        up_s[...] = up if c == 0 else up_s[...] + up
    gate = gate_s[...]
    out[...] = (gate / (1.0 + jnp.exp(-gate)) * up_s[...]).astype(BF)


def late_hidden_of(rows, w_gate, w_up):
    height, units = w_up.shape
    shape = (rows.shape[0] * CAP, units)
    near = [pltpu.with_memory_space_constraint(a, pltpu.VMEM) for a in (rows, w_gate)]
    return pl.pallas_call(
        late_hidden_kernel,
        in_specs=[VMEM_SPEC] * 2 + [pl.BlockSpec(memory_space=pl.ANY)],
        out_specs=VMEM_SPEC,
        out_shape=pltpu.VMEM(shape, BF),
        scratch_shapes=[
            pltpu.VMEM(shape, F32),
            pltpu.VMEM(shape, F32),
            pltpu.VMEM((4, height // 4, units), BF),
            pltpu.SemaphoreType.DMA((4,)),
        ],
        compiler_params=pltpu.CompilerParams(vmem_limit_bytes=8 << 20),
    )(*near, pltpu.with_memory_space_constraint(w_up, pltpu.HBM))


def copy_kernel(value, out):
    out[...] = value[...]


def in_vmem(value):
    shape = jax.ShapeDtypeStruct(value.shape, value.dtype)
    return call(copy_kernel, shape, [value], unplaced=[0])


def stage_kernel(w0, w1, w2, w3, out):
    for k, piece in enumerate((w0, w1, w2, w3)):
        out[k] = piece[...]


def down_kernel(h0, h1, h2, h3, weights, out):
    total = mm(h0[...], weights[0]) + mm(h1[...], weights[1])
    total = total + mm(h2[...], weights[2]) + mm(h3[...], weights[3])
    out[...] = total.astype(BF).reshape(out.shape)


def both_halves(
    where,
    query,
    latent,
    rope_key,
    latent_gain,
    key_up,
    value_up,
    out_proj,
    tokens,
    moe_gain,
    routes,
    group_prob,
    expert_prob,
    w_gate,
    w_up,
    w_down,
):
    experts = lax.axis_size(EP)
    rows, width = tokens.shape
    w_gate, w_up, w_down = w_gate[0], w_up[0], w_down[0]
    down_w, down_r = paired(w_down, weight_mate), paired(w_down, row_mate)
    down_rw = paired(down_w, row_mate)
    gate_w, up_w = paired(w_gate, weight_mate), paired(w_up, weight_mate)
    set_a, set_b = [w_gate, w_up], [in_vmem(gate_w), up_w]
    outgoing, shares = dispatch(tokens, moe_gain, routes, group_prob, expert_prob, experts)
    arrived = lax.all_to_all(outgoing, EP, split_axis=0, concat_axis=0, tiled=True)
    queries, pair = query_and_pair(where, query, latent, rope_key, latent_gain, key_up, value_up)
    mate_rows = paired(arrived, row_mate)
    parts = attend(where, queries, pair)
    own_a = hidden_of(arrived, set_a)
    mate_a = paired(hidden_of(mate_rows, set_a), row_mate)
    mate_b = paired(late_hidden_of(mate_rows, *set_b), row_mate)
    own_b = hidden_of(arrived, set_b)
    shape = jax.ShapeDtypeStruct((4, *w_down.shape), BF)
    down = call(stage_kernel, shape, [w_down, down_w, down_r, down_rw], unplaced=range(4))
    shape = jax.ShapeDtypeStruct((experts, CAP, width), BF)
    arrays = [own_a, own_b, mate_a, mate_b, down]
    result = call(down_kernel, shape, arrays, place=pltpu.HBM)
    returned = lax.all_to_all(result, EP, split_axis=0, concat_axis=0, tiled=True)
    parts = out_parts(where, parts, latent.shape[0])
    height, span = out_proj.shape[0], width // 4
    near = [pltpu.with_memory_space_constraint(a, pltpu.VMEM) for a in [returned, shares] + parts]
    finish = pl.pallas_call(
        finish_kernel,
        in_specs=[SMEM_SPEC] + [VMEM_SPEC] * 6 + [pl.BlockSpec(memory_space=pl.ANY)],
        out_specs=[VMEM_SPEC] * 2,
        out_shape=[
            jax.ShapeDtypeStruct((rows, width), BF),
            jax.ShapeDtypeStruct((latent.shape[0], width), BF),
        ],
        scratch_shapes=[
            pltpu.VMEM((4, latent.shape[0], 4 * V_DIM), BF),
            pltpu.VMEM((4, height, span), BF),
            pltpu.SemaphoreType.DMA((4,)),
        ],
        compiler_params=pltpu.CompilerParams(vmem_limit_bytes=8 << 20),
        name="finish",
    )
    far = pltpu.with_memory_space_constraint(out_proj, pltpu.HBM)
    moe_out, mixed = finish(where, *near, far)
    return mixed, moe_out


def latent_kernel(latent, gain, rope_key, cosine, sine, out):
    width = latent.shape[1]
    half = ROPE_DIM // 2
    out[:, :width] = rms_scale(latent[...], gain[...]).astype(BF)
    rope = rope_key[...].astype(F32)
    crossed = jnp.concatenate([-rope[:, half:], rope[:, :half]], axis=1)
    out[:, width:] = (rope * cosine[...] + crossed * sine[...]).astype(BF)


def heads_kernel(
    where, l0, l1, l2, l3, key_up, value_up, query, cosine, sine, o0, o1, o2, o3, strip_s, heads
):
    latent = key_up.shape[0]
    own = l0.shape[0]
    count = heads.shape[0]
    half = ROPE_DIM // 2
    turned = query[...].astype(F32).T
    for h in range(count):
        at = h * QK_DIM
        a = turned[at + NOPE : at + NOPE + half]
        b = turned[at + NOPE + half : at + QK_DIM]
        heads[h, :NOPE, :] = turned[at : at + NOPE].astype(BF)
        heads[h, NOPE : NOPE + half, :] = (a * cosine[...] - b * sine[...]).astype(BF)
        heads[h, NOPE + half : QK_DIM, :] = (a * sine[...] + b * cosine[...]).astype(BF)
    for k, block in enumerate((l0, l1, l2, l3)):
        strip_s[k * own : (k + 1) * own, :] = block[...]
    got = strip_s[:, :latent]
    keys = mm(key_up[...], got, ((0,), (1,))).astype(BF)
    values = mm(value_up[...], got, ((0,), (1,))).astype(BF)
    eye = (
        lax.broadcasted_iota(jnp.int32, (ROPE_DIM, ROPE_DIM), 0)
        == lax.broadcasted_iota(jnp.int32, (ROPE_DIM, ROPE_DIM), 1)
    ).astype(BF)
    rope = mm(eye, strip_s[:, latent:], ((1,), (1,))).astype(BF)
    for h in range(count):
        heads[h, QK_DIM : QK_DIM + NOPE, :] = keys[h * NOPE : (h + 1) * NOPE]
        heads[h, QK_DIM + NOPE : 2 * QK_DIM, :] = rope
        heads[h, 2 * QK_DIM :, :] = values[h * V_DIM : (h + 1) * V_DIM]
    for k, out in enumerate((o0, o1, o2, o3)):
        out[...] = heads[lax.rem(where[0] + k, 4)]


def stack_kernel(b0, b1, b2, b3, out):
    for j, block in enumerate((b0, b1, b2, b3)):
        out[j] = block[QK_DIM:, :]


def attend_kernel(where, q0, q1, q2, q3, *refs):
    blocks, outs, (q_s, top_s, acc_s) = refs[:8], refs[8:12], refs[12:]
    zh, zl, y, c, x = (where[i] for i in range(5))
    strip = q0.shape[1]
    span = blocks[0].shape[2]
    factor = QK_DIM ** (-0.5) * log2_e
    for j, q in enumerate((q0, q1, q2, q3)):
        at = pl.multiple_of(lax.rem(zh - j + 4, 4) * strip, strip)
        q_s[pl.ds(at, strip), :] = q[:QK_DIM, :].astype(F32).T.astype(BF)
    top_s[...] = jnp.full(top_s.shape, masked_value, F32)
    acc_s[...] = jnp.zeros(acc_s.shape, F32)

    col = lax.broadcasted_iota(jnp.int32, (1, span), 1)
    col_zl = jnp.bitwise_xor(zl, col // strip)
    within = col % strip
    col_x = ((x - within // 32 + 4) % 4) * 32 + within % 32
    query_at = (zl * 8 + y * 2 + c) * strip + lax.broadcasted_iota(jnp.int32, (strip, 1), 0)
    ones = jnp.ones((V_DIM, span), BF)

    def advance(rows, parts, masks):
        q = q_s[rows, :]
        old = top_s[rows, :]
        scores = [mm(q, part[:QK_DIM, :]) for part in parts]
        if masks is not None:
            scores = [jnp.where(m, s, masked_value) for m, s in zip(masks, scores)]
        peak = scores[0]
        for s in scores[1:]:
            peak = jnp.maximum(peak, s)
        new = jnp.maximum(old, jnp.max(peak, axis=1, keepdims=True))
        top_s[rows, :] = new
        base = new[:, :1]
        total = acc_s[rows, :] * jnp.exp2((old - new) * factor)
        for s, part in zip(scores, parts):
            raised = jnp.exp2((s - base) * factor).astype(BF)
            extended = jnp.concatenate([part[QK_DIM:, :], ones], axis=0)
            total = total + mm(raised, extended, ((1,), (1,)))
        acc_s[rows, :] = total

    for m in range(2):
        group = blocks[4 * m : 4 * m + 4]
        masks = []
        for k in range(4):
            key_y = lax.rem(y - k + 4, 4)
            key_at = (col_zl * 8 + key_y * 2 + jnp.bitwise_xor(c, m)) * strip + col_x
            masks.append(key_at <= query_at)

        for g in range(4):
            from_zh = lax.rem(zh - g + 4, 4)
            parts = [block[from_zh] for block in group]
            advance(slice(g * strip, (g + 1) * strip), parts, masks)
            if g < 3:
                advance(slice((g + 1) * strip, 4 * strip), parts, None)
    total = acc_s[...]
    acc_s[:, :V_DIM] = total[:, :V_DIM] / total[:, V_DIM:]
    own = strip // 4
    for k, out in enumerate(outs):
        for g in range(4):
            at = pl.multiple_of(g * strip + lax.rem(x + k, 4) * own, own)
            out[g * own : (g + 1) * own, :] = acc_s[pl.ds(at, own), :V_DIM].astype(BF)


def spread_kernel(where, a0, a1, a2, a3, o0, o1, o2, o3, heads, parts):
    for k, a in enumerate((a0, a1, a2, a3)):
        heads[lax.rem(where[4] - k + 4, 4)] = a[...]
    beside = jnp.concatenate([heads[h] for h in range(4)], axis=1)
    parts[...] = beside.reshape(parts.shape)
    for j, out in enumerate((o0, o1, o2, o3)):
        out[...] = parts[lax.rem(where[0] + j, 4)]


def finish_kernel(
    where, returned, shares, a0, a1, a2, a3, out_proj, moe_out, mixed, parts, weights, sems
):
    count, _, span = weights.shape
    copies = [
        pltpu.make_async_copy(out_proj.at[:, pl.ds(c * span, span)], weights.at[c], sems.at[c])
        for c in range(count)
    ]
    for copy in copies:
        copy.start()
    rows = moe_out.shape[0]
    got = returned[...].reshape(shares.shape[0], moe_out.shape[1])
    both = mm(shares[...], got, ((0,), (0,)))
    moe_out[...] = (both[:rows] + both[rows:]).astype(BF)
    for j, a in enumerate((a0, a1, a2, a3)):
        parts[lax.rem(where[0] - j + 4, 4)] = a[...]
    pieces = [parts[h % 4, :, h // 4 * V_DIM : (h // 4 + 1) * V_DIM] for h in range(16)]
    beside = jnp.concatenate(pieces, axis=1)
    for c, copy in enumerate(copies):
        copy.wait()
        mixed[:, c * span : (c + 1) * span] = mm(beside, weights[c]).astype(BF)


def query_and_pair(where, query, latent, rope_key, latent_gain, key_up, value_up):
    strip = query.shape[0]
    own = latent.shape[0]
    query_start = (((where[0] * 2 + where[1]) * 4 + where[2]) * 2 + where[3]) * strip

    key_cos, key_sin = trig(query_start + where[4] * own + jnp.arange(own, dtype=jnp.int32))
    both = call(
        latent_kernel,
        jax.ShapeDtypeStruct((own, latent.shape[1] + ROPE_DIM), BF),
        [
            latent,
            latent_gain[None, :],
            rope_key,
            jnp.concatenate([key_cos, key_cos], axis=1),
            jnp.concatenate([key_sin, key_sin], axis=1),
        ],
        unplaced=range(3),
    )
    near = [both] + [shifted(both, "x", k) for k in range(1, 4)]
    cosine, sine = trig(query_start + jnp.arange(strip, dtype=jnp.int32))
    blocks = call(
        heads_kernel,
        [jax.ShapeDtypeStruct((QK_DIM + KV_ROWS, strip), BF)] * 4,
        near + [key_up, value_up, query, cosine.T, sine.T],
        where,
        scratch=[
            pltpu.VMEM((strip, both.shape[1]), BF),
            pltpu.VMEM((4, QK_DIM + KV_ROWS, strip), BF),
        ],
        unplaced=range(4, 7),
    )
    blocks = [blocks[0]] + [shifted(blocks[k], "zh", k) for k in range(1, 4)]
    shape = jax.ShapeDtypeStruct((4, KV_ROWS, strip), BF)
    mine = call(stack_kernel, shape, blocks)
    return blocks, jnp.concatenate([mine, shifted(mine, "zl", 1)], axis=2)


def attend(where, blocks, pair):
    strip = blocks[0].shape[1]
    column = [pair] + [shifted(pair, "y", k) for k in range(1, 4)]
    column = column + [shifted(part, "c", 1) for part in column]
    parts = call(
        attend_kernel,
        [jax.ShapeDtypeStruct((strip, V_DIM), BF)] * 4,
        blocks + column,
        where,
        [
            pltpu.VMEM((4 * strip, QK_DIM), BF),
            pltpu.VMEM((4 * strip, 128), F32),
            pltpu.VMEM((4 * strip, 128), F32),
        ],
    )
    return [parts[0]] + [shifted(parts[k], "x", k) for k in range(1, 4)]


def out_parts(where, parts, own):
    strip = parts[0].shape[0]
    parts = call(
        spread_kernel,
        [jax.ShapeDtypeStruct((own, 4 * V_DIM), BF)] * 4,
        parts,
        where,
        [pltpu.VMEM((4, strip, V_DIM), BF), pltpu.VMEM((4, own, 4 * V_DIM), BF)],
    )
    parts = [parts[0]] + [shifted(parts[j], "zh", j) for j in range(1, 4)]
    return parts


def body(
    query,
    latent,
    rope_key,
    latent_gain,
    key_up,
    value_up,
    out_proj,
    tokens,
    moe_gain,
    routes,
    group_prob,
    expert_prob,
    w_gate,
    w_up,
    w_down,
):
    where = jnp.stack([lax.axis_index(n) for n in AXES]).astype(jnp.int32)
    return both_halves(
        where,
        query,
        latent,
        rope_key,
        latent_gain,
        key_up,
        value_up,
        out_proj,
        tokens,
        moe_gain,
        routes,
        group_prob,
        expert_prob,
        w_gate,
        w_up,
        w_down,
    )


def solution(mesh):
    ep, every = EP, AXES
    split = Mesh(mesh.devices.reshape(4, 2, 4, 2, 4), AXES)
    return jax.shard_map(
        body,
        mesh=split,
        in_specs=(
            P(ep, "x"),
            P(every, None),
            P(every, None),
            P(),
            P(None, "x"),
            P(None, "x"),
            P(),
            P(every, None),
            P(),
            P(every, None),
            P(every),
            P(every, None),
            P(ep, None, "x"),
            P(ep, None, "x"),
            P(ep, "x", None),
        ),
        out_specs=(P(every, None), P(every, None)),
        check_vma=False,
    )
```

```python
import jax
import jax.numpy as jnp
from jax import lax
from jax.experimental import pallas as pl
from jax.experimental.pallas import tpu as pltpu
from jax.sharding import Mesh, PartitionSpec as P


NOPE = 64
ROPE_DIM = 32
V_DIM = 64
QK_DIM = NOPE + ROPE_DIM
KV_ROWS = QK_DIM + V_DIM
CAP = 4
BF = jnp.bfloat16
F32 = jnp.float32

epsilon = 1e-06
rope_base = 10000.0
masked_value = -1e30
log2_e = 1.4426950408889634


AXES = ("zh", "zl", "y", "c", "x")
EP = AXES[:4]

SMEM_SPEC = pl.BlockSpec(memory_space=pltpu.SMEM)
VMEM_SPEC = pl.BlockSpec(memory_space=pltpu.VMEM)


def call(kernel, out_shape, arrays, where=None, scratch=(), limit=8 << 20, unplaced=(), place=pltpu.VMEM):
    arrays = [
        pltpu.with_memory_space_constraint(a, pltpu.HBM if i in unplaced else pltpu.VMEM)
        for i, a in enumerate(arrays)
    ]
    specs = [VMEM_SPEC] * len(arrays)
    if where is not None:
        arrays, specs = [where] + arrays, [SMEM_SPEC] + specs
    single = not isinstance(out_shape, (list, tuple))
    if place is not None:
        if single:
            out_shape = place(out_shape.shape, out_shape.dtype)
        else:
            out_shape = [place(s.shape, s.dtype) for s in out_shape]
    return pl.pallas_call(
        kernel,
        in_specs=specs,
        out_specs=VMEM_SPEC if single else [VMEM_SPEC] * len(out_shape),
        out_shape=out_shape,
        scratch_shapes=list(scratch),
        compiler_params=pltpu.CompilerParams(vmem_limit_bytes=limit),
    )(*arrays)


def mm(a, b, dims=((1,), (0,))):
    return lax.dot_general(a, b, (dims, ((), ())), preferred_element_type=F32)


def shifted(value, axis, amount):
    n = lax.axis_size(axis)
    return lax.ppermute(value, axis, [(i, (i + amount) % n) for i in range(n)])


def paired(value, mate):
    n = lax.axis_size("x")
    return lax.ppermute(value, "x", [(i, mate(i)) for i in range(n)])


def weight_mate(i):
    return i ^ 1


def row_mate(i):
    return 3 - i


def trig(positions):
    half = ROPE_DIM // 2
    inverse = rope_base ** (-2.0 * jnp.arange(half, dtype=F32) / ROPE_DIM)
    angles = positions.astype(F32)[:, None] * inverse[None, :]
    return jnp.cos(angles), jnp.sin(angles)


def rms_scale(values, gain):
    widened = values.astype(F32)
    return widened * lax.rsqrt(jnp.mean(widened * widened, axis=-1, keepdims=True) + epsilon) * gain


def dispatch_kernel(tokens, gain, routes, group_prob, expert_prob, outgoing, shares_out):
    rows = tokens.shape[0]
    experts, cap, width = outgoing.shape
    slots = experts * cap
    normed = rms_scale(tokens[...], gain[...]).astype(BF)
    slot = lax.broadcasted_iota(jnp.int32, (slots, rows), 0)
    expert = slot // cap
    first = routes[0:1, :] == expert
    second = routes[1:2, :] == expert
    named = (first | second).astype(BF)
    before = lax.broadcasted_iota(jnp.int32, (rows, rows), 0) < lax.broadcasted_iota(
        jnp.int32, (rows, rows), 1
    )
    prior = mm(named, before.astype(BF))
    mine = (first | second) & (prior == (slot % cap).astype(F32))
    outgoing[...] = mm(mine.astype(BF), normed).reshape(experts, cap, width).astype(BF)
    probs = expert_prob[...]
    shares = group_prob[...] * probs / jnp.sum(probs, axis=0, keepdims=True)
    weights = jnp.where(first, shares[0:1, :], shares[1:2, :])
    weights = jnp.where(mine, weights, 0.0)
    high = weights.astype(BF)
    shares_out[:, 0:rows] = high
    shares_out[:, rows : 2 * rows] = (weights - high.astype(F32)).astype(BF)


def dispatch(tokens, gain, routes, group_prob, expert_prob, experts):
    rows, width = tokens.shape
    return call(
        dispatch_kernel,
        (
            jax.ShapeDtypeStruct((experts, CAP, width), BF),
            jax.ShapeDtypeStruct((experts * CAP, 2 * rows), BF),
        ),
        [tokens, gain[None, :], routes.T, group_prob[None, :], expert_prob.T],
        unplaced=range(5),
        place=pltpu.HBM,
    )


def hidden_kernel(rows, w_gate, w_up, out, gate_s, up_s):
    count, span = out.shape[0], 1024
    gate_s[...] = jnp.zeros(gate_s.shape, F32)
    up_s[...] = jnp.zeros(up_s.shape, F32)

    def add(step, _):
        cols = pl.ds(pl.multiple_of(step * span, span), span)
        got = rows[:, :, cols].reshape(count, span)
        gate_s[...] += mm(got, w_gate[cols, :])
        up_s[...] += mm(got, w_up[cols, :])
        return 0

    lax.fori_loop(0, w_gate.shape[0] // span, add, 0)
    gate = gate_s[...]
    out[...] = (gate / (1.0 + jnp.exp(-gate)) * up_s[...]).astype(BF)


def hidden_of(rows, weights):
    shape = jax.ShapeDtypeStruct((rows.shape[0] * CAP, weights[0].shape[1]), BF)
    scratch = [pltpu.VMEM(shape.shape, F32)] * 2
    return call(hidden_kernel, shape, [rows] + weights, scratch=scratch)


def late_hidden_kernel(rows, w_gate, w_up, out, gate_s, up_s, up_v, sems):
    count, steps = out.shape[0], sems.shape[0]
    span = w_up.shape[0] // steps
    parts = [slice(c * span, (c + 1) * span) for c in range(steps)]
    copies = [
        pltpu.make_async_copy(w_up.at[pl.ds(c * span, span), :], up_v.at[c], sems.at[c])
        for c in range(steps)
    ]
    for copy in copies:
        copy.start()
    for c, cols in enumerate(parts):
        got = rows[:, :, cols].reshape(count, span)
        gate = mm(got, w_gate[cols, :])
        copies[c].wait()
        up = mm(got, up_v[c])
        gate_s[...] = gate if c == 0 else gate_s[...] + gate
        up_s[...] = up if c == 0 else up_s[...] + up
    gate = gate_s[...]
    out[...] = (gate / (1.0 + jnp.exp(-gate)) * up_s[...]).astype(BF)


def late_hidden_of(rows, w_gate, w_up):
    height, units = w_up.shape
    shape = (rows.shape[0] * CAP, units)
    near = [pltpu.with_memory_space_constraint(a, pltpu.VMEM) for a in (rows, w_gate)]
    return pl.pallas_call(
        late_hidden_kernel,
        in_specs=[VMEM_SPEC] * 2 + [pl.BlockSpec(memory_space=pl.ANY)],
        out_specs=VMEM_SPEC,
        out_shape=pltpu.VMEM(shape, BF),
        scratch_shapes=[
            pltpu.VMEM(shape, F32),
            pltpu.VMEM(shape, F32),
            pltpu.VMEM((4, height // 4, units), BF),
            pltpu.SemaphoreType.DMA((4,)),
        ],
        compiler_params=pltpu.CompilerParams(vmem_limit_bytes=8 << 20),
    )(*near, pltpu.with_memory_space_constraint(w_up, pltpu.HBM))


def copy_kernel(value, out):
    out[...] = value[...]


def in_vmem(value):
    shape = jax.ShapeDtypeStruct(value.shape, value.dtype)
    return call(copy_kernel, shape, [value], unplaced=[0])


def stage_kernel(w0, w1, w2, w3, out):
    for k, piece in enumerate((w0, w1, w2, w3)):
        out[k] = piece[...]


def down_kernel(h0, h1, h2, h3, weights, out, pieces, sems):
    count, experts, cap, span = pieces.shape
    hidden = [h[...] for h in (h0, h1, h2, h3)]
    copies = []
    for c in range(count):
        cols = slice(c * span, (c + 1) * span)
        total = mm(hidden[0], weights[0, :, cols])
        for k in range(1, 4):
            total = total + mm(hidden[k], weights[k, :, cols])
        pieces[c] = total.astype(BF).reshape(experts, cap, span)
        copies.append(
            pltpu.make_async_copy(
                pieces.at[c], out.at[:, :, pl.ds(c * span, span)], sems.at[c]
            )
        )
        copies[c].start()
    for copy in copies:
        copy.wait()


def down_of(arrays, experts, width):
    near = [pltpu.with_memory_space_constraint(a, pltpu.VMEM) for a in arrays]
    return pl.pallas_call(
        down_kernel,
        in_specs=[VMEM_SPEC] * len(near),
        out_specs=pl.BlockSpec(memory_space=pl.ANY),
        out_shape=pltpu.HBM((experts, CAP, width), BF),
        scratch_shapes=[
            pltpu.VMEM((4, experts, CAP, width // 4), BF),
            pltpu.SemaphoreType.DMA((4,)),
        ],
        compiler_params=pltpu.CompilerParams(vmem_limit_bytes=8 << 20),
        name="down",
    )(*near)


def both_halves(
    where,
    query,
    latent,
    rope_key,
    latent_gain,
    key_up,
    value_up,
    out_proj,
    tokens,
    moe_gain,
    routes,
    group_prob,
    expert_prob,
    w_gate,
    w_up,
    w_down,
):
    experts = lax.axis_size(EP)
    rows, width = tokens.shape
    w_gate, w_up, w_down = w_gate[0], w_up[0], w_down[0]
    down_w, down_r = paired(w_down, weight_mate), paired(w_down, row_mate)
    down_rw = paired(down_w, row_mate)
    gate_w, up_w = paired(w_gate, weight_mate), paired(w_up, weight_mate)
    set_a, set_b = [w_gate, w_up], [in_vmem(gate_w), up_w]
    outgoing, shares = dispatch(tokens, moe_gain, routes, group_prob, expert_prob, experts)
    arrived = lax.all_to_all(outgoing, EP, split_axis=0, concat_axis=0, tiled=True)
    queries, pair = query_and_pair(where, query, latent, rope_key, latent_gain, key_up, value_up)
    mate_rows = paired(arrived, row_mate)
    parts = attend(where, queries, pair)
    own_a = hidden_of(arrived, set_a)
    mate_a = paired(hidden_of(mate_rows, set_a), row_mate)
    mate_b = paired(late_hidden_of(mate_rows, *set_b), row_mate)
    own_b = hidden_of(arrived, set_b)
    shape = jax.ShapeDtypeStruct((4, *w_down.shape), BF)
    down = call(stage_kernel, shape, [w_down, down_w, down_r, down_rw], unplaced=range(4))
    result = down_of([own_a, own_b, mate_a, mate_b, down], experts, width)
    returned = lax.all_to_all(result, EP, split_axis=0, concat_axis=0, tiled=True)
    parts = out_parts(where, parts, latent.shape[0])
    height, span = out_proj.shape[0], width // 4
    near = [pltpu.with_memory_space_constraint(a, pltpu.VMEM) for a in [returned, shares] + parts]
    finish = pl.pallas_call(
        finish_kernel,
        in_specs=[SMEM_SPEC] + [VMEM_SPEC] * 6 + [pl.BlockSpec(memory_space=pl.ANY)],
        out_specs=[VMEM_SPEC] * 2,
        out_shape=[
            jax.ShapeDtypeStruct((rows, width), BF),
            jax.ShapeDtypeStruct((latent.shape[0], width), BF),
        ],
        scratch_shapes=[
            pltpu.VMEM((4, latent.shape[0], 4 * V_DIM), BF),
            pltpu.VMEM((4, height, span), BF),
            pltpu.SemaphoreType.DMA((4,)),
        ],
        compiler_params=pltpu.CompilerParams(vmem_limit_bytes=8 << 20),
        name="finish",
    )
    far = pltpu.with_memory_space_constraint(out_proj, pltpu.HBM)
    moe_out, mixed = finish(where, *near, far)
    return mixed, moe_out


def latent_kernel(latent, gain, rope_key, cosine, sine, out):
    width = latent.shape[1]
    half = ROPE_DIM // 2
    out[:, :width] = rms_scale(latent[...], gain[...]).astype(BF)
    rope = rope_key[...].astype(F32)
    crossed = jnp.concatenate([-rope[:, half:], rope[:, :half]], axis=1)
    out[:, width:] = (rope * cosine[...] + crossed * sine[...]).astype(BF)


def heads_kernel(
    where, l0, l1, l2, l3, key_up, value_up, query, cosine, sine, o0, o1, o2, o3, strip_s, heads
):
    latent = key_up.shape[0]
    own = l0.shape[0]
    count = heads.shape[0]
    half = ROPE_DIM // 2
    turned = query[...].astype(F32).T
    for h in range(count):
        at = h * QK_DIM
        a = turned[at + NOPE : at + NOPE + half]
        b = turned[at + NOPE + half : at + QK_DIM]
        heads[h, :NOPE, :] = turned[at : at + NOPE].astype(BF)
        heads[h, NOPE : NOPE + half, :] = (a * cosine[...] - b * sine[...]).astype(BF)
        heads[h, NOPE + half : QK_DIM, :] = (a * sine[...] + b * cosine[...]).astype(BF)
    for k, block in enumerate((l0, l1, l2, l3)):
        strip_s[k * own : (k + 1) * own, :] = block[...]
    got = strip_s[:, :latent]
    keys = mm(key_up[...], got, ((0,), (1,))).astype(BF)
    values = mm(value_up[...], got, ((0,), (1,))).astype(BF)
    eye = (
        lax.broadcasted_iota(jnp.int32, (ROPE_DIM, ROPE_DIM), 0)
        == lax.broadcasted_iota(jnp.int32, (ROPE_DIM, ROPE_DIM), 1)
    ).astype(BF)
    rope = mm(eye, strip_s[:, latent:], ((1,), (1,))).astype(BF)
    for h in range(count):
        heads[h, QK_DIM : QK_DIM + NOPE, :] = keys[h * NOPE : (h + 1) * NOPE]
        heads[h, QK_DIM + NOPE : 2 * QK_DIM, :] = rope
        heads[h, 2 * QK_DIM :, :] = values[h * V_DIM : (h + 1) * V_DIM]
    for k, out in enumerate((o0, o1, o2, o3)):
        out[...] = heads[lax.rem(where[0] + k, 4)]


def stack_kernel(b0, b1, b2, b3, out):
    for j, block in enumerate((b0, b1, b2, b3)):
        out[j] = block[QK_DIM:, :]


def attend_kernel(where, q0, q1, q2, q3, *refs):
    blocks, outs, (q_s, top_s, acc_s) = refs[:8], refs[8:12], refs[12:]
    zh, zl, y, c, x = (where[i] for i in range(5))
    strip = q0.shape[1]
    span = blocks[0].shape[2]
    factor = QK_DIM ** (-0.5) * log2_e
    for j, q in enumerate((q0, q1, q2, q3)):
        at = pl.multiple_of(lax.rem(zh - j + 4, 4) * strip, strip)
        q_s[pl.ds(at, strip), :] = q[:QK_DIM, :].astype(F32).T.astype(BF)
    top_s[...] = jnp.full(top_s.shape, masked_value, F32)
    acc_s[...] = jnp.zeros(acc_s.shape, F32)

    col = lax.broadcasted_iota(jnp.int32, (1, span), 1)
    col_zl = jnp.bitwise_xor(zl, col // strip)
    within = col % strip
    col_x = ((x - within // 32 + 4) % 4) * 32 + within % 32
    query_at = (zl * 8 + y * 2 + c) * strip + lax.broadcasted_iota(jnp.int32, (strip, 1), 0)
    ones = jnp.ones((V_DIM, span), BF)

    def advance(rows, parts, masks):
        q = q_s[rows, :]
        old = top_s[rows, :]
        scores = [mm(q, part[:QK_DIM, :]) for part in parts]
        if masks is not None:
            scores = [jnp.where(m, s, masked_value) for m, s in zip(masks, scores)]
        peak = scores[0]
        for s in scores[1:]:
            peak = jnp.maximum(peak, s)
        new = jnp.maximum(old, jnp.max(peak, axis=1, keepdims=True))
        top_s[rows, :] = new
        base = new[:, :1]
        total = acc_s[rows, :] * jnp.exp2((old - new) * factor)
        for s, part in zip(scores, parts):
            raised = jnp.exp2((s - base) * factor).astype(BF)
            extended = jnp.concatenate([part[QK_DIM:, :], ones], axis=0)
            total = total + mm(raised, extended, ((1,), (1,)))
        acc_s[rows, :] = total

    for m in range(2):
        group = blocks[4 * m : 4 * m + 4]
        masks = []
        for k in range(4):
            key_y = lax.rem(y - k + 4, 4)
            key_at = (col_zl * 8 + key_y * 2 + jnp.bitwise_xor(c, m)) * strip + col_x
            masks.append(key_at <= query_at)

        for g in range(4):
            from_zh = lax.rem(zh - g + 4, 4)
            parts = [block[from_zh] for block in group]
            advance(slice(g * strip, (g + 1) * strip), parts, masks)
            if g < 3:
                advance(slice((g + 1) * strip, 4 * strip), parts, None)
    total = acc_s[...]
    acc_s[:, :V_DIM] = total[:, :V_DIM] / total[:, V_DIM:]
    own = strip // 4
    for k, out in enumerate(outs):
        for g in range(4):
            at = pl.multiple_of(g * strip + lax.rem(x + k, 4) * own, own)
            out[g * own : (g + 1) * own, :] = acc_s[pl.ds(at, own), :V_DIM].astype(BF)


def spread_kernel(where, a0, a1, a2, a3, o0, o1, o2, o3, heads, parts):
    for k, a in enumerate((a0, a1, a2, a3)):
        heads[lax.rem(where[4] - k + 4, 4)] = a[...]
    beside = jnp.concatenate([heads[h] for h in range(4)], axis=1)
    parts[...] = beside.reshape(parts.shape)
    for j, out in enumerate((o0, o1, o2, o3)):
        out[...] = parts[lax.rem(where[0] + j, 4)]


def finish_kernel(
    where, returned, shares, a0, a1, a2, a3, out_proj, moe_out, mixed, parts, weights, sems
):
    count, _, span = weights.shape
    copies = [
        pltpu.make_async_copy(out_proj.at[:, pl.ds(c * span, span)], weights.at[c], sems.at[c])
        for c in range(count)
    ]
    for copy in copies:
        copy.start()
    rows = moe_out.shape[0]
    got = returned[...].reshape(shares.shape[0], moe_out.shape[1])
    both = mm(shares[...], got, ((0,), (0,)))
    moe_out[...] = (both[:rows] + both[rows:]).astype(BF)
    for j, a in enumerate((a0, a1, a2, a3)):
        parts[lax.rem(where[0] - j + 4, 4)] = a[...]
    pieces = [parts[h % 4, :, h // 4 * V_DIM : (h // 4 + 1) * V_DIM] for h in range(16)]
    beside = jnp.concatenate(pieces, axis=1)
    for c, copy in enumerate(copies):
        copy.wait()
        mixed[:, c * span : (c + 1) * span] = mm(beside, weights[c]).astype(BF)


def query_and_pair(where, query, latent, rope_key, latent_gain, key_up, value_up):
    strip = query.shape[0]
    own = latent.shape[0]
    query_start = (((where[0] * 2 + where[1]) * 4 + where[2]) * 2 + where[3]) * strip

    key_cos, key_sin = trig(query_start + where[4] * own + jnp.arange(own, dtype=jnp.int32))
    both = call(
        latent_kernel,
        jax.ShapeDtypeStruct((own, latent.shape[1] + ROPE_DIM), BF),
        [
            latent,
            latent_gain[None, :],
            rope_key,
            jnp.concatenate([key_cos, key_cos], axis=1),
            jnp.concatenate([key_sin, key_sin], axis=1),
        ],
        unplaced=range(3),
    )
    near = [both] + [shifted(both, "x", k) for k in range(1, 4)]
    cosine, sine = trig(query_start + jnp.arange(strip, dtype=jnp.int32))
    blocks = call(
        heads_kernel,
        [jax.ShapeDtypeStruct((QK_DIM + KV_ROWS, strip), BF)] * 4,
        near + [key_up, value_up, query, cosine.T, sine.T],
        where,
        scratch=[
            pltpu.VMEM((strip, both.shape[1]), BF),
            pltpu.VMEM((4, QK_DIM + KV_ROWS, strip), BF),
        ],
        unplaced=range(4, 7),
    )
    blocks = [blocks[0]] + [shifted(blocks[k], "zh", k) for k in range(1, 4)]
    shape = jax.ShapeDtypeStruct((4, KV_ROWS, strip), BF)
    mine = call(stack_kernel, shape, blocks)
    return blocks, jnp.concatenate([mine, shifted(mine, "zl", 1)], axis=2)


def attend(where, blocks, pair):
    strip = blocks[0].shape[1]
    column = [pair] + [shifted(pair, "y", k) for k in range(1, 4)]
    column = column + [shifted(part, "c", 1) for part in column]
    parts = call(
        attend_kernel,
        [jax.ShapeDtypeStruct((strip, V_DIM), BF)] * 4,
        blocks + column,
        where,
        [
            pltpu.VMEM((4 * strip, QK_DIM), BF),
            pltpu.VMEM((4 * strip, 128), F32),
            pltpu.VMEM((4 * strip, 128), F32),
        ],
    )
    return [parts[0]] + [shifted(parts[k], "x", k) for k in range(1, 4)]


def out_parts(where, parts, own):
    strip = parts[0].shape[0]
    parts = call(
        spread_kernel,
        [jax.ShapeDtypeStruct((own, 4 * V_DIM), BF)] * 4,
        parts,
        where,
        [pltpu.VMEM((4, strip, V_DIM), BF), pltpu.VMEM((4, own, 4 * V_DIM), BF)],
    )
    parts = [parts[0]] + [shifted(parts[j], "zh", j) for j in range(1, 4)]
    return parts


def body(
    query,
    latent,
    rope_key,
    latent_gain,
    key_up,
    value_up,
    out_proj,
    tokens,
    moe_gain,
    routes,
    group_prob,
    expert_prob,
    w_gate,
    w_up,
    w_down,
):
    where = jnp.stack([lax.axis_index(n) for n in AXES]).astype(jnp.int32)
    return both_halves(
        where,
        query,
        latent,
        rope_key,
        latent_gain,
        key_up,
        value_up,
        out_proj,
        tokens,
        moe_gain,
        routes,
        group_prob,
        expert_prob,
        w_gate,
        w_up,
        w_down,
    )


def solution(mesh):
    ep, every = EP, AXES
    split = Mesh(mesh.devices.reshape(4, 2, 4, 2, 4), AXES)
    return jax.shard_map(
        body,
        mesh=split,
        in_specs=(
            P(ep, "x"),
            P(every, None),
            P(every, None),
            P(),
            P(None, "x"),
            P(None, "x"),
            P(),
            P(every, None),
            P(),
            P(every, None),
            P(every),
            P(every, None),
            P(ep, None, "x"),
            P(ep, None, "x"),
            P(ep, "x", None),
        ),
        out_specs=(P(every, None), P(every, None)),
        check_vma=False,
    )
```
